32 devices in a mesh: sp: 8 (over z, x), tp: 4 (over y, core).
Axes of the slice: x: 2, y: 2, z: 4, core: 2. Of those that a mesh axis runs over, the one named last changes fastest.
Arguments:
- tokens: bfloat16 [6144, 4096], P('sp', 'tp'), may hold values from -12 to 12
- query_weight: bfloat16 [4096, 2048], P(None, 'tp'), may hold values from -0.09375 to 0.09375
- key_weight: bfloat16 [4096, 2048], P(None, 'tp'), may hold values from -0.09375 to 0.09375
- value_weight: bfloat16 [4096, 2048], P(None, 'tp'), may hold values from -0.09375 to 0.09375
- position_bias: float32 [16, 320], P('tp'), may hold values from -104 to 154
- out_grad: bfloat16 [6144, 2048], P('sp', 'tp'), may hold values from -6 to 6
Outputs:
- input_grad: bfloat16 [6144, 4096], P('sp', 'tp')
- query_weight_grad: float32 [4096, 2048], P('sp', 'tp')
- key_weight_grad: float32 [4096, 2048], P('sp', 'tp')
- value_weight_grad: float32 [4096, 2048], P('sp', 'tp')
- bias_grad: float32 [16, 320], P('tp')
The draws below stay inside these ranges and needn't reach their ends.
All inputs are finite; a program needn't handle non-finite values.
Results may differ from the reference program's by a relative error of at most 0.014.
Values may be sent and summed in bfloat16 or wider, within the bound.
A program may use at most 128 MiB of HBM per device.

```python
import jax
import jax.numpy as jnp
import numpy as np
from jax import lax

WIDTH = 4096
HEADS = 16
HEAD_DIM = 128
SEGMENT = 64
PREVIOUS = 4
CLIP = 256
TOKENS = 6144
ATT_WIDTH = 2048
BIAS_LEN = 320
N_TP = 4


def draw_tokens(key, part):
    base = jax.random.normal(jax.random.fold_in(key, 11), (TOKENS, WIDTH), jnp.float32)
    base = jnp.clip(base, -6.0, 6.0)
    return base.astype(jnp.bfloat16)


def draw_position_bias(key, part):
    base = jax.random.normal(jax.random.fold_in(key, 21), (HEADS, BIAS_LEN), jnp.float32)
    base = jnp.clip(base, -4.0, 4.0)
    return base.astype(jnp.float32)


def shard_levels(rng, shape, split, smallest, top_value):
    level = 1.0
    for dim, blocks in split:
        heights = jax.random.uniform(jax.random.fold_in(jax.random.fold_in(rng, 6), dim), (blocks,), jnp.float32, smallest / len(split), top_value / len(split))
        level = level * jnp.repeat(jnp.exp(heights), shape[dim] // blocks).reshape((-1,) + (1,) * (len(shape) - 1 - dim))
    return level


def bell_draw(stream_key, extent, scale, most, shards=(), kind=jnp.bfloat16):
    values = scale * jax.random.normal(stream_key, extent, jnp.float32)
    if shards:
        values = values * shard_levels(stream_key, extent, shards, -0.22, 0.18)
    return jnp.clip(values, -most, most).astype(kind)


def setup_inputs(seed: int = 0) -> dict:
    arg_keys = jax.random.split(jax.random.key(seed), 7)
    tokens = draw_tokens(jax.random.fold_in(arg_keys[6], 71), 0)
    query_weight = bell_draw(arg_keys[1], (WIDTH, ATT_WIDTH), WIDTH ** -0.5, 0.09375, ((1, 4),))
    key_weight = bell_draw(arg_keys[2], (WIDTH, ATT_WIDTH), WIDTH ** -0.5, 0.09375, ((1, 4),))
    value_weight = bell_draw(arg_keys[3], (WIDTH, ATT_WIDTH), WIDTH ** -0.5, 0.09375, ((1, 4),))
    position_bias = draw_position_bias(jax.random.fold_in(arg_keys[6], 71), 0)
    out_grad = bell_draw(arg_keys[5], (TOKENS, ATT_WIDTH), 1.0, 6.0, ((0, 8), (1, 4)))
    return {"tokens": tokens, "query_weight": query_weight, "key_weight": key_weight, "value_weight": value_weight, "position_bias": position_bias, "out_grad": out_grad}


def bias_index(segment, reach, clip):
    query_pos = np.arange(segment)[:, None]
    band_pos = np.arange(reach + segment)[None, :]
    return (np.minimum(reach + query_pos - band_pos, clip) + segment - 1).astype(np.int32)


def fold_band(parts, count, head):
    shaped = parts.reshape(count, PREVIOUS + 1, SEGMENT, head)
    total = jnp.zeros((count + PREVIOUS, SEGMENT, head), jnp.float32)
    for band in range(PREVIOUS + 1):
        total = total.at[band:band + count].add(shaped[:, band])
    return total.reshape((count + PREVIOUS) * SEGMENT, head)


def head_grads(operands):
    query, keys, values, upstream, table = operands
    length, head = query.shape
    reach = PREVIOUS * SEGMENT
    count = length // SEGMENT
    factor = head ** -0.5
    padding = jnp.zeros((reach, head), keys.dtype)
    key_seg = jnp.concatenate([padding, keys]).reshape(count + PREVIOUS, SEGMENT, head)
    value_seg = jnp.concatenate([padding, values]).reshape(count + PREVIOUS, SEGMENT, head)
    key_band = jnp.stack([key_seg[band:band + count] for band in range(PREVIOUS + 1)], axis=1).reshape(count, reach + SEGMENT, head)
    value_band = jnp.stack([value_seg[band:band + count] for band in range(PREVIOUS + 1)], axis=1).reshape(count, reach + SEGMENT, head)
    query_seg = query.reshape(count, SEGMENT, head)
    grad_seg = upstream.reshape(count, SEGMENT, head)
    flat_index = bias_index(SEGMENT, reach, CLIP)
    bias = table[flat_index]
    scores = jnp.einsum('cqd,ckd->cqk', query_seg.astype(jnp.float32), key_band.astype(jnp.float32)) * factor + bias[None]
    key_pos = jnp.arange(count)[:, None] * SEGMENT - reach + jnp.arange(reach + SEGMENT)[None, :]
    valid = (key_pos >= 0)[:, None, :]
    masked = jnp.where(valid, scores, -jnp.inf)
    top = jnp.max(masked, axis=-1, keepdims=True)
    logsum = top + jnp.log(jnp.sum(jnp.exp(masked - top), axis=-1, keepdims=True))
    weights = jnp.exp(masked - logsum)
    weights_low = weights.astype(jnp.bfloat16)
    prob_grad = jnp.einsum('cqd,ckd->cqk', grad_seg.astype(jnp.float32), value_band.astype(jnp.float32))
    delta = jnp.sum(weights * prob_grad, axis=-1, keepdims=True)
    score_grad = weights * (prob_grad - delta)
    score_low = score_grad.astype(jnp.bfloat16)
    query_grad = (jnp.einsum('cqk,ckd->cqd', score_low.astype(jnp.float32), key_band.astype(jnp.float32)) * factor).reshape(length, head).astype(jnp.bfloat16)
    key_parts = jnp.einsum('cqk,cqd->ckd', score_low.astype(jnp.float32), query_seg.astype(jnp.float32)) * factor
    value_parts = jnp.einsum('cqk,cqd->ckd', weights_low.astype(jnp.float32), grad_seg.astype(jnp.float32))
    key_grad = fold_band(key_parts, count, head)[reach:].astype(jnp.bfloat16)
    value_grad = fold_band(value_parts, count, head)[reach:].astype(jnp.bfloat16)
    summed = jnp.sum(score_grad, axis=0).reshape(-1)
    table_grad = jnp.zeros((table.shape[0],), jnp.float32).at[flat_index.reshape(-1)].add(summed)
    return query_grad, key_grad, value_grad, table_grad


def reference(tokens, query_weight, key_weight, value_weight, position_bias, out_grad):
    query = jnp.dot(tokens, query_weight, preferred_element_type=jnp.float32).astype(jnp.bfloat16)
    keys = jnp.dot(tokens, key_weight, preferred_element_type=jnp.float32).astype(jnp.bfloat16)
    values = jnp.dot(tokens, value_weight, preferred_element_type=jnp.float32).astype(jnp.bfloat16)

    def by_head(array):
        return array.reshape(TOKENS, HEADS, HEAD_DIM).transpose(1, 0, 2)

    def by_token(array):
        return array.transpose(1, 0, 2).reshape(TOKENS, HEADS * HEAD_DIM)

    head_query, head_key, head_value, bias_grad = lax.map(head_grads, (by_head(query), by_head(keys), by_head(values), by_head(out_grad), position_bias))
    query_grad = by_token(head_query)
    key_grad = by_token(head_key)
    value_grad = by_token(head_value)
    tokens_t = tokens.T
    query_weight_grad = jnp.dot(tokens_t, query_grad, preferred_element_type=jnp.float32)
    key_weight_grad = jnp.dot(tokens_t, key_grad, preferred_element_type=jnp.float32)
    value_weight_grad = jnp.dot(tokens_t, value_grad, preferred_element_type=jnp.float32)
    group = HEADS * HEAD_DIM // N_TP
    total = jnp.zeros((TOKENS, WIDTH), jnp.float32)
    for number in range(N_TP):
        lower = number * group
        upper = lower + group
        term = jnp.dot(query_grad[:, lower:upper], query_weight[:, lower:upper].T, preferred_element_type=jnp.float32)
        term = term + jnp.dot(key_grad[:, lower:upper], key_weight[:, lower:upper].T, preferred_element_type=jnp.float32)
        term = term + jnp.dot(value_grad[:, lower:upper], value_weight[:, lower:upper].T, preferred_element_type=jnp.float32)
        rounded = lax.optimization_barrier(term.astype(jnp.bfloat16))
        total = total + rounded.astype(jnp.float32)
    input_grad = total.astype(jnp.bfloat16)
    return (input_grad, query_weight_grad, key_weight_grad, value_weight_grad, bias_grad)
```

```python
import functools

import jax
import jax.numpy as jnp
from jax import lax
from jax.experimental import pallas as pl
from jax.experimental.pallas import tpu as pltpu
from jax.sharding import PartitionSpec as P

SEGMENT = 64
PREVIOUS = 4
CLIP = 256
ROWS = 2 * SEGMENT
REACH = PREVIOUS * SEGMENT
WINDOW = ROWS + REACH
TABLE = 512
HIDDEN = -1e30


def contract_rows(left, right):
    return lax.dot_general(
        left, right, (((0,), (0,)), ((), ())), preferred_element_type=jnp.float32
    )


def contract_cols(left, right):
    return lax.dot_general(
        left, right, (((1,), (1,)), ((), ())), preferred_element_type=jnp.float32
    )


def diagonal_sums(tile):
    half = tile.shape[0] // 2
    while half >= 8:
        tile = tile[:half] + pltpu.roll(tile[half:], TABLE - half, 1)
        half //= 2
    row = lax.broadcasted_iota(jnp.int32, tile.shape, 0)
    for step in (4, 2, 1):
        tile = jnp.where((row & step) != 0, pltpu.roll(tile, TABLE - step, 1), tile)
    return jnp.sum(tile, axis=0, keepdims=True)


def attention_kernel(
    factor,
    first_ref,
    q_ref,
    k_ref,
    v_ref,
    prev_ref,
    g_ref,
    table_ref,
    dq_ref,
    dk_ref,
    dv_ref,
    dk_tail_ref,
    dv_tail_ref,
    back_ref,
    table_grad_ref,
    k_all,
    v_all,
    dk_all,
    dv_all,
):
    length = q_ref.shape[0]
    k_all[:REACH] = prev_ref[0]
    k_all[REACH:] = k_ref[...]
    v_all[:REACH] = prev_ref[1]
    v_all[REACH:] = v_ref[...]
    dk_all[...] = jnp.zeros_like(dk_all)
    dv_all[...] = jnp.zeros_like(dv_all)
    first = first_ref[0]
    table = jnp.broadcast_to(table_ref[0], (ROWS, TABLE))
    bias = pltpu.roll(table, 0, 1, stride=1, stride_axis=0)[:, :WINDOW]
    row = lax.broadcasted_iota(jnp.int32, (ROWS, WINDOW), 0) // SEGMENT
    column = lax.broadcasted_iota(jnp.int32, (ROWS, WINDOW), 1)
    behind = column // SEGMENT - row
    bias = jnp.where((behind >= 0) & (behind <= PREVIOUS), bias, HIDDEN)
    bias_sum = jnp.zeros((ROWS, WINDOW), jnp.float32)
    for start in range(0, length, ROWS):
        q = q_ref[start : start + ROWS]
        g = g_ref[start : start + ROWS]
        k = k_all[start : start + WINDOW]
        v = v_all[start : start + WINDOW]
        mask = bias
        if start < REACH:
            mask = jnp.where(column + start < first, HIDDEN, bias)
        scores = contract_cols(q, k) * factor + mask
        top = jnp.max(scores, axis=1, keepdims=True)
        raised = jnp.exp(scores - top)
        weights = raised * (1.0 / jnp.sum(raised, axis=1, keepdims=True))
        prob_grad = contract_cols(g, v)
        delta = jnp.sum(weights * prob_grad, axis=1, keepdims=True)
        score_grad = weights * (prob_grad - delta)
        bias_sum = bias_sum + score_grad
        low = score_grad.astype(jnp.bfloat16)
        dq = jnp.dot(low, k, preferred_element_type=jnp.float32) * factor
        dq_ref[start : start + ROWS] = dq.astype(jnp.bfloat16)
        dk_all[start : start + WINDOW] += contract_rows(low, q)
        dv_all[start : start + WINDOW] += contract_rows(weights.astype(jnp.bfloat16), g)
    back_ref[0] = (dk_all[:REACH] * factor).astype(jnp.bfloat16)
    back_ref[1] = dv_all[:REACH].astype(jnp.bfloat16)
    dk_ref[...] = (dk_all[REACH:length] * factor).astype(jnp.bfloat16)
    dv_ref[...] = dv_all[REACH:length].astype(jnp.bfloat16)
    dk_tail_ref[...] = dk_all[length:] * factor
    dv_tail_ref[...] = dv_all[length:]
    padded = jnp.concatenate([bias_sum, jnp.zeros((ROWS, TABLE - WINDOW), jnp.float32)], axis=1)
    table_grad_ref[0] = diagonal_sums(padded)


def attention(query, keys, values, prev, out_grad, position_bias):
    length, width = query.shape
    heads, entries = position_bias.shape
    head = width // heads
    factor = head ** (-0.5)
    table = jnp.concatenate(
        [
            position_bias[:, ::-1],
            jnp.zeros((heads, WINDOW - entries), jnp.float32),
            jnp.broadcast_to(position_bias[:, entries - 1 :], (heads, TABLE - WINDOW)),
        ],
        axis=1,
    )[:, None]
    first = jnp.where(lax.axis_index("sp") == 0, REACH, 0).astype(jnp.int32)[None]

    def rows(count):
        return pl.BlockSpec((count, head), lambda h: (0, h))

    line = pl.BlockSpec((1, 1, TABLE), lambda h: (h, 0, 0))

    def shape(count, kind):
        return jax.ShapeDtypeStruct((count, width), kind)

    body = length - REACH
    elements = heads * length * WINDOW
    outs = pl.pallas_call(
        functools.partial(attention_kernel, factor),
        grid=(heads,),
        in_specs=[
            pl.BlockSpec(memory_space=pltpu.SMEM),
            rows(length),
            rows(length),
            rows(length),
            pl.BlockSpec((2, REACH, head), lambda h: (0, 0, h)),
            rows(length),
            line,
        ],
        out_specs=[
            rows(length),
            rows(body),
            rows(body),
            rows(REACH),
            rows(REACH),
            pl.BlockSpec((2, REACH, head), lambda h: (0, 0, h)),
            line,
        ],
        out_shape=[
            shape(length, jnp.bfloat16),
            shape(body, jnp.bfloat16),
            shape(body, jnp.bfloat16),
            shape(REACH, jnp.float32),
            shape(REACH, jnp.float32),
            jax.ShapeDtypeStruct((2, REACH, width), jnp.bfloat16),
            jax.ShapeDtypeStruct((heads, 1, TABLE), jnp.float32),
        ],
        scratch_shapes=[
            pltpu.VMEM((length + REACH, head), jnp.bfloat16),
            pltpu.VMEM((length + REACH, head), jnp.bfloat16),
            pltpu.VMEM((length + REACH, head), jnp.float32),
            pltpu.VMEM((length + REACH, head), jnp.float32),
        ],
        cost_estimate=pl.CostEstimate(
            flops=10 * elements * head, bytes_accessed=14 * length * width, transcendentals=elements
        ),
    )(first, query, keys, values, prev, out_grad, table)
    return outs


def table_to_bias(summed, entries):
    near = summed[:, 1:entries][:, ::-1]
    far = summed[:, :1] + jnp.sum(summed[:, WINDOW:], axis=1, keepdims=True)
    return jnp.concatenate([near, far], axis=1)


def ring_columns(count):
    columns = 1
    while (2 * columns) ** 2 <= count:
        columns *= 2
    return columns


def ring_place(index, count):
    columns = ring_columns(count)
    rows = count // columns
    row, column = index // columns, index % columns
    above = rows - 1 - row
    across = jnp.where(above % 2 == 0, column - 1, columns - 1 - column)
    return jnp.where(column == 0, row, rows + above * (columns - 1) + across)


def ring_index(place, count):
    columns = ring_columns(count)
    rows = count // columns
    later = jnp.maximum(place - rows, 0)
    above, across = later // (columns - 1), later % (columns - 1)
    column = jnp.where(above % 2 == 0, 1 + across, columns - 1 - across)
    return jnp.where(place < rows, place * columns, (rows - 1 - above) * columns + column)


def ring_kernel(
    count,
    parts,
    whole_hbm,
    dq_hbm,
    dk_hbm,
    dv_hbm,
    dk_tail_ref,
    dv_tail_ref,
    back_ref,
    line_ref,
    wq_hbm,
    wk_hbm,
    wv_hbm,
    input_ref,
    oq_ref,
    ok_ref,
    ov_ref,
    line_out_ref,
    whole,
    grads,
    weights,
    after,
    sent,
    got,
    lines,
    pair_sent,
    pair_got,
    cross_sent,
    cross_got,
    kept,
    load_sem,
    back_send,
    back_recv,
    send_sem,
    recv_sem,
    line_send,
    line_recv,
    pair_send,
    pair_recv,
    cross_send,
    cross_recv,
):
    me = lax.axis_index("sp")
    seat = lax.axis_index("tp")
    core = lax.rem(seat, 2)
    row = seat // 2
    pairs = parts // 2
    partner = seat + 1 - 2 * core
    place = ring_place(me, count)
    length = whole.shape[0]
    body = length - REACH
    block = input_ref.shape[1]
    bands = length // REACH

    loads = [
        pltpu.make_async_copy(whole_hbm, whole, load_sem.at[0]),
        pltpu.make_async_copy(dq_hbm, grads.at[0], load_sem.at[1]),
        pltpu.make_async_copy(dk_hbm, grads.at[1, pl.ds(0, body)], load_sem.at[2]),
        pltpu.make_async_copy(dv_hbm, grads.at[2, pl.ds(0, body)], load_sem.at[3]),
        pltpu.make_async_copy(wq_hbm, weights.at[0], load_sem.at[4]),
        pltpu.make_async_copy(wk_hbm, weights.at[1], load_sem.at[5]),
        pltpu.make_async_copy(wv_hbm, weights.at[2], load_sem.at[6]),
    ]
    for load in loads:
        load.start()

    barrier = pltpu.get_barrier_semaphore()
    for ahead in range(1, count):
        peer = lax.rem(me + ahead, count)
        pl.semaphore_signal(
            barrier, inc=1, device_id={"sp": peer}, device_id_type=pl.DeviceIdType.MESH
        )
    for ahead in range(1, parts):
        peer = lax.rem(seat + ahead, parts)
        pl.semaphore_signal(
            barrier, inc=1, device_id={"tp": peer}, device_id_type=pl.DeviceIdType.MESH
        )
    pl.semaphore_wait(barrier, count + parts - 2)

    outs = (oq_ref, ok_ref, ov_ref)
    half = got.shape[3]
    onward = (
        ring_index(lax.rem(place + 1, count), count),
        ring_index(lax.rem(place + count - 1, count), count),
    )

    def remote(src, dst, send, recv, device):
        return pltpu.make_async_remote_copy(
            src_ref=src,
            dst_ref=dst,
            send_sem=send,
            recv_sem=recv,
            device_id=device,
            device_id_type=pl.DeviceIdType.MESH,
        )

    def own(target, side, chain):
        start = pl.multiple_of((2 * ring_index(target, count) + side) * half, half)
        return contract_rows(whole[:, pl.ds(start, half)], grads[chain])

    def target_of(step, side):
        if side == 0:
            return lax.rem(place - 1 - step + 2 * count, count)
        return lax.rem(place + 1 + step, count)

    def first_copy(side, chain):
        return remote(
            sent.at[side, chain],
            got.at[side, chain, 0],
            send_sem.at[side, chain, 0],
            recv_sem.at[side, chain, 0],
            {"sp": onward[side]},
        )

    def copy_of(step, side, chain):
        return remote(
            got.at[side, chain, step - 1],
            got.at[side, chain, step],
            send_sem.at[side, chain, step],
            recv_sem.at[side, chain, step],
            {"sp": onward[side]},
        )

    def received(step, side, chain):
        return remote(
            sent.at[side, chain],
            got.at[side, chain, step],
            send_sem.at[side, chain, step],
            recv_sem.at[side, chain, step],
            {"sp": onward[side]},
        )

    def line_copy(ahead):
        return remote(
            line_ref,
            lines.at[ahead - 1],
            line_send.at[ahead - 1],
            line_recv.at[ahead - 1],
            {"sp": lax.rem(me + ahead, count)},
        )

    def back_copy(which):
        return remote(
            back_ref.at[which],
            after.at[which],
            back_send.at[which],
            back_recv.at[which],
            {"sp": lax.rem(me + count - 1, count)},
        )

    def rows(band):
        return pl.ds(pl.multiple_of(band * REACH, REACH), REACH)

    def part(band, target):
        start = pl.multiple_of(target * block, block)
        term = contract_cols(grads[0, rows(band)], weights[0, pl.ds(start, block)])
        term += contract_cols(grads[1, rows(band)], weights[1, pl.ds(start, block)])
        return term + contract_cols(grads[2, rows(band)], weights[2, pl.ds(start, block)])

    def pair_copy(band, away):
        return remote(
            pair_sent.at[band, away],
            pair_got.at[band, away],
            pair_send.at[band, away],
            pair_recv.at[band, away],
            {"tp": partner},
        )

    def cross_copy(band, away):
        return remote(
            cross_sent.at[band, away - 1],
            cross_got.at[band, away - 1],
            cross_send.at[band, away - 1],
            cross_recv.at[band, away - 1],
            {"tp": lax.rem(seat + 2 * away, parts)},
        )

    def to_partner(band):
        for away in range(pairs):
            target = 2 * lax.rem(row + away, pairs) + 1 - core
            pair_sent[band, away] = part(band, target).astype(jnp.bfloat16)
            pair_copy(band, away).start()

    def across(band):
        for away in range(1, pairs):
            term = part(band, lax.rem(seat + 2 * away, parts))
            pair_copy(band, away).wait_recv()
            term = term + pair_got[band, away].astype(jnp.float32)
            cross_sent[band, away - 1] = term.astype(jnp.bfloat16)
            cross_copy(band, away).start()
        term = part(band, seat)
        pair_copy(band, 0).wait_recv()
        kept[band] = term + pair_got[band, 0].astype(jnp.float32)

    def finish(band):
        term = kept[band]
        for away in range(1, pairs):
            cross_copy(band, away).wait_recv()
            term = term + cross_got[band, away - 1].astype(jnp.float32)
        input_ref[rows(band)] = term.astype(jnp.bfloat16)

    def work(unit):
        band = unit // 2

        @pl.when(lax.rem(unit, 2) == 0)
        def _():
            to_partner(band)

        @pl.when(lax.rem(unit, 2) == 1)
        def _():
            across(band)

        @pl.when((lax.rem(unit, 2) == 1) & (unit > 2))
        def _():
            finish(band - 1)

    @pl.when(me > 0)
    def _():
        back_copy(0).start()
        back_copy(1).start()

    loads[0].wait()
    loads[1].wait()
    tails = (dk_tail_ref, dv_tail_ref)
    for chain in range(3):
        if chain > 0:
            which = chain - 1

            @pl.when(me < count - 1)
            def _():
                back_copy(which).wait_recv()

            @pl.when(me == count - 1)
            def _():
                after[which] = jnp.zeros_like(after[which])

            loads[1 + chain].wait()
            tail = tails[which][...] + after[which].astype(jnp.float32)
            grads[chain, body:] = tail.astype(jnp.bfloat16)
        for side in range(2):
            sent[side, chain] = own(target_of(0, side), side, chain).astype(jnp.bfloat16)
            first_copy(side, chain).start()
    for ahead in range(1, count):
        line_copy(ahead).start()
    for matrix in range(3):
        loads[4 + matrix].wait()

    units = 2 * bands
    chains = [(chain, side) for chain in range(3) for side in range(2)]

    @pl.loop(1, count - 1)
    def _(step):
        for chain, side in chains:
            part_of = own(target_of(step, side), side, chain)
            received(step - 1, side, chain).wait_recv()
            total = part_of + got[side, chain, step - 1].astype(jnp.float32)
            got[side, chain, step - 1] = total.astype(jnp.bfloat16)
            copy_of(step, side, chain).start()
            if (chain, side) == (1, 1):

                @pl.when(step <= units)
                def _():
                    work(step - 1)

    for unit in range(min(count - 2, units), units):
        work(unit)
    total = line_ref[...]
    for ahead in range(1, count):
        line_copy(ahead).wait()
        total = total + lines[ahead - 1]
    line_out_ref[...] = total
    for chain, side in chains:
        if (chain, side) == (2, 0):
            finish(bands - 1)
        part_of = own(place, side, chain)
        received(count - 2, side, chain).wait_recv()
        total = part_of + got[side, chain, count - 2].astype(jnp.float32)
        outs[chain][side * half : (side + 1) * half] = total

    @pl.when(me > 0)
    def _():
        back_copy(0).wait_send()
        back_copy(1).wait_send()

    @pl.loop(0, count - 1)
    def _(step):
        for chain, side in chains:
            received(step, side, chain).wait_send()

    @pl.loop(0, bands)
    def _(band):
        for away in range(pairs):
            pair_copy(band, away).wait_send()
        for away in range(1, pairs):
            cross_copy(band, away).wait_send()


def final_grads(whole, grads, tails, back, lines, weights):
    count = lax.axis_size("sp")
    parts = lax.axis_size("tp")
    pairs = parts // 2
    length, features = whole.shape
    width = weights[0].shape[1]
    half = features // count // 2
    block = features // parts
    bands = length // REACH
    vmem = pl.BlockSpec(memory_space=pltpu.VMEM)
    anywhere = pl.BlockSpec(memory_space=pl.ANY)
    out = jax.ShapeDtypeStruct((2 * half, width), jnp.float32)
    dma = pltpu.SemaphoreType.DMA
    low = jnp.bfloat16
    return pl.pallas_call(
        functools.partial(ring_kernel, count, parts),
        in_specs=[anywhere] * 4 + [vmem] * 4 + [anywhere] * 3,
        out_specs=[vmem] * 5,
        out_shape=[
            jax.ShapeDtypeStruct((length, block), low),
            out,
            out,
            out,
            jax.ShapeDtypeStruct(lines.shape, jnp.float32),
        ],
        scratch_shapes=[
            pltpu.VMEM((length, features), low),
            pltpu.VMEM((3, length, width), low),
            pltpu.VMEM((3, features, width), low),
            pltpu.VMEM((2, REACH, width), low),
            pltpu.VMEM((2, 3, half, width), low),
            pltpu.VMEM((2, 3, count - 1, half, width), low),
            pltpu.VMEM((count - 1,) + lines.shape, jnp.float32),
            pltpu.VMEM((bands, pairs, REACH, block), low),
            pltpu.VMEM((bands, pairs, REACH, block), low),
            pltpu.VMEM((bands, pairs - 1, REACH, block), low),
            pltpu.VMEM((bands, pairs - 1, REACH, block), low),
            pltpu.VMEM((bands, REACH, block), jnp.float32),
            dma((7,)),
            dma((2,)),
            dma((2,)),
            dma((2, 3, count - 1)),
            dma((2, 3, count - 1)),
            dma((count - 1,)),
            dma((count - 1,)),
            dma((bands, pairs)),
            dma((bands, pairs)),
            dma((bands, pairs - 1)),
            dma((bands, pairs - 1)),
        ],
        compiler_params=pltpu.CompilerParams(
            collective_id=0, has_side_effects=True, vmem_limit_bytes=63 * 1024 * 1024
        ),
        cost_estimate=pl.CostEstimate(
            flops=12 * length * features * width,
            bytes_accessed=400_000_000,
            transcendentals=0,
        ),
    )(whole, *grads, *tails, back, lines, *weights)


def gather_kernel(
    parts,
    tokens_ref,
    wq_ref,
    wk_ref,
    wv_ref,
    whole_ref,
    q_ref,
    k_ref,
    v_ref,
    prev_ref,
    held,
    weights,
    total,
    halo,
    halo_got,
    side_send,
    side_recv,
    far_send,
    far_recv,
    relay_send,
    relay_recv,
    halo_send,
    halo_recv,
    load_sem,
    store_sem,
):
    me = lax.axis_index("tp")
    seat = lax.axis_index("sp")
    seats = lax.axis_size("sp")
    partner = me + 1 - 2 * lax.rem(me, 2)
    chunks = held.shape[0]
    block = tokens_ref.shape[1]
    width = q_ref.shape[1]
    pairs = parts // 2
    matrices = (wq_ref, wk_ref, wv_ref)

    def source(device, away):
        return lax.rem(device + parts - 2 * away, parts)

    order = [me, partner]
    for away in range(1, pairs):
        order += [source(me, away), source(partner, away)]

    def load(slot, matrix):
        start = pl.multiple_of(order[slot] * block, block)
        return pltpu.make_async_copy(
            matrices[matrix].at[pl.ds(start, block)],
            weights.at[slot, matrix],
            load_sem.at[slot, matrix],
        )

    for slot in range(parts):
        for matrix in range(3):
            load(slot, matrix).start()

    barrier = pltpu.get_barrier_semaphore()
    for ahead in range(1, parts):
        pl.semaphore_signal(
            barrier,
            inc=1,
            device_id={"tp": lax.rem(me + ahead, parts)},
            device_id_type=pl.DeviceIdType.MESH,
        )
    onward = lax.rem(seat + 1, seats)
    for other in (onward, lax.rem(seat + seats - 1, seats)):
        pl.semaphore_signal(
            barrier, inc=1, device_id={"sp": other}, device_id_type=pl.DeviceIdType.MESH
        )
    pl.semaphore_wait(barrier, parts + 1)

    def rows(chunk):
        return pl.ds(chunk * REACH, REACH)

    def remote(src, dst, send, recv, device):
        return pltpu.make_async_remote_copy(
            src_ref=src,
            dst_ref=dst,
            send_sem=send,
            recv_sem=recv,
            device_id=device,
            device_id_type=pl.DeviceIdType.MESH,
        )

    def far(chunk, away):
        return remote(
            tokens_ref.at[rows(chunk)],
            held.at[chunk, me],
            far_send.at[chunk, away - 1],
            far_recv.at[chunk, away - 1],
            {"tp": lax.rem(me + 2 * away, parts)},
        )

    def side(chunk):
        return remote(
            tokens_ref.at[rows(chunk)],
            held.at[chunk, me],
            side_send.at[chunk],
            side_recv.at[chunk],
            {"tp": partner},
        )

    def relay(chunk, away):
        place = held.at[chunk, source(me, away)]
        return remote(
            place,
            place,
            relay_send.at[chunk, away - 1],
            relay_recv.at[chunk, away - 1],
            {"tp": partner},
        )

    def neighbour():
        return remote(halo, halo_got, halo_send, halo_recv, {"sp": onward})

    def store(chunk, slot):
        start = pl.multiple_of(order[slot] * block, block)
        src = tokens_ref.at[rows(chunk)] if slot == 0 else held.at[chunk, order[slot]]
        return pltpu.make_async_copy(
            src, whole_ref.at[rows(chunk), pl.ds(start, block)], store_sem.at[chunk, slot]
        )

    def add(chunk, slot, value):
        for matrix in range(3):
            term = jnp.dot(value, weights[slot, matrix], preferred_element_type=jnp.float32)
            if slot == 0:
                total[matrix, chunk] = term
            else:
                total[matrix, chunk] += term

    backwards = list(range(chunks))[::-1]
    for chunk in backwards:
        for away in range(1, pairs):
            far(chunk, away).start()
        side(chunk).start()
    for slot in range(2):
        for matrix in range(3):
            load(slot, matrix).wait()
        for chunk in backwards:
            if slot == 1:
                side(chunk).wait_recv()
            store(chunk, slot).start()
            value = tokens_ref[rows(chunk)] if slot == 0 else held[chunk, partner]
            add(chunk, slot, value)
    for slot in range(2, parts):
        for matrix in range(3):
            load(slot, matrix).wait()
    outs = (q_ref, k_ref, v_ref)
    for chunk in backwards:
        for away in range(1, pairs):
            far(chunk, away).wait_recv()
            relay(chunk, away).start()
            store(chunk, 2 * away).start()
            add(chunk, 2 * away, held[chunk, source(me, away)])
        for away in range(1, pairs):
            relay(chunk, away).wait_recv()
            store(chunk, 2 * away + 1).start()
            add(chunk, 2 * away + 1, held[chunk, source(partner, away)])
        for matrix in range(3):
            outs[matrix][rows(chunk)] = total[matrix, chunk].astype(jnp.bfloat16)
        if chunk == chunks - 1:
            halo[0] = total[1, chunk].astype(jnp.bfloat16)
            halo[1] = total[2, chunk].astype(jnp.bfloat16)
            neighbour().start()
    neighbour().wait()
    prev_ref[...] = halo_got[...]
    for chunk in backwards:
        side(chunk).wait_send()
        for away in range(1, pairs):
            far(chunk, away).wait_send()
            relay(chunk, away).wait_send()
        for slot in range(parts):
            store(chunk, slot).wait()


def project(tokens, query_weight, key_weight, value_weight):
    parts = lax.axis_size("tp")
    length, block = tokens.shape
    width = query_weight.shape[1]
    chunks = length // REACH
    pairs = parts // 2
    vmem = pl.BlockSpec(memory_space=pltpu.VMEM)
    anywhere = pl.BlockSpec(memory_space=pl.ANY)
    narrow = jax.ShapeDtypeStruct((length, width), jnp.bfloat16)
    dma = pltpu.SemaphoreType.DMA
    return pl.pallas_call(
        functools.partial(gather_kernel, parts),
        in_specs=[vmem, anywhere, anywhere, anywhere],
        out_specs=[anywhere, vmem, vmem, vmem, vmem],
        out_shape=[
            jax.ShapeDtypeStruct((length, block * parts), jnp.bfloat16),
            narrow,
            narrow,
            narrow,
            jax.ShapeDtypeStruct((2, REACH, width), jnp.bfloat16),
        ],
        scratch_shapes=[
            pltpu.VMEM((chunks, parts, REACH, block), jnp.bfloat16),
            pltpu.VMEM((parts, 3, block, width), jnp.bfloat16),
            pltpu.VMEM((3, chunks, REACH, width), jnp.float32),
            pltpu.VMEM((2, REACH, width), jnp.bfloat16),
            pltpu.VMEM((2, REACH, width), jnp.bfloat16),
            dma((chunks,)),
            dma((chunks,)),
            dma((chunks, pairs - 1)),
            dma((chunks, pairs - 1)),
            dma((chunks, pairs - 1)),
            dma((chunks, pairs - 1)),
            dma(()),
            dma(()),
            dma((parts, 3)),
            dma((chunks, parts)),
        ],
        compiler_params=pltpu.CompilerParams(
            collective_id=1, has_side_effects=True, vmem_limit_bytes=56 * 1024 * 1024
        ),
        cost_estimate=pl.CostEstimate(
            flops=6 * length * block * parts * width, bytes_accessed=150_000_000, transcendentals=0
        ),
    )(tokens, query_weight, key_weight, value_weight)


def shards(tokens, query_weight, key_weight, value_weight, position_bias, out_grad):
    whole, query, keys, values, prev = project(tokens, query_weight, key_weight, value_weight)
    query_grad, key_body, value_body, key_tail, value_tail, back, lines = attention(
        query, keys, values, prev, out_grad, position_bias
    )
    input_grad, query_weight_grad, key_weight_grad, value_weight_grad, lines = final_grads(
        whole,
        (query_grad, key_body, value_body),
        (key_tail, value_tail),
        back,
        lines[:, 0],
        (query_weight, key_weight, value_weight),
    )
    bias_grad = table_to_bias(lines, position_bias.shape[1])
    return input_grad, query_weight_grad, key_weight_grad, value_weight_grad, bias_grad


def solution(mesh):
    in_specs = (
        P("sp", "tp"),
        P(None, "tp"),
        P(None, "tp"),
        P(None, "tp"),
        P("tp", None),
        P("sp", "tp"),
    )
    out_specs = (P("sp", "tp"), P("sp", "tp"), P("sp", "tp"), P("sp", "tp"), P("tp", None))
    return jax.shard_map(shards, mesh=mesh, in_specs=in_specs, out_specs=out_specs, check_vma=False)
```

```python
import functools

import jax
import jax.numpy as jnp
from jax import lax
from jax.experimental import pallas as pl
from jax.experimental.pallas import tpu as pltpu
from jax.sharding import PartitionSpec as P

SEGMENT = 64
PREVIOUS = 4
CLIP = 256
ROWS = 2 * SEGMENT
REACH = PREVIOUS * SEGMENT
WINDOW = ROWS + REACH
TABLE = 512
LANES = 128
HIDDEN = -1e30


def contract_rows(left, right):
    return lax.dot_general(
        left, right, (((0,), (0,)), ((), ())), preferred_element_type=jnp.float32
    )


def contract_cols(left, right):
    return lax.dot_general(
        left, right, (((1,), (1,)), ((), ())), preferred_element_type=jnp.float32
    )


def diagonal_sums(tile):
    half = tile.shape[0] // 2
    while half >= 8:
        tile = tile[:half] + pltpu.roll(tile[half:], TABLE - half, 1)
        half //= 2
    row = lax.broadcasted_iota(jnp.int32, tile.shape, 0)
    for step in (4, 2, 1):
        tile = jnp.where((row & step) != 0, pltpu.roll(tile, TABLE - step, 1), tile)
    return jnp.sum(tile, axis=0, keepdims=True)


def attention_kernel(
    factor,
    first_ref,
    q_ref,
    k_ref,
    v_ref,
    prev_ref,
    g_ref,
    table_ref,
    dq_ref,
    dk_ref,
    dv_ref,
    dk_tail_ref,
    dv_tail_ref,
    back_ref,
    table_grad_ref,
    k_all,
    v_all,
    dk_all,
    dv_all,
):
    length = q_ref.shape[0]
    k_all[:REACH] = prev_ref[0]
    k_all[REACH:] = k_ref[...]
    v_all[:REACH] = prev_ref[1]
    v_all[REACH:] = v_ref[...]
    dk_all[...] = jnp.zeros_like(dk_all)
    dv_all[...] = jnp.zeros_like(dv_all)
    first = first_ref[0]
    table = jnp.broadcast_to(table_ref[0], (ROWS, TABLE))
    bias = pltpu.roll(table, 0, 1, stride=1, stride_axis=0)[:, :WINDOW]
    row = lax.broadcasted_iota(jnp.int32, (ROWS, WINDOW), 0) // SEGMENT
    column = lax.broadcasted_iota(jnp.int32, (ROWS, WINDOW), 1)
    behind = column // SEGMENT - row
    bias = jnp.where((behind >= 0) & (behind <= PREVIOUS), bias, HIDDEN)
    bias_sum = jnp.zeros((ROWS, WINDOW), jnp.float32)
    for start in range(0, length, ROWS):
        q = q_ref[start : start + ROWS]
        g = g_ref[start : start + ROWS]
        k = k_all[start : start + WINDOW]
        v = v_all[start : start + WINDOW]
        mask = bias
        if start < REACH:
            mask = jnp.where(column + start < first, HIDDEN, bias)
        scores = contract_cols(q, k) * factor + mask
        top = jnp.max(scores, axis=1, keepdims=True)
        raised = jnp.exp(scores - top)
        weights = raised * (1.0 / jnp.sum(raised, axis=1, keepdims=True))
        prob_grad = contract_cols(g, v)
        delta = jnp.sum(weights * prob_grad, axis=1, keepdims=True)
        score_grad = weights * (prob_grad - delta)
        bias_sum = bias_sum + score_grad
        low = score_grad.astype(jnp.bfloat16)
        dq = jnp.dot(low, k, preferred_element_type=jnp.float32) * factor
        dq_ref[start : start + ROWS] = dq.astype(jnp.bfloat16)
        dk_all[start : start + WINDOW] += contract_rows(low, q)
        dv_all[start : start + WINDOW] += contract_rows(weights.astype(jnp.bfloat16), g)
    back_ref[0] = (dk_all[:REACH] * factor).astype(jnp.bfloat16)
    back_ref[1] = dv_all[:REACH].astype(jnp.bfloat16)
    dk_ref[...] = (dk_all[REACH:length] * factor).astype(jnp.bfloat16)
    dv_ref[...] = dv_all[REACH:length].astype(jnp.bfloat16)
    dk_tail_ref[...] = dk_all[length:] * factor
    dv_tail_ref[...] = dv_all[length:]
    padded = jnp.concatenate([bias_sum, jnp.zeros((ROWS, TABLE - WINDOW), jnp.float32)], axis=1)
    table_grad_ref[0] = diagonal_sums(padded)


def attention(query, keys, values, prev, out_grad, position_bias):
    length, width = query.shape
    heads, entries = position_bias.shape
    head = width // heads
    factor = head ** (-0.5)
    table = jnp.concatenate(
        [
            position_bias[:, ::-1],
            jnp.zeros((heads, WINDOW - entries), jnp.float32),
            jnp.broadcast_to(position_bias[:, entries - 1 :], (heads, TABLE - WINDOW)),
        ],
        axis=1,
    )[:, None]
    first = jnp.where(lax.axis_index("sp") == 0, REACH, 0).astype(jnp.int32)[None]

    def rows(count):
        return pl.BlockSpec((count, head), lambda h: (0, h))

    line = pl.BlockSpec((1, 1, TABLE), lambda h: (h, 0, 0))

    def shape(count, kind):
        return jax.ShapeDtypeStruct((count, width), kind)

    body = length - REACH
    elements = heads * length * WINDOW
    outs = pl.pallas_call(
        functools.partial(attention_kernel, factor),
        grid=(heads,),
        in_specs=[
            pl.BlockSpec(memory_space=pltpu.SMEM),
            rows(length),
            rows(length),
            rows(length),
            pl.BlockSpec((2, REACH, head), lambda h: (0, 0, h)),
            rows(length),
            line,
        ],
        out_specs=[
            rows(length),
            rows(body),
            rows(body),
            rows(REACH),
            rows(REACH),
            pl.BlockSpec((2, REACH, head), lambda h: (0, 0, h)),
            line,
        ],
        out_shape=[
            shape(length, jnp.bfloat16),
            shape(body, jnp.bfloat16),
            shape(body, jnp.bfloat16),
            shape(REACH, jnp.float32),
            shape(REACH, jnp.float32),
            jax.ShapeDtypeStruct((2, REACH, width), jnp.bfloat16),
            jax.ShapeDtypeStruct((heads, 1, TABLE), jnp.float32),
        ],
        scratch_shapes=[
            pltpu.VMEM((length + REACH, head), jnp.bfloat16),
            pltpu.VMEM((length + REACH, head), jnp.bfloat16),
            pltpu.VMEM((length + REACH, head), jnp.float32),
            pltpu.VMEM((length + REACH, head), jnp.float32),
        ],
        cost_estimate=pl.CostEstimate(
            flops=10 * elements * head, bytes_accessed=14 * length * width, transcendentals=elements
        ),
    )(first, query, keys, values, prev, out_grad, table)
    return outs


def table_to_bias(summed, entries):
    near = summed[:, 1:entries][:, ::-1]
    far = summed[:, :1] + jnp.sum(summed[:, WINDOW:], axis=1, keepdims=True)
    return jnp.concatenate([near, far], axis=1)


def ring_columns(count):
    columns = 1
    while (2 * columns) ** 2 <= count:
        columns *= 2
    return columns


def ring_place(index, count):
    columns = ring_columns(count)
    rows = count // columns
    row, column = index // columns, index % columns
    above = rows - 1 - row
    across = jnp.where(above % 2 == 0, column - 1, columns - 1 - column)
    return jnp.where(column == 0, row, rows + above * (columns - 1) + across)


def ring_index(place, count):
    columns = ring_columns(count)
    rows = count // columns
    later = jnp.maximum(place - rows, 0)
    above, across = later // (columns - 1), later % (columns - 1)
    column = jnp.where(above % 2 == 0, 1 + across, columns - 1 - across)
    return jnp.where(place < rows, place * columns, (rows - 1 - above) * columns + column)


def remote(src, dst, send, recv, device):
    return pltpu.make_async_remote_copy(
        src_ref=src,
        dst_ref=dst,
        send_sem=send,
        recv_sem=recv,
        device_id=device,
        device_id_type=pl.DeviceIdType.MESH,
    )


def meet(count, parts):
    me = lax.axis_index("sp")
    seat = lax.axis_index("tp")
    barrier = pltpu.get_barrier_semaphore()
    for ahead in range(1, count):
        peer = lax.rem(me + ahead, count)
        pl.semaphore_signal(
            barrier, inc=1, device_id={"sp": peer}, device_id_type=pl.DeviceIdType.MESH
        )
    for ahead in range(1, parts):
        peer = lax.rem(seat + ahead, parts)
        pl.semaphore_signal(
            barrier, inc=1, device_id={"tp": peer}, device_id_type=pl.DeviceIdType.MESH
        )
    pl.semaphore_wait(barrier, count + parts - 2)


def final_loads(hbm, whole, grads, weights, load_sem):
    whole_hbm, dq_hbm, dk_hbm, dv_hbm, wq_hbm, wk_hbm, wv_hbm = hbm
    body = whole.shape[0] - REACH
    return [
        pltpu.make_async_copy(dq_hbm, grads.at[0], load_sem.at[0]),
        pltpu.make_async_copy(dk_hbm, grads.at[1, pl.ds(0, body)], load_sem.at[1]),
        pltpu.make_async_copy(dv_hbm, grads.at[2, pl.ds(0, body)], load_sem.at[2]),
        pltpu.make_async_copy(whole_hbm, whole, load_sem.at[3]),
        pltpu.make_async_copy(wq_hbm, weights.at[0], load_sem.at[4]),
        pltpu.make_async_copy(wk_hbm, weights.at[1], load_sem.at[5]),
        pltpu.make_async_copy(wv_hbm, weights.at[2], load_sem.at[6]),
    ]


class Halo:
    def __init__(self, count, grads, tails, back_ref, after, send, recv):
        self.me = lax.axis_index("sp")
        self.count = count
        self.grads, self.tails = grads, tails
        self.back_ref, self.after, self.sems = back_ref, after, (send, recv)

    def copy(self, which):
        return remote(
            self.back_ref.at[which],
            self.after.at[which],
            self.sems[0].at[which],
            self.sems[1].at[which],
            {"sp": lax.rem(self.me + self.count - 1, self.count)},
        )

    def start(self):
        @pl.when(self.me > 0)
        def _():
            self.copy(0).start()
            self.copy(1).start()

    def join(self, which):
        after = self.after

        @pl.when(self.me < self.count - 1)
        def _():
            self.copy(which).wait_recv()

        @pl.when(self.me == self.count - 1)
        def _():
            after[which] = jnp.zeros_like(after[which])

        tail = self.tails[which][...] + after[which].astype(jnp.float32)
        body = self.grads.shape[1] - REACH
        self.grads[1 + which, body:] = tail.astype(jnp.bfloat16)

    def drain(self):
        @pl.when(self.me > 0)
        def _():
            self.copy(0).wait_send()
            self.copy(1).wait_send()


class Lines:
    def __init__(self, count, line_ref, out_ref, lines, send, recv):
        self.me = lax.axis_index("sp")
        self.count = count
        self.line_ref, self.out_ref, self.lines = line_ref, out_ref, lines
        self.sems = (send, recv)

    def copy(self, ahead):
        return remote(
            self.line_ref,
            self.lines.at[ahead - 1],
            self.sems[0].at[ahead - 1],
            self.sems[1].at[ahead - 1],
            {"sp": lax.rem(self.me + ahead, self.count)},
        )

    def start(self):
        for ahead in range(1, self.count):
            self.copy(ahead).start()

    def finish(self):
        total = self.line_ref[...]
        for ahead in range(1, self.count):
            self.copy(ahead).wait()
            total = total + self.lines[ahead - 1]
        self.out_ref[...] = total


class InputGrad:
    def __init__(self, parts, grads, weights, input_ref, buffers, sems):
        self.seat = lax.axis_index("tp")
        self.core = lax.rem(self.seat, 2)
        self.row = self.seat // 2
        self.parts, self.pairs = parts, parts // 2
        self.grads, self.weights, self.input_ref = grads, weights, input_ref
        self.pair_sent, self.pair_got, self.cross_sent, self.cross_got, self.kept = buffers
        self.sems = sems
        self.block = input_ref.shape[1]
        self.bands = input_ref.shape[0] // REACH
        self.units = 2 * self.bands

    def rows(self, band):
        return pl.ds(pl.multiple_of(band * REACH, REACH), REACH)

    def part(self, band, target):
        block = pl.ds(pl.multiple_of(target * self.block, self.block), self.block)
        rows = self.rows(band)
        term = contract_cols(self.grads[0, rows], self.weights[0, block])
        term += contract_cols(self.grads[1, rows], self.weights[1, block])
        return term + contract_cols(self.grads[2, rows], self.weights[2, block])

    def pair_copy(self, band, away):
        return remote(
            self.pair_sent.at[band, away],
            self.pair_got.at[band, away],
            self.sems[0].at[band, away],
            self.sems[1].at[band, away],
            {"tp": self.seat + 1 - 2 * self.core},
        )

    def cross_copy(self, band, away):
        return remote(
            self.cross_sent.at[band, away - 1],
            self.cross_got.at[band, away - 1],
            self.sems[2].at[band, away - 1],
            self.sems[3].at[band, away - 1],
            {"tp": lax.rem(self.seat + 2 * away, self.parts)},
        )

    def to_partner(self, band):
        for away in range(self.pairs):
            target = 2 * lax.rem(self.row + away, self.pairs) + 1 - self.core
            self.pair_sent[band, away] = self.part(band, target).astype(jnp.bfloat16)
            self.pair_copy(band, away).start()

    def across(self, band):
        for away in range(1, self.pairs):
            term = self.part(band, lax.rem(self.seat + 2 * away, self.parts))
            self.pair_copy(band, away).wait_recv()
            term = term + self.pair_got[band, away].astype(jnp.float32)
            self.cross_sent[band, away - 1] = term.astype(jnp.bfloat16)
            self.cross_copy(band, away).start()
        term = self.part(band, self.seat)
        self.pair_copy(band, 0).wait_recv()
        self.kept[band] = term + self.pair_got[band, 0].astype(jnp.float32)

    def finish(self, band):
        term = self.kept[band]
        for away in range(1, self.pairs):
            self.cross_copy(band, away).wait_recv()
            term = term + self.cross_got[band, away - 1].astype(jnp.float32)
        self.input_ref[self.rows(band)] = term.astype(jnp.bfloat16)

    def work(self, unit):
        band = unit // 2

        @pl.when(lax.rem(unit, 2) == 0)
        def _():
            self.to_partner(band)

        @pl.when(lax.rem(unit, 2) == 1)
        def _():
            self.across(band)

        @pl.when((lax.rem(unit, 2) == 1) & (unit > 2))
        def _():
            self.finish(band - 1)

    def drain(self):
        @pl.loop(0, self.bands)
        def _(band):
            for away in range(self.pairs):
                self.pair_copy(band, away).wait_send()
            for away in range(1, self.pairs):
                self.cross_copy(band, away).wait_send()


def ring_kernel(
    count,
    parts,
    whole_hbm,
    dq_hbm,
    dk_hbm,
    dv_hbm,
    wq_hbm,
    wk_hbm,
    wv_hbm,
    dk_tail_ref,
    dv_tail_ref,
    back_ref,
    line_ref,
    input_ref,
    oq_ref,
    ok_ref,
    ov_ref,
    line_out_ref,
    whole,
    grads,
    weights,
    after,
    lines,
    pair_sent,
    pair_got,
    cross_sent,
    cross_got,
    kept,
    load_sem,
    back_send,
    back_recv,
    line_send,
    line_recv,
    pair_send,
    pair_recv,
    cross_send,
    cross_recv,
    sent,
    got,
    send_sem,
    recv_sem,
):
    me = lax.axis_index("sp")
    place = ring_place(me, count)
    hbm = (whole_hbm, dq_hbm, dk_hbm, dv_hbm, wq_hbm, wk_hbm, wv_hbm)
    loads = final_loads(hbm, whole, grads, weights, load_sem)
    for load in loads:
        load.start()
    meet(count, parts)
    halo = Halo(
        count, grads, (dk_tail_ref, dv_tail_ref), back_ref, after, back_send, back_recv
    )
    shared = Lines(count, line_ref, line_out_ref, lines, line_send, line_recv)
    buffers = (pair_sent, pair_got, cross_sent, cross_got, kept)
    sems = (pair_send, pair_recv, cross_send, cross_recv)
    grad_in = InputGrad(parts, grads, weights, input_ref, buffers, sems)

    outs = (oq_ref, ok_ref, ov_ref)
    half = got.shape[3]
    onward = (
        ring_index(lax.rem(place + 1, count), count),
        ring_index(lax.rem(place + count - 1, count), count),
    )

    def own(target, side, chain):
        start = pl.multiple_of((2 * ring_index(target, count) + side) * half, half)
        return contract_rows(whole[:, pl.ds(start, half)], grads[chain])

    def target_of(step, side):
        if side == 0:
            return lax.rem(place - 1 - step + 2 * count, count)
        return lax.rem(place + 1 + step, count)

    def copy_of(src, step, side, chain):
        return remote(
            src,
            got.at[side, chain, step],
            send_sem.at[side, chain, step],
            recv_sem.at[side, chain, step],
            {"sp": onward[side]},
        )

    halo.start()
    for load in loads:
        load.wait()
    for chain in range(3):
        if chain > 0:
            halo.join(chain - 1)
        for side in range(2):
            sent[side, chain] = own(target_of(0, side), side, chain).astype(jnp.bfloat16)
            copy_of(sent.at[side, chain], 0, side, chain).start()
    shared.start()

    chains = [(chain, side) for chain in range(3) for side in range(2)]

    @pl.loop(1, count - 1)
    def _(step):
        for chain, side in chains:
            part_of = own(target_of(step, side), side, chain)
            place_of = got.at[side, chain, step - 1]
            copy_of(sent.at[side, chain], step - 1, side, chain).wait_recv()
            total = part_of + place_of[...].astype(jnp.float32)
            place_of[...] = total.astype(jnp.bfloat16)
            copy_of(place_of, step, side, chain).start()
            if (chain, side) == (1, 1):

                @pl.when(step <= grad_in.units)
                def _():
                    grad_in.work(step - 1)

    for unit in range(min(count - 2, grad_in.units), grad_in.units):
        grad_in.work(unit)
    shared.finish()
    for chain, side in chains:
        if (chain, side) == (2, 0):
            grad_in.finish(grad_in.bands - 1)
        part_of = own(place, side, chain)
        copy_of(sent.at[side, chain], count - 2, side, chain).wait_recv()
        total = part_of + got[side, chain, count - 2].astype(jnp.float32)
        outs[chain][side * half : (side + 1) * half] = total

    halo.drain()

    @pl.loop(0, count - 1)
    def _(step):
        for chain, side in chains:
            copy_of(sent.at[side, chain], step, side, chain).wait_send()

    grad_in.drain()


def paired(count, parts):
    return count == 8 and ring_columns(count) == 2 and parts == 4


def pair_places(me):
    level, side = me // 2, lax.rem(me, 2)
    inner = (level == 1) | (level == 2)
    near = level // 2
    made = jnp.where(inner, 1 - near, near)
    partner = 2 * (level + 1 - 2 * lax.rem(level, 2)) + side
    return level, side, inner, near, made, partner


def pair_kernel(
    count,
    parts,
    whole_hbm,
    dq_hbm,
    dk_hbm,
    dv_hbm,
    wq_hbm,
    wk_hbm,
    wv_hbm,
    theirs_hbm,
    dk_tail_ref,
    dv_tail_ref,
    back_ref,
    line_ref,
    input_ref,
    oq_ref,
    ok_ref,
    ov_ref,
    line_out_ref,
    whole,
    grads,
    weights,
    after,
    lines,
    pair_sent,
    pair_got,
    cross_sent,
    cross_got,
    kept,
    load_sem,
    back_send,
    back_recv,
    line_send,
    line_recv,
    pair_send,
    pair_recv,
    cross_send,
    cross_recv,
    theirs,
    their_grads,
    x_sent,
    x_got,
    sent,
    got,
    result,
    theirs_sem,
    swap_send,
    swap_recv,
    x_send,
    x_recv,
    send_sem,
    recv_sem,
    out_sem,
):
    me = lax.axis_index("sp")
    level, side, inner, near, made, partner = pair_places(me)
    hbm = (whole_hbm, dq_hbm, dk_hbm, dv_hbm, wq_hbm, wk_hbm, wv_hbm)
    loads = final_loads(hbm, whole, grads, weights, load_sem)
    loads.insert(4, pltpu.make_async_copy(theirs_hbm, theirs, theirs_sem.at[0]))
    for load in loads:
        load.start()
    meet(count, parts)
    halo = Halo(
        count, grads, (dk_tail_ref, dv_tail_ref), back_ref, after, back_send, back_recv
    )
    shared = Lines(count, line_ref, line_out_ref, lines, line_send, line_recv)
    buffers = (pair_sent, pair_got, cross_sent, cross_got, kept)
    sems = (pair_send, pair_recv, cross_send, cross_recv)
    grad_in = InputGrad(parts, grads, weights, input_ref, buffers, sems)

    chunks, depth, tile = x_sent.shape[0], x_sent.shape[2], x_sent.shape[3]
    per = chunks // 3
    outs = (oq_ref, ok_ref, ov_ref)
    deep = 2 * (1 + made)
    rim = 6 * made
    slot = jnp.where(inner, 0, 1)

    def columns(chunk):
        return pl.ds(pl.multiple_of(lax.rem(chunk, per) * tile, tile), tile)

    def swap(chunk):
        return remote(
            grads.at[chunk // per, :, columns(chunk)],
            their_grads.at[chunk // per, :, columns(chunk)],
            swap_send.at[chunk],
            swap_recv.at[chunk],
            {"sp": partner},
        )

    def x_copy(chunk):
        return remote(
            x_sent.at[chunk],
            x_got.at[chunk],
            x_send.at[chunk],
            x_recv.at[chunk],
            {"sp": 2 * level + 1 - side},
        )

    def deep_copy(chunk):
        return remote(
            sent.at[0, chunk],
            got.at[slot, chunk],
            send_sem.at[0, chunk],
            recv_sem.at[slot, chunk],
            {"sp": deep + side},
        )

    def rim_copy(chunk):
        return remote(
            sent.at[1, chunk],
            got.at[0, chunk],
            send_sem.at[1, chunk],
            recv_sem.at[0, chunk],
            {"sp": rim + side},
        )

    def arrived(chunk, which):
        return remote(
            sent.at[0, chunk],
            got.at[which, chunk],
            send_sem.at[0, chunk],
            recv_sem.at[which, chunk],
            {"sp": deep + side},
        )

    def sums(target, chunk):
        start = pl.multiple_of(target * depth, depth)
        mine = whole[:, pl.ds(start, depth)]
        start = pl.multiple_of((target - made * (count // 2)) * depth, depth)
        their = theirs[:, pl.ds(start, depth)]
        term = contract_rows(mine, grads[chunk // per, :, columns(chunk)])
        return term + contract_rows(their, their_grads[chunk // per, :, columns(chunk)])

    def halve(chunk):
        swap(chunk).wait_recv()
        x_sent[chunk, 0] = sums(deep + 1 - side, chunk).astype(jnp.bfloat16)
        x_sent[chunk, 1] = sums(rim + 1 - side, chunk).astype(jnp.bfloat16)
        x_copy(chunk).start()

    def onward(chunk):
        term = sums(deep + side, chunk)
        x_copy(chunk).wait_recv()
        term = term + x_got[chunk, 0].astype(jnp.float32)
        sent[0, chunk] = term.astype(jnp.bfloat16)
        deep_copy(chunk).start()
        term = sums(rim + side, chunk) + x_got[chunk, 1].astype(jnp.float32)

        @pl.when(inner)
        def _():
            sent[1, chunk] = term.astype(jnp.bfloat16)
            rim_copy(chunk).start()

        @pl.when(jnp.logical_not(inner))
        def _():
            result[chunk // per, :, columns(chunk)] = term

    def store(chunk, matrix):
        return pltpu.make_async_copy(
            result.at[matrix, :, columns(chunk)],
            outs[matrix].at[:, columns(chunk)],
            out_sem.at[chunk],
        )

    def finish(chunk):
        arrived(chunk, 0).wait_recv()
        term = got[0, chunk].astype(jnp.float32)

        @pl.when(inner)
        def _():
            arrived(chunk, 1).wait_recv()
            total = term + got[1, chunk].astype(jnp.float32)
            result[chunk // per, :, columns(chunk)] = total

        @pl.when(jnp.logical_not(inner))
        def _():
            total = term + result[chunk // per, :, columns(chunk)]
            result[chunk // per, :, columns(chunk)] = total

        for matrix in range(3):

            @pl.when(chunk // per == matrix)
            def _():
                store(chunk, matrix).start()

    halo.start()
    loads[0].wait()
    for chunk in range(per):
        swap(chunk).start()
    for which in range(2):
        loads[1 + which].wait()
        halo.join(which)
        for chunk in range(per):
            swap((1 + which) * per + chunk).start()
    for load in loads[3:]:
        load.wait()
    shared.start()

    lag = 3

    @pl.loop(0, chunks + lag)
    def _(step):
        @pl.when(step < chunks)
        def _():
            halve(step)

        @pl.when((step > 0) & (step <= chunks))
        def _():
            onward(step - 1)

        @pl.when(step >= lag)
        def _():
            finish(step - lag)

        unit = (step - 1) // 2

        @pl.when((lax.rem(step, 2) == 1) & (unit < grad_in.units))
        def _():
            grad_in.work(unit)

    for unit in range(min((chunks + lag) // 2, grad_in.units), grad_in.units):
        grad_in.work(unit)
    shared.finish()
    grad_in.finish(grad_in.bands - 1)
    halo.drain()

    @pl.loop(0, chunks)
    def _(chunk):
        swap(chunk).wait_send()
        x_copy(chunk).wait_send()
        deep_copy(chunk).wait_send()
        store(chunk, 0).wait()

        @pl.when(inner)
        def _():
            rim_copy(chunk).wait_send()

    grad_in.drain()


def final_grads(whole, theirs, grads, tails, back, lines, weights):
    count = lax.axis_size("sp")
    parts = lax.axis_size("tp")
    pairs = parts // 2
    length, features = whole.shape
    width = weights[0].shape[1]
    depth = features // count
    block = features // parts
    bands = length // REACH
    vmem = pl.BlockSpec(memory_space=pltpu.VMEM)
    anywhere = pl.BlockSpec(memory_space=pl.ANY)
    out = jax.ShapeDtypeStruct((depth, width), jnp.float32)
    dma = pltpu.SemaphoreType.DMA
    low = jnp.bfloat16
    pair = paired(count, parts)
    scratch = [
        pltpu.VMEM((length, features), low),
        pltpu.VMEM((3, length, width), low),
        pltpu.VMEM((3, features, width), low),
        pltpu.VMEM((2, REACH, width), low),
        pltpu.VMEM((count - 1,) + lines.shape, jnp.float32),
        pltpu.VMEM((bands, pairs, REACH, block), low),
        pltpu.VMEM((bands, pairs, REACH, block), low),
        pltpu.VMEM((bands, pairs - 1, REACH, block), low),
        pltpu.VMEM((bands, pairs - 1, REACH, block), low),
        pltpu.VMEM((bands, REACH, block), jnp.float32),
        dma((7,)),
        dma((2,)),
        dma((2,)),
        dma((count - 1,)),
        dma((count - 1,)),
        dma((bands, pairs)),
        dma((bands, pairs)),
        dma((bands, pairs - 1)),
        dma((bands, pairs - 1)),
    ]
    if pair:
        tile = min(width, LANES)
        chunks = 3 * width // tile
        scratch += [
            pltpu.VMEM((length, features // 2), low),
            pltpu.VMEM((3, length, width), low),
            pltpu.VMEM((chunks, 2, depth, tile), low),
            pltpu.VMEM((chunks, 2, depth, tile), low),
            pltpu.VMEM((2, chunks, depth, tile), low),
            pltpu.VMEM((2, chunks, depth, tile), low),
            pltpu.VMEM((3, depth, width), jnp.float32),
            dma((1,)),
            dma((chunks,)),
            dma((chunks,)),
            dma((chunks,)),
            dma((chunks,)),
            dma((2, chunks)),
            dma((2, chunks)),
            dma((chunks,)),
        ]
    else:
        scratch += [
            pltpu.VMEM((2, 3, depth // 2, width), low),
            pltpu.VMEM((2, 3, count - 1, depth // 2, width), low),
            dma((2, 3, count - 1)),
            dma((2, 3, count - 1)),
        ]
    place = anywhere if pair else vmem
    return pl.pallas_call(
        functools.partial(pair_kernel if pair else ring_kernel, count, parts),
        in_specs=[anywhere] * (7 + pair) + [vmem] * 4,
        out_specs=[vmem] + [place] * 3 + [vmem],
        out_shape=[
            jax.ShapeDtypeStruct((length, block), low),
            out,
            out,
            out,
            jax.ShapeDtypeStruct(lines.shape, jnp.float32),
        ],
        scratch_shapes=scratch,
        compiler_params=pltpu.CompilerParams(
            collective_id=0, has_side_effects=True, vmem_limit_bytes=63 * 1024 * 1024
        ),
        cost_estimate=pl.CostEstimate(
            flops=12 * length * features * width,
            bytes_accessed=400_000_000,
            transcendentals=0,
        ),
    )(whole, *grads, *weights, *theirs, *tails, back, lines)


def gather_kernel(
    parts,
    tokens_ref,
    wq_ref,
    wk_ref,
    wv_ref,
    whole_ref,
    q_ref,
    k_ref,
    v_ref,
    prev_ref,
    theirs_ref,
    held,
    weights,
    total,
    halo,
    halo_got,
    side_send,
    side_recv,
    far_send,
    far_recv,
    relay_send,
    relay_recv,
    halo_send,
    halo_recv,
    load_sem,
    store_sem,
    *ship_refs,
):
    me = lax.axis_index("tp")
    seat = lax.axis_index("sp")
    seats = lax.axis_size("sp")
    partner = me + 1 - 2 * lax.rem(me, 2)
    chunks = held.shape[0]
    block = tokens_ref.shape[1]
    width = q_ref.shape[1]
    pairs = parts // 2
    matrices = (wq_ref, wk_ref, wv_ref)

    def source(device, away):
        return lax.rem(device + parts - 2 * away, parts)

    order = [me, partner]
    for away in range(1, pairs):
        order += [source(me, away), source(partner, away)]

    def load(slot, matrix):
        start = pl.multiple_of(order[slot] * block, block)
        return pltpu.make_async_copy(
            matrices[matrix].at[pl.ds(start, block)],
            weights.at[slot, matrix],
            load_sem.at[slot, matrix],
        )

    for slot in range(parts):
        for matrix in range(3):
            load(slot, matrix).start()

    barrier = pltpu.get_barrier_semaphore()
    for ahead in range(1, parts):
        pl.semaphore_signal(
            barrier,
            inc=1,
            device_id={"tp": lax.rem(me + ahead, parts)},
            device_id_type=pl.DeviceIdType.MESH,
        )
    onward = lax.rem(seat + 1, seats)
    for other in (onward, lax.rem(seat + seats - 1, seats)):
        pl.semaphore_signal(
            barrier, inc=1, device_id={"sp": other}, device_id_type=pl.DeviceIdType.MESH
        )
    ship = len(ship_refs) > 0
    if ship:
        level, lane, inner, near, made, mate = pair_places(seat)
        pl.semaphore_signal(
            barrier, inc=1, device_id={"sp": mate}, device_id_type=pl.DeviceIdType.MESH
        )
    pl.semaphore_wait(barrier, parts + 1 + ship)

    def rows(chunk):
        return pl.ds(chunk * REACH, REACH)

    def far(chunk, away):
        return remote(
            tokens_ref.at[rows(chunk)],
            held.at[chunk, me],
            far_send.at[chunk, away - 1],
            far_recv.at[chunk, away - 1],
            {"tp": lax.rem(me + 2 * away, parts)},
        )

    def side(chunk):
        return remote(
            tokens_ref.at[rows(chunk)],
            held.at[chunk, me],
            side_send.at[chunk],
            side_recv.at[chunk],
            {"tp": partner},
        )

    def relay(chunk, away):
        place = held.at[chunk, source(me, away)]
        return remote(
            place,
            place,
            relay_send.at[chunk, away - 1],
            relay_recv.at[chunk, away - 1],
            {"tp": partner},
        )

    def neighbour():
        return remote(halo, halo_got, halo_send, halo_recv, {"sp": onward})

    def store(chunk, slot):
        start = pl.multiple_of(order[slot] * block, block)
        src = tokens_ref.at[rows(chunk)] if slot == 0 else held.at[chunk, order[slot]]
        return pltpu.make_async_copy(
            src, whole_ref.at[rows(chunk), pl.ds(start, block)], store_sem.at[chunk, slot]
        )

    def add(chunk, slot, value):
        for matrix in range(3):
            term = jnp.dot(value, weights[slot, matrix], preferred_element_type=jnp.float32)
            if slot == 0:
                total[matrix, chunk] = term
            else:
                total[matrix, chunk] += term

    if ship:
        ship_got, ship_send, ship_recv, pass_send, pass_recv, keep_sem = ship_refs
        core = lax.rem(me, 2)
        shipped = jnp.where(inner, near, 1 - near)
        ready = me // 2 == shipped

        def ship_copy(chunk, src):
            return remote(
                src,
                ship_got.at[chunk, core],
                ship_send.at[chunk],
                ship_recv.at[chunk],
                {"sp": mate},
            )

        def pass_on(chunk):
            place = ship_got.at[chunk, core]
            return remote(
                place, place, pass_send.at[chunk], pass_recv.at[chunk], {"tp": partner}
            )

        def keep(chunk, which):
            start = pl.multiple_of(which * block, block)
            return pltpu.make_async_copy(
                ship_got.at[chunk, which],
                theirs_ref.at[rows(chunk), pl.ds(start, block)],
                keep_sem.at[chunk, which],
            )

    backwards = list(range(chunks))[::-1]
    for chunk in backwards:
        for away in range(1, pairs):
            far(chunk, away).start()
        side(chunk).start()
        if ship:

            @pl.when(ready)
            def _():
                ship_copy(chunk, tokens_ref.at[rows(chunk)]).start()

    for slot in range(2):
        for matrix in range(3):
            load(slot, matrix).wait()
        for chunk in backwards:
            if slot == 1:
                side(chunk).wait_recv()
            store(chunk, slot).start()
            value = tokens_ref[rows(chunk)] if slot == 0 else held[chunk, partner]
            add(chunk, slot, value)
    for slot in range(2, parts):
        for matrix in range(3):
            load(slot, matrix).wait()
    outs = (q_ref, k_ref, v_ref)
    for chunk in backwards:
        for away in range(1, pairs):
            far(chunk, away).wait_recv()
            relay(chunk, away).start()
            if ship:

                @pl.when(jnp.logical_not(ready))
                def _():
                    ship_copy(chunk, held.at[chunk, source(me, 1)]).start()

            store(chunk, 2 * away).start()
            add(chunk, 2 * away, held[chunk, source(me, away)])
        for away in range(1, pairs):
            relay(chunk, away).wait_recv()
            store(chunk, 2 * away + 1).start()
            add(chunk, 2 * away + 1, held[chunk, source(partner, away)])
        for matrix in range(3):
            outs[matrix][rows(chunk)] = total[matrix, chunk].astype(jnp.bfloat16)
        if chunk == chunks - 1:
            halo[0] = total[1, chunk].astype(jnp.bfloat16)
            halo[1] = total[2, chunk].astype(jnp.bfloat16)
            neighbour().start()
        if ship and chunk + 1 < chunks:
            ship_copy(chunk + 1, tokens_ref.at[rows(chunk)]).wait_recv()
            pass_on(chunk + 1).start()
            keep(chunk + 1, core).start()
    neighbour().wait()
    prev_ref[...] = halo_got[...]
    if ship:
        ship_copy(0, tokens_ref.at[rows(0)]).wait_recv()
        pass_on(0).start()
        keep(0, core).start()
        for chunk in backwards:
            pass_on(chunk).wait_recv()
            keep(chunk, 1 - core).start()
        for chunk in backwards:
            ship_copy(chunk, tokens_ref.at[rows(chunk)]).wait_send()
            pass_on(chunk).wait_send()
            keep(chunk, core).wait()
            keep(chunk, 1 - core).wait()
    for chunk in backwards:
        side(chunk).wait_send()
        for away in range(1, pairs):
            far(chunk, away).wait_send()
            relay(chunk, away).wait_send()
        for slot in range(parts):
            store(chunk, slot).wait()


def project(tokens, query_weight, key_weight, value_weight):
    parts = lax.axis_size("tp")
    length, block = tokens.shape
    width = query_weight.shape[1]
    chunks = length // REACH
    pairs = parts // 2
    vmem = pl.BlockSpec(memory_space=pltpu.VMEM)
    anywhere = pl.BlockSpec(memory_space=pl.ANY)
    narrow = jax.ShapeDtypeStruct((length, width), jnp.bfloat16)
    dma = pltpu.SemaphoreType.DMA
    ship = paired(lax.axis_size("sp"), parts)
    extra = []
    if ship:
        extra = [
            pltpu.VMEM((chunks, 2, REACH, block), jnp.bfloat16),
            dma((chunks,)),
            dma((chunks,)),
            dma((chunks,)),
            dma((chunks,)),
            dma((chunks, 2)),
        ]
    return pl.pallas_call(
        functools.partial(gather_kernel, parts),
        in_specs=[vmem, anywhere, anywhere, anywhere],
        out_specs=[anywhere, vmem, vmem, vmem, vmem, anywhere],
        out_shape=[
            jax.ShapeDtypeStruct((length, block * parts), jnp.bfloat16),
            narrow,
            narrow,
            narrow,
            jax.ShapeDtypeStruct((2, REACH, width), jnp.bfloat16),
            jax.ShapeDtypeStruct((length, 2 * block) if ship else (8, LANES), jnp.bfloat16),
        ],
        scratch_shapes=[
            pltpu.VMEM((chunks, parts, REACH, block), jnp.bfloat16),
            pltpu.VMEM((parts, 3, block, width), jnp.bfloat16),
            pltpu.VMEM((3, chunks, REACH, width), jnp.float32),
            pltpu.VMEM((2, REACH, width), jnp.bfloat16),
            pltpu.VMEM((2, REACH, width), jnp.bfloat16),
            dma((chunks,)),
            dma((chunks,)),
            dma((chunks, pairs - 1)),
            dma((chunks, pairs - 1)),
            dma((chunks, pairs - 1)),
            dma((chunks, pairs - 1)),
            dma(()),
            dma(()),
            dma((parts, 3)),
            dma((chunks, parts)),
        ]
        + extra,
        compiler_params=pltpu.CompilerParams(
            collective_id=1, has_side_effects=True, vmem_limit_bytes=56 * 1024 * 1024
        ),
        cost_estimate=pl.CostEstimate(
            flops=6 * length * block * parts * width, bytes_accessed=150_000_000, transcendentals=0
        ),
    )(tokens, query_weight, key_weight, value_weight)


def shards(tokens, query_weight, key_weight, value_weight, position_bias, out_grad):
    whole, query, keys, values, prev, theirs = project(
        tokens, query_weight, key_weight, value_weight
    )
    query_grad, key_body, value_body, key_tail, value_tail, back, lines = attention(
        query, keys, values, prev, out_grad, position_bias
    )
    input_grad, query_weight_grad, key_weight_grad, value_weight_grad, lines = final_grads(
        whole,
        (theirs,) if paired(lax.axis_size("sp"), lax.axis_size("tp")) else (),
        (query_grad, key_body, value_body),
        (key_tail, value_tail),
        back,
        lines[:, 0],
        (query_weight, key_weight, value_weight),
    )
    bias_grad = table_to_bias(lines, position_bias.shape[1])
    return input_grad, query_weight_grad, key_weight_grad, value_weight_grad, bias_grad


def solution(mesh):
    in_specs = (
        P("sp", "tp"),
        P(None, "tp"),
        P(None, "tp"),
        P(None, "tp"),
        P("tp", None),
        P("sp", "tp"),
    )
    out_specs = (P("sp", "tp"), P("sp", "tp"), P("sp", "tp"), P("sp", "tp"), P("tp", None))
    return jax.shard_map(shards, mesh=mesh, in_specs=in_specs, out_specs=out_specs, check_vma=False)
```

```python
import functools

import jax
import jax.numpy as jnp
from jax import lax
from jax.experimental import pallas as pl
from jax.experimental.pallas import tpu as pltpu
from jax.sharding import PartitionSpec as P

SEGMENT = 64
PREVIOUS = 4
CLIP = 256
ROWS = 2 * SEGMENT
REACH = PREVIOUS * SEGMENT
WINDOW = ROWS + REACH
TABLE = 512
LANES = 128
GRAIN = 256
HIDDEN = -1e30


def contract_rows(left, right):
    return lax.dot_general(
        left, right, (((0,), (0,)), ((), ())), preferred_element_type=jnp.float32
    )


def contract_cols(left, right):
    return lax.dot_general(
        left, right, (((1,), (1,)), ((), ())), preferred_element_type=jnp.float32
    )


def diagonal_sums(tile):
    half = tile.shape[0] // 2
    while half >= 8:
        tile = tile[:half] + pltpu.roll(tile[half:], TABLE - half, 1)
        half //= 2
    row = lax.broadcasted_iota(jnp.int32, tile.shape, 0)
    for step in (4, 2, 1):
        tile = jnp.where((row & step) != 0, pltpu.roll(tile, TABLE - step, 1), tile)
    return jnp.sum(tile, axis=0, keepdims=True)


def table_map(entries):
    entry = lax.broadcasted_iota(jnp.int32, (entries, TABLE), 0)
    column = lax.broadcasted_iota(jnp.int32, (entries, TABLE), 1)
    near = column + entry == entries - 1
    far = (column >= WINDOW) & (entry == entries - 1)
    return jnp.where(near | far, 1.0, 0.0).astype(jnp.float32)


def exact(left, right, axis):
    return lax.dot_general(
        left,
        right,
        (((1,), (axis,)), ((), ())),
        precision=lax.Precision.HIGHEST,
        preferred_element_type=jnp.float32,
    )


class Attention:
    def __init__(self, factor, heads, q_all, k_all, v_all, g_ref, dq_ref, scratch):
        self.factor, self.heads = factor, heads
        self.q_all, self.k_all, self.v_all = q_all, k_all, v_all
        self.g_ref, self.dq_ref = g_ref, dq_ref
        self.bias_all, self.bias_sum, self.dk_all, self.dv_all = scratch
        self.head = q_all.shape[1] // heads

    def begin(self, table_rows):
        self.dk_all[...] = jnp.zeros_like(self.dk_all)
        self.dv_all[...] = jnp.zeros_like(self.dv_all)
        self.bias_sum[...] = jnp.zeros_like(self.bias_sum)
        row = lax.broadcasted_iota(jnp.int32, (ROWS, WINDOW), 0) // SEGMENT
        column = lax.broadcasted_iota(jnp.int32, (ROWS, WINDOW), 1)
        behind = column // SEGMENT - row
        seen = (behind >= 0) & (behind <= PREVIOUS)
        for head in range(self.heads):
            table = jnp.broadcast_to(table_rows[head : head + 1], (ROWS, TABLE))
            bias = pltpu.roll(table, 0, 1, stride=1, stride_axis=0)[:, :WINDOW]
            self.bias_all[head] = jnp.where(seen, bias, HIDDEN)

    def attend(self, start):
        @pl.loop(0, self.heads)
        def _(head):
            columns = pl.ds(pl.multiple_of(head * self.head, self.head), self.head)
            rows = slice(start, start + ROWS)
            window = slice(start, start + WINDOW)
            q = self.q_all[rows, columns]
            g = self.g_ref[rows, columns]
            k = self.k_all[window, columns]
            v = self.v_all[window, columns]
            mask = self.bias_all[head]
            if start < REACH:
                first = jnp.where(lax.axis_index("sp") == 0, REACH - start, 0)
                column = lax.broadcasted_iota(jnp.int32, (ROWS, WINDOW), 1)
                mask = jnp.where(column < first, HIDDEN, mask)
            scores = contract_cols(q, k) * self.factor + mask
            top = jnp.max(scores, axis=1, keepdims=True)
            raised = jnp.exp(scores - top)
            weights = raised * (1.0 / jnp.sum(raised, axis=1, keepdims=True))
            prob_grad = contract_cols(g, v)
            delta = jnp.sum(weights * prob_grad, axis=1, keepdims=True)
            score_grad = weights * (prob_grad - delta)
            self.bias_sum[head] += score_grad
            low = score_grad.astype(jnp.bfloat16)
            dq = jnp.dot(low, k, preferred_element_type=jnp.float32) * self.factor
            self.dq_ref[rows, columns] = dq.astype(jnp.bfloat16)
            self.dk_all[window, columns] += contract_rows(low, q)
            self.dv_all[window, columns] += contract_rows(weights.astype(jnp.bfloat16), g)

    def end(self, dk_ref, dv_ref, dk_tail_ref, dv_tail_ref, back_ref, line_ref):
        length = self.q_all.shape[0]
        dk_all, dv_all, factor = self.dk_all, self.dv_all, self.factor
        back_ref[0] = (dk_all[:REACH] * factor).astype(jnp.bfloat16)
        back_ref[1] = dv_all[:REACH].astype(jnp.bfloat16)
        dk_ref[...] = (dk_all[REACH:length] * factor).astype(jnp.bfloat16)
        dv_ref[...] = dv_all[REACH:length].astype(jnp.bfloat16)
        dk_tail_ref[...] = dk_all[length:] * factor
        dv_tail_ref[...] = dv_all[length:]
        for head in range(self.heads):
            blank = jnp.zeros((ROWS, TABLE - WINDOW), jnp.float32)
            padded = jnp.concatenate([self.bias_sum[head], blank], axis=1)
            line_ref[head : head + 1] = diagonal_sums(padded)


def ring_columns(count):
    columns = 1
    while (2 * columns) ** 2 <= count:
        columns *= 2
    return columns


def ring_place(index, count):
    columns = ring_columns(count)
    rows = count // columns
    row, column = index // columns, index % columns
    above = rows - 1 - row
    across = jnp.where(above % 2 == 0, column - 1, columns - 1 - column)
    return jnp.where(column == 0, row, rows + above * (columns - 1) + across)


def ring_index(place, count):
    columns = ring_columns(count)
    rows = count // columns
    later = jnp.maximum(place - rows, 0)
    above, across = later // (columns - 1), later % (columns - 1)
    column = jnp.where(above % 2 == 0, 1 + across, columns - 1 - across)
    return jnp.where(place < rows, place * columns, (rows - 1 - above) * columns + column)


def remote(src, dst, send, recv, device):
    return pltpu.make_async_remote_copy(
        src_ref=src,
        dst_ref=dst,
        send_sem=send,
        recv_sem=recv,
        device_id=device,
        device_id_type=pl.DeviceIdType.MESH,
    )


def meet(count, parts):
    me = lax.axis_index("sp")
    seat = lax.axis_index("tp")
    barrier = pltpu.get_barrier_semaphore()
    for ahead in range(1, count):
        peer = lax.rem(me + ahead, count)
        pl.semaphore_signal(
            barrier, inc=1, device_id={"sp": peer}, device_id_type=pl.DeviceIdType.MESH
        )
    for ahead in range(1, parts):
        peer = lax.rem(seat + ahead, parts)
        pl.semaphore_signal(
            barrier, inc=1, device_id={"tp": peer}, device_id_type=pl.DeviceIdType.MESH
        )
    pl.semaphore_wait(barrier, count + parts - 2)


def final_loads(hbm, whole, grads, weights, load_sem):
    whole_hbm, dq_hbm, dk_hbm, dv_hbm, wq_hbm, wk_hbm, wv_hbm = hbm
    body = whole.shape[0] - REACH
    return [
        pltpu.make_async_copy(dq_hbm, grads.at[0], load_sem.at[0]),
        pltpu.make_async_copy(dk_hbm, grads.at[1, pl.ds(0, body)], load_sem.at[1]),
        pltpu.make_async_copy(dv_hbm, grads.at[2, pl.ds(0, body)], load_sem.at[2]),
        pltpu.make_async_copy(whole_hbm, whole, load_sem.at[3]),
        pltpu.make_async_copy(wq_hbm, weights.at[0], load_sem.at[4]),
        pltpu.make_async_copy(wk_hbm, weights.at[1], load_sem.at[5]),
        pltpu.make_async_copy(wv_hbm, weights.at[2], load_sem.at[6]),
    ]


class Halo:
    def __init__(self, count, grads, tails, back_ref, after, send, recv):
        self.me = lax.axis_index("sp")
        self.count = count
        self.grads, self.tails = grads, tails
        self.back_ref, self.after, self.sems = back_ref, after, (send, recv)

    def copy(self, which):
        return remote(
            self.back_ref.at[which],
            self.after.at[which],
            self.sems[0].at[which],
            self.sems[1].at[which],
            {"sp": lax.rem(self.me + self.count - 1, self.count)},
        )

    def start(self):
        @pl.when(self.me > 0)
        def _():
            self.copy(0).start()
            self.copy(1).start()

    def join(self, which):
        after = self.after

        @pl.when(self.me < self.count - 1)
        def _():
            self.copy(which).wait_recv()

        @pl.when(self.me == self.count - 1)
        def _():
            after[which] = jnp.zeros_like(after[which])

        tail = self.tails[which][...] + after[which].astype(jnp.float32)
        body = self.grads.shape[1] - REACH
        self.grads[1 + which, body:] = tail.astype(jnp.bfloat16)

    def drain(self):
        @pl.when(self.me > 0)
        def _():
            self.copy(0).wait_send()
            self.copy(1).wait_send()


class Lines:
    def __init__(self, count, line_ref, out_ref, lines, send, recv):
        self.me = lax.axis_index("sp")
        self.count = count
        self.line_ref, self.out_ref, self.lines = line_ref, out_ref, lines
        self.sems = (send, recv)

    def copy(self, ahead):
        return remote(
            self.line_ref,
            self.lines.at[ahead - 1],
            self.sems[0].at[ahead - 1],
            self.sems[1].at[ahead - 1],
            {"sp": lax.rem(self.me + ahead, self.count)},
        )

    def start(self):
        for ahead in range(1, self.count):
            self.copy(ahead).start()

    def finish(self):
        total = self.line_ref[...]
        for ahead in range(1, self.count):
            self.copy(ahead).wait()
            total = total + self.lines[ahead - 1]
        self.out_ref[...] = exact(total, table_map(self.out_ref.shape[1]), 1)


class InputGrad:
    def __init__(self, parts, grads, weights, input_ref, buffers, sems):
        self.seat = lax.axis_index("tp")
        self.core = lax.rem(self.seat, 2)
        self.row = self.seat // 2
        self.parts, self.pairs = parts, parts // 2
        self.grads, self.weights, self.input_ref = grads, weights, input_ref
        self.pair_sent, self.pair_got, self.cross_sent, self.cross_got, self.kept = buffers
        self.sems = sems
        self.block = input_ref.shape[1]
        self.bands = input_ref.shape[0] // REACH
        self.units = 2 * self.bands

    def rows(self, band):
        return pl.ds(pl.multiple_of(band * REACH, REACH), REACH)

    def part(self, band, target):
        block = pl.ds(pl.multiple_of(target * self.block, self.block), self.block)
        rows = self.rows(band)
        term = contract_cols(self.grads[0, rows], self.weights[0, block])
        term += contract_cols(self.grads[1, rows], self.weights[1, block])
        return term + contract_cols(self.grads[2, rows], self.weights[2, block])

    def pair_copy(self, band, away):
        return remote(
            self.pair_sent.at[band, away],
            self.pair_got.at[band, away],
            self.sems[0].at[band, away],
            self.sems[1].at[band, away],
            {"tp": self.seat + 1 - 2 * self.core},
        )

    def cross_copy(self, band, away):
        return remote(
            self.cross_sent.at[band, away - 1],
            self.cross_got.at[band, away - 1],
            self.sems[2].at[band, away - 1],
            self.sems[3].at[band, away - 1],
            {"tp": lax.rem(self.seat + 2 * away, self.parts)},
        )

    def to_partner(self, band):
        for away in range(self.pairs):
            target = 2 * lax.rem(self.row + away, self.pairs) + 1 - self.core
            self.pair_sent[band, away] = self.part(band, target).astype(jnp.bfloat16)
            self.pair_copy(band, away).start()

    def across(self, band):
        for away in range(1, self.pairs):
            term = self.part(band, lax.rem(self.seat + 2 * away, self.parts))
            self.pair_copy(band, away).wait_recv()
            term = term + self.pair_got[band, away].astype(jnp.float32)
            self.cross_sent[band, away - 1] = term.astype(jnp.bfloat16)
            self.cross_copy(band, away).start()
        term = self.part(band, self.seat)
        self.pair_copy(band, 0).wait_recv()
        self.kept[band] = term + self.pair_got[band, 0].astype(jnp.float32)

    def finish(self, band):
        term = self.kept[band]
        for away in range(1, self.pairs):
            self.cross_copy(band, away).wait_recv()
            term = term + self.cross_got[band, away - 1].astype(jnp.float32)
        self.input_ref[self.rows(band)] = term.astype(jnp.bfloat16)

    def work(self, unit):
        band = unit // 2

        @pl.when(lax.rem(unit, 2) == 0)
        def _():
            self.to_partner(band)

        @pl.when(lax.rem(unit, 2) == 1)
        def _():
            self.across(band)

        @pl.when((lax.rem(unit, 2) == 1) & (unit > 2))
        def _():
            self.finish(band - 1)

    def drain(self):
        @pl.loop(0, self.bands)
        def _(band):
            for away in range(self.pairs):
                self.pair_copy(band, away).wait_send()
            for away in range(1, self.pairs):
                self.cross_copy(band, away).wait_send()


def ring_kernel(
    count,
    parts,
    whole_hbm,
    dq_hbm,
    dk_hbm,
    dv_hbm,
    wq_hbm,
    wk_hbm,
    wv_hbm,
    dk_tail_ref,
    dv_tail_ref,
    back_ref,
    line_ref,
    input_ref,
    oq_ref,
    ok_ref,
    ov_ref,
    line_out_ref,
    whole,
    grads,
    weights,
    after,
    lines,
    pair_sent,
    pair_got,
    cross_sent,
    cross_got,
    kept,
    load_sem,
    back_send,
    back_recv,
    line_send,
    line_recv,
    pair_send,
    pair_recv,
    cross_send,
    cross_recv,
    sent,
    got,
    send_sem,
    recv_sem,
):
    me = lax.axis_index("sp")
    place = ring_place(me, count)
    hbm = (whole_hbm, dq_hbm, dk_hbm, dv_hbm, wq_hbm, wk_hbm, wv_hbm)
    loads = final_loads(hbm, whole, grads, weights, load_sem)
    for load in loads:
        load.start()
    meet(count, parts)
    halo = Halo(
        count, grads, (dk_tail_ref, dv_tail_ref), back_ref, after, back_send, back_recv
    )
    shared = Lines(count, line_ref, line_out_ref, lines, line_send, line_recv)
    buffers = (pair_sent, pair_got, cross_sent, cross_got, kept)
    sems = (pair_send, pair_recv, cross_send, cross_recv)
    grad_in = InputGrad(parts, grads, weights, input_ref, buffers, sems)

    outs = (oq_ref, ok_ref, ov_ref)
    half = got.shape[3]
    onward = (
        ring_index(lax.rem(place + 1, count), count),
        ring_index(lax.rem(place + count - 1, count), count),
    )

    def own(target, side, chain):
        start = pl.multiple_of((2 * ring_index(target, count) + side) * half, half)
        return contract_rows(whole[:, pl.ds(start, half)], grads[chain])

    def target_of(step, side):
        if side == 0:
            return lax.rem(place - 1 - step + 2 * count, count)
        return lax.rem(place + 1 + step, count)

    def copy_of(src, step, side, chain):
        return remote(
            src,
            got.at[side, chain, step],
            send_sem.at[side, chain, step],
            recv_sem.at[side, chain, step],
            {"sp": onward[side]},
        )

    halo.start()
    for load in loads:
        load.wait()
    for chain in range(3):
        if chain > 0:
            halo.join(chain - 1)
        for side in range(2):
            sent[side, chain] = own(target_of(0, side), side, chain).astype(jnp.bfloat16)
            copy_of(sent.at[side, chain], 0, side, chain).start()
    shared.start()

    chains = [(chain, side) for chain in range(3) for side in range(2)]

    @pl.loop(1, count - 1)
    def _(step):
        for chain, side in chains:
            part_of = own(target_of(step, side), side, chain)
            place_of = got.at[side, chain, step - 1]
            copy_of(sent.at[side, chain], step - 1, side, chain).wait_recv()
            total = part_of + place_of[...].astype(jnp.float32)
            place_of[...] = total.astype(jnp.bfloat16)
            copy_of(place_of, step, side, chain).start()
            if (chain, side) == (1, 1):

                @pl.when(step <= grad_in.units)
                def _():
                    grad_in.work(step - 1)

    for unit in range(min(count - 2, grad_in.units), grad_in.units):
        grad_in.work(unit)
    shared.finish()
    for chain, side in chains:
        if (chain, side) == (2, 0):
            grad_in.finish(grad_in.bands - 1)
        part_of = own(place, side, chain)
        copy_of(sent.at[side, chain], count - 2, side, chain).wait_recv()
        total = part_of + got[side, chain, count - 2].astype(jnp.float32)
        outs[chain][side * half : (side + 1) * half] = total

    halo.drain()

    @pl.loop(0, count - 1)
    def _(step):
        for chain, side in chains:
            copy_of(sent.at[side, chain], step, side, chain).wait_send()

    grad_in.drain()


def paired(count, parts):
    return count == 8 and ring_columns(count) == 2 and parts == 4


def pair_places(me):
    level, side = me // 2, lax.rem(me, 2)
    inner = (level == 1) | (level == 2)
    near = level // 2
    made = jnp.where(inner, 1 - near, near)
    partner = 2 * (level + 1 - 2 * lax.rem(level, 2)) + side
    return level, side, inner, near, made, partner


def pair_kernel(
    count,
    parts,
    whole_hbm,
    dq_hbm,
    dk_hbm,
    dv_hbm,
    wq_hbm,
    wk_hbm,
    wv_hbm,
    theirs_hbm,
    dk_tail_ref,
    dv_tail_ref,
    back_ref,
    line_ref,
    input_ref,
    oq_ref,
    ok_ref,
    ov_ref,
    line_out_ref,
    whole,
    grads,
    weights,
    after,
    lines,
    pair_sent,
    pair_got,
    cross_sent,
    cross_got,
    kept,
    load_sem,
    back_send,
    back_recv,
    line_send,
    line_recv,
    pair_send,
    pair_recv,
    cross_send,
    cross_recv,
    theirs,
    their_grads,
    x_sent,
    x_got,
    sent,
    got,
    result,
    theirs_sem,
    swap_send,
    swap_recv,
    x_send,
    x_recv,
    send_sem,
    recv_sem,
    out_sem,
):
    me = lax.axis_index("sp")
    level, side, inner, near, made, partner = pair_places(me)
    hbm = (whole_hbm, dq_hbm, dk_hbm, dv_hbm, wq_hbm, wk_hbm, wv_hbm)
    loads = final_loads(hbm, whole, grads, weights, load_sem)
    loads.insert(4, pltpu.make_async_copy(theirs_hbm, theirs, theirs_sem.at[0]))
    for load in loads:
        load.start()
    meet(count, parts)
    halo = Halo(
        count, grads, (dk_tail_ref, dv_tail_ref), back_ref, after, back_send, back_recv
    )
    shared = Lines(count, line_ref, line_out_ref, lines, line_send, line_recv)
    buffers = (pair_sent, pair_got, cross_sent, cross_got, kept)
    sems = (pair_send, pair_recv, cross_send, cross_recv)
    grad_in = InputGrad(parts, grads, weights, input_ref, buffers, sems)

    chunks, depth, tile = x_sent.shape[0], x_sent.shape[2], x_sent.shape[3]
    per = chunks // 3
    outs = (oq_ref, ok_ref, ov_ref)
    deep = 2 * (1 + made)
    rim = 6 * made
    slot = jnp.where(inner, 0, 1)

    def columns(chunk):
        return pl.ds(pl.multiple_of(lax.rem(chunk, per) * tile, tile), tile)

    def swap(chunk):
        return remote(
            grads.at[chunk // per, :, columns(chunk)],
            their_grads.at[chunk // per, :, columns(chunk)],
            swap_send.at[chunk],
            swap_recv.at[chunk],
            {"sp": partner},
        )

    def x_copy(chunk):
        return remote(
            x_sent.at[chunk],
            x_got.at[chunk],
            x_send.at[chunk],
            x_recv.at[chunk],
            {"sp": 2 * level + 1 - side},
        )

    def deep_copy(chunk):
        return remote(
            sent.at[0, chunk],
            got.at[slot, chunk],
            send_sem.at[0, chunk],
            recv_sem.at[slot, chunk],
            {"sp": deep + side},
        )

    def rim_copy(chunk):
        return remote(
            sent.at[1, chunk],
            got.at[0, chunk],
            send_sem.at[1, chunk],
            recv_sem.at[0, chunk],
            {"sp": rim + side},
        )

    def arrived(chunk, which):
        return remote(
            sent.at[0, chunk],
            got.at[which, chunk],
            send_sem.at[0, chunk],
            recv_sem.at[which, chunk],
            {"sp": deep + side},
        )

    def sums(target, chunk):
        start = pl.multiple_of(target * depth, depth)
        mine = whole[:, pl.ds(start, depth)]
        start = pl.multiple_of((target - made * (count // 2)) * depth, depth)
        their = theirs[:, pl.ds(start, depth)]
        term = contract_rows(mine, grads[chunk // per, :, columns(chunk)])
        return term + contract_rows(their, their_grads[chunk // per, :, columns(chunk)])

    def halve(chunk):
        swap(chunk).wait_recv()
        x_sent[chunk, 0] = sums(deep + 1 - side, chunk).astype(jnp.bfloat16)
        x_sent[chunk, 1] = sums(rim + 1 - side, chunk).astype(jnp.bfloat16)
        x_copy(chunk).start()

    def onward(chunk):
        term = sums(deep + side, chunk)
        x_copy(chunk).wait_recv()
        term = term + x_got[chunk, 0].astype(jnp.float32)
        sent[0, chunk] = term.astype(jnp.bfloat16)
        deep_copy(chunk).start()
        term = sums(rim + side, chunk) + x_got[chunk, 1].astype(jnp.float32)

        @pl.when(inner)
        def _():
            sent[1, chunk] = term.astype(jnp.bfloat16)
            rim_copy(chunk).start()

        @pl.when(jnp.logical_not(inner))
        def _():
            result[chunk // per, :, columns(chunk)] = term

    def store(chunk, matrix):
        return pltpu.make_async_copy(
            result.at[matrix, :, columns(chunk)],
            outs[matrix].at[:, columns(chunk)],
            out_sem.at[chunk],
        )

    def finish(chunk):
        arrived(chunk, 0).wait_recv()
        term = got[0, chunk].astype(jnp.float32)

        @pl.when(inner)
        def _():
            arrived(chunk, 1).wait_recv()
            total = term + got[1, chunk].astype(jnp.float32)
            result[chunk // per, :, columns(chunk)] = total

        @pl.when(jnp.logical_not(inner))
        def _():
            total = term + result[chunk // per, :, columns(chunk)]
            result[chunk // per, :, columns(chunk)] = total

        for matrix in range(3):

            @pl.when(chunk // per == matrix)
            def _():
                store(chunk, matrix).start()

    halo.start()
    loads[0].wait()
    for chunk in range(per):
        swap(chunk).start()
    for which in range(2):
        loads[1 + which].wait()
        halo.join(which)
        for chunk in range(per):
            swap((1 + which) * per + chunk).start()
    for load in loads[3:]:
        load.wait()
    shared.start()

    lag = 3 * chunks // 4

    @pl.loop(0, chunks + lag)
    def _(step):
        @pl.when(step < chunks)
        def _():
            halve(step)

        @pl.when((step > 0) & (step <= chunks))
        def _():
            onward(step - 1)

        @pl.when(step >= lag)
        def _():
            finish(step - lag)

        unit = (step - 1) // 2

        @pl.when((lax.rem(step, 2) == 1) & (unit < grad_in.units))
        def _():
            grad_in.work(unit)

    for unit in range(min((chunks + lag) // 2, grad_in.units), grad_in.units):
        grad_in.work(unit)
    shared.finish()
    grad_in.finish(grad_in.bands - 1)
    halo.drain()

    @pl.loop(0, chunks)
    def _(chunk):
        swap(chunk).wait_send()
        x_copy(chunk).wait_send()
        deep_copy(chunk).wait_send()
        store(chunk, 0).wait()

        @pl.when(inner)
        def _():
            rim_copy(chunk).wait_send()

    grad_in.drain()


def final_grads(whole, theirs, grads, tails, back, lines, weights, entries):
    count = lax.axis_size("sp")
    parts = lax.axis_size("tp")
    pairs = parts // 2
    length, features = whole.shape
    width = weights[0].shape[1]
    depth = features // count
    block = features // parts
    bands = length // REACH
    vmem = pl.BlockSpec(memory_space=pltpu.VMEM)
    anywhere = pl.BlockSpec(memory_space=pl.ANY)
    out = jax.ShapeDtypeStruct((depth, width), jnp.float32)
    dma = pltpu.SemaphoreType.DMA
    low = jnp.bfloat16
    pair = paired(count, parts)
    scratch = [
        pltpu.VMEM((length, features), low),
        pltpu.VMEM((3, length, width), low),
        pltpu.VMEM((3, features, width), low),
        pltpu.VMEM((2, REACH, width), low),
        pltpu.VMEM((count - 1,) + lines.shape, jnp.float32),
        pltpu.VMEM((bands, pairs, REACH, block), low),
        pltpu.VMEM((bands, pairs, REACH, block), low),
        pltpu.VMEM((bands, pairs - 1, REACH, block), low),
        pltpu.VMEM((bands, pairs - 1, REACH, block), low),
        pltpu.VMEM((bands, REACH, block), jnp.float32),
        dma((7,)),
        dma((2,)),
        dma((2,)),
        dma((count - 1,)),
        dma((count - 1,)),
        dma((bands, pairs)),
        dma((bands, pairs)),
        dma((bands, pairs - 1)),
        dma((bands, pairs - 1)),
    ]
    if pair:
        tile = min(width, LANES)
        chunks = 3 * width // tile
        scratch += [
            pltpu.VMEM((length, features // 2), low),
            pltpu.VMEM((3, length, width), low),
            pltpu.VMEM((chunks, 2, depth, tile), low),
            pltpu.VMEM((chunks, 2, depth, tile), low),
            pltpu.VMEM((2, chunks, depth, tile), low),
            pltpu.VMEM((2, chunks, depth, tile), low),
            pltpu.VMEM((3, depth, width), jnp.float32),
            dma((1,)),
            dma((chunks,)),
            dma((chunks,)),
            dma((chunks,)),
            dma((chunks,)),
            dma((2, chunks)),
            dma((2, chunks)),
            dma((chunks,)),
        ]
    else:
        scratch += [
            pltpu.VMEM((2, 3, depth // 2, width), low),
            pltpu.VMEM((2, 3, count - 1, depth // 2, width), low),
            dma((2, 3, count - 1)),
            dma((2, 3, count - 1)),
        ]
    place = anywhere if pair else vmem
    return pl.pallas_call(
        functools.partial(pair_kernel if pair else ring_kernel, count, parts),
        in_specs=[anywhere] * (7 + pair) + [vmem] * 4,
        out_specs=[vmem] + [place] * 3 + [vmem],
        out_shape=[
            jax.ShapeDtypeStruct((length, block), low),
            out,
            out,
            out,
            jax.ShapeDtypeStruct((lines.shape[0], entries), jnp.float32),
        ],
        scratch_shapes=scratch,
        compiler_params=pltpu.CompilerParams(
            collective_id=0, has_side_effects=True, vmem_limit_bytes=63 * 1024 * 1024
        ),
        cost_estimate=pl.CostEstimate(
            flops=12 * length * features * width,
            bytes_accessed=400_000_000,
            transcendentals=0,
        ),
    )(whole, *grads, *weights, *theirs, *tails, back, lines)


def gather_kernel(
    parts,
    tokens_ref,
    wq_ref,
    wk_ref,
    wv_ref,
    g_ref,
    bias_ref,
    whole_ref,
    theirs_ref,
    dq_ref,
    dk_ref,
    dv_ref,
    dk_tail_ref,
    dv_tail_ref,
    back_ref,
    line_ref,
    held,
    weights,
    total,
    halo,
    halo_got,
    q_all,
    k_all,
    v_all,
    bias_all,
    bias_sum,
    dk_all,
    dv_all,
    side_send,
    side_recv,
    far_send,
    far_recv,
    relay_send,
    relay_recv,
    halo_send,
    halo_recv,
    load_sem,
    store_sem,
    *ship_refs,
):
    me = lax.axis_index("tp")
    seat = lax.axis_index("sp")
    seats = lax.axis_size("sp")
    partner = me + 1 - 2 * lax.rem(me, 2)
    chunks = held.shape[0]
    block = tokens_ref.shape[1]
    grain = held.shape[2]
    length = tokens_ref.shape[0]
    heads, entries = bias_ref.shape
    pairs = parts // 2
    matrices = (wq_ref, wk_ref, wv_ref)

    def source(device, away):
        return lax.rem(device + parts - 2 * away, parts)

    order = [me, partner]
    for away in range(1, pairs):
        order += [source(me, away), source(partner, away)]

    def load(slot, matrix):
        start = pl.multiple_of(order[slot] * block, block)
        return pltpu.make_async_copy(
            matrices[matrix].at[pl.ds(start, block)],
            weights.at[slot, matrix],
            load_sem.at[slot, matrix],
        )

    for slot in range(parts):
        for matrix in range(3):
            load(slot, matrix).start()

    barrier = pltpu.get_barrier_semaphore()
    for ahead in range(1, parts):
        pl.semaphore_signal(
            barrier,
            inc=1,
            device_id={"tp": lax.rem(me + ahead, parts)},
            device_id_type=pl.DeviceIdType.MESH,
        )
    onward = lax.rem(seat + 1, seats)
    for other in (onward, lax.rem(seat + seats - 1, seats)):
        pl.semaphore_signal(
            barrier, inc=1, device_id={"sp": other}, device_id_type=pl.DeviceIdType.MESH
        )
    ship = len(ship_refs) > 0
    if ship:
        level, lane, inner, near, made, mate = pair_places(seat)
        pl.semaphore_signal(
            barrier, inc=1, device_id={"sp": mate}, device_id_type=pl.DeviceIdType.MESH
        )
    pl.semaphore_wait(barrier, parts + 1 + ship)

    def rows(chunk):
        return pl.ds(chunk * grain, grain)

    def far(chunk, away):
        return remote(
            tokens_ref.at[rows(chunk)],
            held.at[chunk, me],
            far_send.at[chunk, away - 1],
            far_recv.at[chunk, away - 1],
            {"tp": lax.rem(me + 2 * away, parts)},
        )

    def side(chunk):
        return remote(
            tokens_ref.at[rows(chunk)],
            held.at[chunk, me],
            side_send.at[chunk],
            side_recv.at[chunk],
            {"tp": partner},
        )

    def relay(chunk, away):
        place = held.at[chunk, source(me, away)]
        return remote(
            place,
            place,
            relay_send.at[chunk, away - 1],
            relay_recv.at[chunk, away - 1],
            {"tp": partner},
        )

    def neighbour():
        return remote(halo, halo_got, halo_send, halo_recv, {"sp": onward})

    scratch = (bias_all, bias_sum, dk_all, dv_all)
    factor = (q_all.shape[1] // heads) ** (-0.5)
    work = Attention(factor, heads, q_all, k_all, v_all, g_ref, dq_ref, scratch)

    def store(chunk, slot):
        start = pl.multiple_of(order[slot] * block, block)
        src = tokens_ref.at[rows(chunk)] if slot == 0 else held.at[chunk, order[slot]]
        return pltpu.make_async_copy(
            src, whole_ref.at[rows(chunk), pl.ds(start, block)], store_sem.at[chunk, slot]
        )

    def add(chunk, slot, value):
        for matrix in range(3):
            term = jnp.dot(value, weights[slot, matrix], preferred_element_type=jnp.float32)
            if slot == 0:
                total[matrix, chunk] = term
            else:
                total[matrix, chunk] += term

    if ship:
        ship_got, ship_send, ship_recv, pass_send, pass_recv, keep_sem = ship_refs
        core = lax.rem(me, 2)
        shipped = jnp.where(inner, near, 1 - near)
        ready = me // 2 == shipped

        def ship_copy(chunk, src):
            return remote(
                src,
                ship_got.at[chunk, core],
                ship_send.at[chunk],
                ship_recv.at[chunk],
                {"sp": mate},
            )

        def pass_on(chunk):
            place = ship_got.at[chunk, core]
            return remote(
                place, place, pass_send.at[chunk], pass_recv.at[chunk], {"tp": partner}
            )

        def keep(chunk, which):
            start = pl.multiple_of(which * block, block)
            return pltpu.make_async_copy(
                ship_got.at[chunk, which],
                theirs_ref.at[rows(chunk), pl.ds(start, block)],
                keep_sem.at[chunk, which],
            )

    backwards = list(range(chunks))[::-1]
    for chunk in backwards:
        for away in range(1, pairs):
            far(chunk, away).start()
        side(chunk).start()
        if ship:

            @pl.when(ready)
            def _():
                ship_copy(chunk, tokens_ref.at[rows(chunk)]).start()

    for slot in range(2):
        for matrix in range(3):
            load(slot, matrix).wait()
        for chunk in backwards:
            if slot == 1:
                side(chunk).wait_recv()
            store(chunk, slot).start()
            value = tokens_ref[rows(chunk)] if slot == 0 else held[chunk, partner]
            add(chunk, slot, value)
    for slot in range(2, parts):
        for matrix in range(3):
            load(slot, matrix).wait()
    work.begin(exact(bias_ref[...], table_map(entries), 0))
    waiting = list(range(0, length, ROWS))
    for chunk in backwards:
        for away in range(1, pairs):
            far(chunk, away).wait_recv()
            relay(chunk, away).start()
            if ship:

                @pl.when(jnp.logical_not(ready))
                def _():
                    ship_copy(chunk, held.at[chunk, source(me, 1)]).start()

            store(chunk, 2 * away).start()
            add(chunk, 2 * away, held[chunk, source(me, away)])
        for away in range(1, pairs):
            relay(chunk, away).wait_recv()
            store(chunk, 2 * away + 1).start()
            add(chunk, 2 * away + 1, held[chunk, source(partner, away)])
        low = chunk * grain
        q_all[low : low + grain] = total[0, chunk].astype(jnp.bfloat16)
        k_all[REACH + low : REACH + low + grain] = total[1, chunk].astype(jnp.bfloat16)
        v_all[REACH + low : REACH + low + grain] = total[2, chunk].astype(jnp.bfloat16)
        if low == length - REACH:
            halo[0] = k_all[length:]
            halo[1] = v_all[length:]

            @pl.when(seat < seats - 1)
            def _():
                neighbour().start()

        while waiting and waiting[-1] >= low + REACH:
            work.attend(waiting.pop())

    @pl.when(seat > 0)
    def _():
        neighbour().wait_recv()

    @pl.when(seat == 0)
    def _():
        halo_got[...] = jnp.zeros_like(halo_got)

    k_all[:REACH] = halo_got[0]
    v_all[:REACH] = halo_got[1]
    while waiting:
        work.attend(waiting.pop())
    work.end(dk_ref, dv_ref, dk_tail_ref, dv_tail_ref, back_ref, line_ref)

    @pl.when(seat < seats - 1)
    def _():
        neighbour().wait_send()

    if ship:
        for chunk in backwards:
            ship_copy(chunk, tokens_ref.at[rows(chunk)]).wait_recv()
            pass_on(chunk).start()
            keep(chunk, core).start()
        for chunk in backwards:
            pass_on(chunk).wait_recv()
            keep(chunk, 1 - core).start()
        for chunk in backwards:
            ship_copy(chunk, tokens_ref.at[rows(chunk)]).wait_send()
            pass_on(chunk).wait_send()
            keep(chunk, core).wait()
            keep(chunk, 1 - core).wait()
    for chunk in backwards:
        side(chunk).wait_send()
        for away in range(1, pairs):
            far(chunk, away).wait_send()
            relay(chunk, away).wait_send()
        for slot in range(parts):
            store(chunk, slot).wait()


def attention_grads(tokens, query_weight, key_weight, value_weight, position_bias, out_grad):
    parts = lax.axis_size("tp")
    length, block = tokens.shape
    width = query_weight.shape[1]
    heads = position_bias.shape[0]
    chunks = length // GRAIN
    pairs = parts // 2
    body = length - REACH
    vmem = pl.BlockSpec(memory_space=pltpu.VMEM)
    anywhere = pl.BlockSpec(memory_space=pl.ANY)
    low = jnp.bfloat16

    def shape(kind, *sizes):
        return jax.ShapeDtypeStruct(sizes, kind)

    dma = pltpu.SemaphoreType.DMA
    ship = paired(lax.axis_size("sp"), parts)
    extra = []
    if ship:
        extra = [
            pltpu.VMEM((chunks, 2, GRAIN, block), jnp.bfloat16),
            dma((chunks,)),
            dma((chunks,)),
            dma((chunks,)),
            dma((chunks,)),
            dma((chunks, 2)),
        ]
    return pl.pallas_call(
        functools.partial(gather_kernel, parts),
        in_specs=[vmem, anywhere, anywhere, anywhere, vmem, vmem],
        out_specs=[anywhere] * 2 + [vmem] * 7,
        out_shape=[
            shape(low, length, block * parts),
            shape(low, *((length, 2 * block) if ship else (8, LANES))),
            shape(low, length, width),
            shape(low, body, width),
            shape(low, body, width),
            shape(jnp.float32, REACH, width),
            shape(jnp.float32, REACH, width),
            shape(low, 2, REACH, width),
            shape(jnp.float32, heads, TABLE),
        ],
        scratch_shapes=[
            pltpu.VMEM((chunks, parts, GRAIN, block), low),
            pltpu.VMEM((parts, 3, block, width), jnp.bfloat16),
            pltpu.VMEM((3, chunks, GRAIN, width), jnp.float32),
            pltpu.VMEM((2, REACH, width), low),
            pltpu.VMEM((2, REACH, width), low),
            pltpu.VMEM((length, width), low),
            pltpu.VMEM((length + REACH, width), low),
            pltpu.VMEM((length + REACH, width), low),
            pltpu.VMEM((heads, ROWS, WINDOW), jnp.float32),
            pltpu.VMEM((heads, ROWS, WINDOW), jnp.float32),
            pltpu.VMEM((length + REACH, width), jnp.float32),
            pltpu.VMEM((length + REACH, width), jnp.float32),
            dma((chunks,)),
            dma((chunks,)),
            dma((chunks, pairs - 1)),
            dma((chunks, pairs - 1)),
            dma((chunks, pairs - 1)),
            dma((chunks, pairs - 1)),
            dma(()),
            dma(()),
            dma((parts, 3)),
            dma((chunks, parts)),
        ]
        + extra,
        compiler_params=pltpu.CompilerParams(
            collective_id=1, has_side_effects=True, vmem_limit_bytes=56 * 1024 * 1024
        ),
        cost_estimate=pl.CostEstimate(
            flops=6 * length * block * parts * width, bytes_accessed=150_000_000, transcendentals=0
        ),
    )(tokens, query_weight, key_weight, value_weight, out_grad, position_bias)


def shards(tokens, query_weight, key_weight, value_weight, position_bias, out_grad):
    outs = attention_grads(
        tokens, query_weight, key_weight, value_weight, position_bias, out_grad
    )
    whole, theirs, query_grad, key_body, value_body, key_tail, value_tail, back, lines = outs
    return final_grads(
        whole,
        (theirs,) if paired(lax.axis_size("sp"), lax.axis_size("tp")) else (),
        (query_grad, key_body, value_body),
        (key_tail, value_tail),
        back,
        lines,
        (query_weight, key_weight, value_weight),
        position_bias.shape[1],
    )


def solution(mesh):
    in_specs = (
        P("sp", "tp"),
        P(None, "tp"),
        P(None, "tp"),
        P(None, "tp"),
        P("tp", None),
        P("sp", "tp"),
    )
    out_specs = (P("sp", "tp"), P("sp", "tp"), P("sp", "tp"), P("sp", "tp"), P("tp", None))
    return jax.shard_map(shards, mesh=mesh, in_specs=in_specs, out_specs=out_specs, check_vma=False)
```

```python
import functools

import jax
import jax.numpy as jnp
from jax import lax
from jax.experimental import pallas as pl
from jax.experimental.pallas import tpu as pltpu
from jax.sharding import PartitionSpec as P

SEGMENT = 64
PREVIOUS = 4
CLIP = 256
ROWS = 2 * SEGMENT
REACH = PREVIOUS * SEGMENT
WINDOW = ROWS + REACH
TABLE = 512
LANES = 128
GRAIN = 128
HIDDEN = -1e30


def contract_rows(left, right):
    return lax.dot_general(
        left, right, (((0,), (0,)), ((), ())), preferred_element_type=jnp.float32
    )


def contract_cols(left, right):
    return lax.dot_general(
        left, right, (((1,), (1,)), ((), ())), preferred_element_type=jnp.float32
    )


def diagonal_sums(tile):
    half = tile.shape[0] // 2
    while half >= 8:
        tile = tile[:half] + pltpu.roll(tile[half:], TABLE - half, 1)
        half //= 2
    row = lax.broadcasted_iota(jnp.int32, tile.shape, 0)
    for step in (4, 2, 1):
        tile = jnp.where((row & step) != 0, pltpu.roll(tile, TABLE - step, 1), tile)
    return jnp.sum(tile, axis=0, keepdims=True)


def table_map(entries):
    entry = lax.broadcasted_iota(jnp.int32, (entries, TABLE), 0)
    column = lax.broadcasted_iota(jnp.int32, (entries, TABLE), 1)
    near = column + entry == entries - 1
    far = (column >= WINDOW) & (entry == entries - 1)
    return jnp.where(near | far, 1.0, 0.0).astype(jnp.float32)


def exact(left, right, axis):
    return lax.dot_general(
        left,
        right,
        (((1,), (axis,)), ((), ())),
        precision=lax.Precision.HIGHEST,
        preferred_element_type=jnp.float32,
    )


class Attention:
    def __init__(self, factor, heads, q_all, k_all, v_all, g_ref, dq_ref, scratch):
        self.factor, self.heads = factor, heads
        self.q_all, self.k_all, self.v_all = q_all, k_all, v_all
        self.g_ref, self.dq_ref = g_ref, dq_ref
        self.bias_all, self.bias_sum, self.dk_all, self.dv_all = scratch
        self.head = q_all.shape[1] // heads

    def begin(self, table_rows):
        self.dk_all[...] = jnp.zeros_like(self.dk_all)
        self.dv_all[...] = jnp.zeros_like(self.dv_all)
        self.bias_sum[...] = jnp.zeros_like(self.bias_sum)
        row = lax.broadcasted_iota(jnp.int32, (ROWS, WINDOW), 0) // SEGMENT
        column = lax.broadcasted_iota(jnp.int32, (ROWS, WINDOW), 1)
        behind = column // SEGMENT - row
        seen = (behind >= 0) & (behind <= PREVIOUS)
        for head in range(self.heads):
            table = jnp.broadcast_to(table_rows[head : head + 1], (ROWS, TABLE))
            bias = pltpu.roll(table, 0, 1, stride=1, stride_axis=0)[:, :WINDOW]
            self.bias_all[head] = jnp.where(seen, bias, HIDDEN)

    def attend(self, start):
        @pl.loop(0, self.heads)
        def _(head):
            columns = pl.ds(pl.multiple_of(head * self.head, self.head), self.head)
            rows = slice(start, start + ROWS)
            window = slice(start, start + WINDOW)
            q = self.q_all[rows, columns]
            g = self.g_ref[rows, columns]
            k = self.k_all[window, columns]
            v = self.v_all[window, columns]
            mask = self.bias_all[head]
            if start < REACH:
                first = jnp.where(lax.axis_index("sp") == 0, REACH - start, 0)
                column = lax.broadcasted_iota(jnp.int32, (ROWS, WINDOW), 1)
                mask = jnp.where(column < first, HIDDEN, mask)
            scores = contract_cols(q, k) * self.factor + mask
            top = jnp.max(scores, axis=1, keepdims=True)
            raised = jnp.exp(scores - top)
            weights = raised * (1.0 / jnp.sum(raised, axis=1, keepdims=True))
            prob_grad = contract_cols(g, v)
            delta = jnp.sum(weights * prob_grad, axis=1, keepdims=True)
            score_grad = weights * (prob_grad - delta)
            self.bias_sum[head] += score_grad
            low = score_grad.astype(jnp.bfloat16)
            dq = jnp.dot(low, k, preferred_element_type=jnp.float32) * self.factor
            self.dq_ref[rows, columns] = dq.astype(jnp.bfloat16)
            self.dk_all[window, columns] += contract_rows(low, q)
            self.dv_all[window, columns] += contract_rows(weights.astype(jnp.bfloat16), g)

    def behind(self, back):
        back[0] = (self.dk_all[:REACH] * self.factor).astype(jnp.bfloat16)
        back[1] = self.dv_all[:REACH].astype(jnp.bfloat16)

    def end(self, dk_ref, dv_ref, line_ref):
        length = self.q_all.shape[0]
        body = length - REACH
        dk_all, dv_all, factor = self.dk_all, self.dv_all, self.factor
        dk_ref[:body] = (dk_all[REACH:length] * factor).astype(jnp.bfloat16)
        dv_ref[:body] = dv_all[REACH:length].astype(jnp.bfloat16)
        for head in range(self.heads):
            blank = jnp.zeros((ROWS, TABLE - WINDOW), jnp.float32)
            padded = jnp.concatenate([self.bias_sum[head], blank], axis=1)
            line_ref[head : head + 1] = diagonal_sums(padded)

    def join(self, dk_ref, dv_ref, after):
        length = self.q_all.shape[0]
        dk = self.dk_all[length:] * self.factor + after[0].astype(jnp.float32)
        dk_ref[length - REACH :] = dk.astype(jnp.bfloat16)
        dv = self.dv_all[length:] + after[1].astype(jnp.float32)
        dv_ref[length - REACH :] = dv.astype(jnp.bfloat16)


def ring_columns(count):
    columns = 1
    while (2 * columns) ** 2 <= count:
        columns *= 2
    return columns


def ring_place(index, count):
    columns = ring_columns(count)
    rows = count // columns
    row, column = index // columns, index % columns
    above = rows - 1 - row
    across = jnp.where(above % 2 == 0, column - 1, columns - 1 - column)
    return jnp.where(column == 0, row, rows + above * (columns - 1) + across)


def ring_index(place, count):
    columns = ring_columns(count)
    rows = count // columns
    later = jnp.maximum(place - rows, 0)
    above, across = later // (columns - 1), later % (columns - 1)
    column = jnp.where(above % 2 == 0, 1 + across, columns - 1 - across)
    return jnp.where(place < rows, place * columns, (rows - 1 - above) * columns + column)


def remote(src, dst, send, recv, device):
    return pltpu.make_async_remote_copy(
        src_ref=src,
        dst_ref=dst,
        send_sem=send,
        recv_sem=recv,
        device_id=device,
        device_id_type=pl.DeviceIdType.MESH,
    )


def meet(count, parts):
    me = lax.axis_index("sp")
    seat = lax.axis_index("tp")
    barrier = pltpu.get_barrier_semaphore()
    for ahead in range(1, count):
        peer = lax.rem(me + ahead, count)
        pl.semaphore_signal(
            barrier, inc=1, device_id={"sp": peer}, device_id_type=pl.DeviceIdType.MESH
        )
    for ahead in range(1, parts):
        peer = lax.rem(seat + ahead, parts)
        pl.semaphore_signal(
            barrier, inc=1, device_id={"tp": peer}, device_id_type=pl.DeviceIdType.MESH
        )
    pl.semaphore_wait(barrier, count + parts - 2)


def final_loads(hbm, grads, weights, load_sem):
    dq_hbm, dk_hbm, dv_hbm, wq_hbm, wk_hbm, wv_hbm = hbm
    return [
        pltpu.make_async_copy(dq_hbm, grads.at[0], load_sem.at[0]),
        pltpu.make_async_copy(dk_hbm, grads.at[1], load_sem.at[1]),
        pltpu.make_async_copy(dv_hbm, grads.at[2], load_sem.at[2]),
        pltpu.make_async_copy(wq_hbm, weights.at[0], load_sem.at[3]),
        pltpu.make_async_copy(wk_hbm, weights.at[1], load_sem.at[4]),
        pltpu.make_async_copy(wv_hbm, weights.at[2], load_sem.at[5]),
    ]


class Lines:
    def __init__(self, count, line_ref, out_ref, lines, send, recv):
        self.me = lax.axis_index("sp")
        self.count = count
        self.line_ref, self.out_ref, self.lines = line_ref, out_ref, lines
        self.sems = (send, recv)

    def copy(self, ahead):
        return remote(
            self.line_ref,
            self.lines.at[ahead - 1],
            self.sems[0].at[ahead - 1],
            self.sems[1].at[ahead - 1],
            {"sp": lax.rem(self.me + ahead, self.count)},
        )

    def start(self):
        for ahead in range(1, self.count):
            self.copy(ahead).start()

    def finish(self):
        total = self.line_ref[...]
        for ahead in range(1, self.count):
            self.copy(ahead).wait()
            total = total + self.lines[ahead - 1]
        self.out_ref[...] = exact(total, table_map(self.out_ref.shape[1]), 1)


class InputGrad:
    def __init__(self, parts, grads, weights, input_ref, buffers, sems):
        self.seat = lax.axis_index("tp")
        self.core = lax.rem(self.seat, 2)
        self.row = self.seat // 2
        self.parts, self.pairs = parts, parts // 2
        self.grads, self.weights, self.input_ref = grads, weights, input_ref
        self.pair_sent, self.pair_got, self.cross_sent, self.cross_got, self.kept = buffers
        self.sems = sems
        self.block = input_ref.shape[1]
        self.bands = input_ref.shape[0] // REACH
        self.units = 2 * self.bands

    def rows(self, band):
        return pl.ds(pl.multiple_of(band * REACH, REACH), REACH)

    def part(self, band, target):
        block = pl.ds(pl.multiple_of(target * self.block, self.block), self.block)
        rows = self.rows(band)
        term = contract_cols(self.grads[0, rows], self.weights[0, block])
        term += contract_cols(self.grads[1, rows], self.weights[1, block])
        return term + contract_cols(self.grads[2, rows], self.weights[2, block])

    def pair_copy(self, band, away):
        return remote(
            self.pair_sent.at[band, away],
            self.pair_got.at[band, away],
            self.sems[0].at[band, away],
            self.sems[1].at[band, away],
            {"tp": self.seat + 1 - 2 * self.core},
        )

    def cross_copy(self, band, away):
        return remote(
            self.cross_sent.at[band, away - 1],
            self.cross_got.at[band, away - 1],
            self.sems[2].at[band, away - 1],
            self.sems[3].at[band, away - 1],
            {"tp": lax.rem(self.seat + 2 * away, self.parts)},
        )

    def to_partner(self, band):
        for away in range(self.pairs):
            target = 2 * lax.rem(self.row + away, self.pairs) + 1 - self.core
            self.pair_sent[band, away] = self.part(band, target).astype(jnp.bfloat16)
            self.pair_copy(band, away).start()

    def across(self, band):
        for away in range(1, self.pairs):
            term = self.part(band, lax.rem(self.seat + 2 * away, self.parts))
            self.pair_copy(band, away).wait_recv()
            term = term + self.pair_got[band, away].astype(jnp.float32)
            self.cross_sent[band, away - 1] = term.astype(jnp.bfloat16)
            self.cross_copy(band, away).start()
        term = self.part(band, self.seat)
        self.pair_copy(band, 0).wait_recv()
        self.kept[band] = term + self.pair_got[band, 0].astype(jnp.float32)

    def finish(self, band):
        term = self.kept[band]
        for away in range(1, self.pairs):
            self.cross_copy(band, away).wait_recv()
            term = term + self.cross_got[band, away - 1].astype(jnp.float32)
        self.input_ref[self.rows(band)] = term.astype(jnp.bfloat16)

    def work(self, unit):
        band = unit // 2

        @pl.when(lax.rem(unit, 2) == 0)
        def _():
            self.to_partner(band)

        @pl.when(lax.rem(unit, 2) == 1)
        def _():
            self.across(band)

        @pl.when((lax.rem(unit, 2) == 1) & (unit > 2))
        def _():
            self.finish(band - 1)

    def drain(self):
        @pl.loop(0, self.bands)
        def _(band):
            for away in range(self.pairs):
                self.pair_copy(band, away).wait_send()
            for away in range(1, self.pairs):
                self.cross_copy(band, away).wait_send()


def ring_kernel(
    count,
    parts,
    whole_hbm,
    dq_hbm,
    dk_hbm,
    dv_hbm,
    wq_hbm,
    wk_hbm,
    wv_hbm,
    line_ref,
    input_ref,
    oq_ref,
    ok_ref,
    ov_ref,
    line_out_ref,
    whole,
    grads,
    weights,
    lines,
    pair_sent,
    pair_got,
    cross_sent,
    cross_got,
    kept,
    load_sem,
    line_send,
    line_recv,
    pair_send,
    pair_recv,
    cross_send,
    cross_recv,
    sent,
    got,
    send_sem,
    recv_sem,
):
    me = lax.axis_index("sp")
    place = ring_place(me, count)
    hbm = (dq_hbm, dk_hbm, dv_hbm, wq_hbm, wk_hbm, wv_hbm)
    loads = final_loads(hbm, grads, weights, load_sem)
    loads.append(pltpu.make_async_copy(whole_hbm, whole, load_sem.at[6]))
    for load in loads:
        load.start()
    meet(count, parts)
    shared = Lines(count, line_ref, line_out_ref, lines, line_send, line_recv)
    buffers = (pair_sent, pair_got, cross_sent, cross_got, kept)
    sems = (pair_send, pair_recv, cross_send, cross_recv)
    grad_in = InputGrad(parts, grads, weights, input_ref, buffers, sems)

    outs = (oq_ref, ok_ref, ov_ref)
    half = got.shape[3]
    onward = (
        ring_index(lax.rem(place + 1, count), count),
        ring_index(lax.rem(place + count - 1, count), count),
    )

    def own(target, side, chain):
        start = pl.multiple_of((2 * ring_index(target, count) + side) * half, half)
        return contract_rows(whole[:, pl.ds(start, half)], grads[chain])

    def target_of(step, side):
        if side == 0:
            return lax.rem(place - 1 - step + 2 * count, count)
        return lax.rem(place + 1 + step, count)

    def copy_of(src, step, side, chain):
        return remote(
            src,
            got.at[side, chain, step],
            send_sem.at[side, chain, step],
            recv_sem.at[side, chain, step],
            {"sp": onward[side]},
        )

    for load in loads:
        load.wait()
    for chain in range(3):
        for side in range(2):
            sent[side, chain] = own(target_of(0, side), side, chain).astype(jnp.bfloat16)
            copy_of(sent.at[side, chain], 0, side, chain).start()
    shared.start()

    chains = [(chain, side) for chain in range(3) for side in range(2)]

    @pl.loop(1, count - 1)
    def _(step):
        for chain, side in chains:
            part_of = own(target_of(step, side), side, chain)
            place_of = got.at[side, chain, step - 1]
            copy_of(sent.at[side, chain], step - 1, side, chain).wait_recv()
            total = part_of + place_of[...].astype(jnp.float32)
            place_of[...] = total.astype(jnp.bfloat16)
            copy_of(place_of, step, side, chain).start()
            if (chain, side) == (1, 1):

                @pl.when(step <= grad_in.units)
                def _():
                    grad_in.work(step - 1)

    for unit in range(min(count - 2, grad_in.units), grad_in.units):
        grad_in.work(unit)
    shared.finish()
    for chain, side in chains:
        if (chain, side) == (2, 0):
            grad_in.finish(grad_in.bands - 1)
        part_of = own(place, side, chain)
        copy_of(sent.at[side, chain], count - 2, side, chain).wait_recv()
        total = part_of + got[side, chain, count - 2].astype(jnp.float32)
        outs[chain][side * half : (side + 1) * half] = total

    @pl.loop(0, count - 1)
    def _(step):
        for chain, side in chains:
            copy_of(sent.at[side, chain], step, side, chain).wait_send()

    grad_in.drain()


def paired(count, parts):
    return count == 8 and ring_columns(count) == 2 and parts == 4


def pair_places(me):
    level, side = me // 2, lax.rem(me, 2)
    inner = (level == 1) | (level == 2)
    near = level // 2
    made = jnp.where(inner, 1 - near, near)
    partner = 2 * (level + 1 - 2 * lax.rem(level, 2)) + side
    return level, side, inner, near, made, partner


def pair_kernel(
    count,
    parts,
    whole_hbm,
    dq_hbm,
    dk_hbm,
    dv_hbm,
    wq_hbm,
    wk_hbm,
    wv_hbm,
    theirs_hbm,
    line_ref,
    input_ref,
    oq_ref,
    ok_ref,
    ov_ref,
    line_out_ref,
    turned,
    grads,
    weights,
    lines,
    pair_sent,
    pair_got,
    cross_sent,
    cross_got,
    kept,
    load_sem,
    line_send,
    line_recv,
    pair_send,
    pair_recv,
    cross_send,
    cross_recv,
    theirs,
    their_grads,
    x_sent,
    x_got,
    sent,
    got,
    result,
    theirs_sem,
    swap_send,
    swap_recv,
    x_send,
    x_recv,
    send_sem,
    recv_sem,
    out_sem,
):
    me = lax.axis_index("sp")
    level, side, inner, near, made, partner = pair_places(me)
    hbm = (dq_hbm, dk_hbm, dv_hbm, wq_hbm, wk_hbm, wv_hbm)
    loads = final_loads(hbm, grads, weights, load_sem)
    bands, pairs, _, block = pair_sent.shape
    length = grads.shape[1]

    def rows(band):
        return pl.ds(band * REACH, REACH)

    def piece(band, part):
        start = pl.multiple_of((made * pairs + part) * block, block)
        return pltpu.make_async_copy(
            whole_hbm.at[rows(band), pl.ds(start, block)],
            pair_sent.at[band, part],
            theirs_sem.at[1 + band * pairs + part],
        )

    own_loads = [piece(band, part) for band in range(bands) for part in range(pairs)]
    loads[3:3] = own_loads + [pltpu.make_async_copy(theirs_hbm, theirs, theirs_sem.at[0])]
    for load in loads:
        load.start()
    meet(count, parts)
    shared = Lines(count, line_ref, line_out_ref, lines, line_send, line_recv)
    buffers = (pair_sent, pair_got, cross_sent, cross_got, kept)
    sems = (pair_send, pair_recv, cross_send, cross_recv)
    grad_in = InputGrad(parts, grads, weights, input_ref, buffers, sems)

    chunks, depth, tile = x_sent.shape[0], x_sent.shape[2], x_sent.shape[3]
    per = chunks // 3
    outs = (oq_ref, ok_ref, ov_ref)
    deep = 2 * (1 + made)
    rim = 6 * made
    slot = jnp.where(inner, 0, 1)

    def columns(chunk):
        return pl.ds(pl.multiple_of(lax.rem(chunk, per) * tile, tile), tile)

    def swap(chunk):
        return remote(
            grads.at[chunk // per, :, columns(chunk)],
            their_grads.at[chunk // per, :, columns(chunk)],
            swap_send.at[chunk],
            swap_recv.at[chunk],
            {"sp": partner},
        )

    def x_copy(chunk):
        return remote(
            x_sent.at[chunk],
            x_got.at[chunk],
            x_send.at[chunk],
            x_recv.at[chunk],
            {"sp": 2 * level + 1 - side},
        )

    def deep_copy(chunk):
        return remote(
            sent.at[0, chunk],
            got.at[slot, chunk],
            send_sem.at[0, chunk],
            recv_sem.at[slot, chunk],
            {"sp": deep + side},
        )

    def rim_copy(chunk):
        return remote(
            sent.at[1, chunk],
            got.at[0, chunk],
            send_sem.at[1, chunk],
            recv_sem.at[0, chunk],
            {"sp": rim + side},
        )

    def arrived(chunk, which):
        return remote(
            sent.at[0, chunk],
            got.at[which, chunk],
            send_sem.at[0, chunk],
            recv_sem.at[which, chunk],
            {"sp": deep + side},
        )

    def sums(target, chunk):
        start = pl.multiple_of((target - made * (count // 2)) * depth, depth)
        features = pl.ds(start, depth)
        mine = grads[chunk // per, :, columns(chunk)]
        other = their_grads[chunk // per, :, columns(chunk)]
        term = jnp.dot(turned[features, :length], mine, preferred_element_type=jnp.float32)
        return term + jnp.dot(
            turned[features, length:], other, preferred_element_type=jnp.float32
        )

    def halve(chunk):
        swap(chunk).wait_recv()
        x_sent[chunk, 0] = sums(deep + 1 - side, chunk).astype(jnp.bfloat16)
        x_sent[chunk, 1] = sums(rim + 1 - side, chunk).astype(jnp.bfloat16)
        x_copy(chunk).start()

    def onward(chunk):
        term = sums(deep + side, chunk)
        x_copy(chunk).wait_recv()
        term = term + x_got[chunk, 0].astype(jnp.float32)
        sent[0, chunk] = term.astype(jnp.bfloat16)
        deep_copy(chunk).start()
        term = sums(rim + side, chunk) + x_got[chunk, 1].astype(jnp.float32)

        @pl.when(inner)
        def _():
            sent[1, chunk] = term.astype(jnp.bfloat16)
            rim_copy(chunk).start()

        @pl.when(jnp.logical_not(inner))
        def _():
            result[chunk // per, :, columns(chunk)] = term

    def store(chunk, matrix):
        return pltpu.make_async_copy(
            result.at[matrix, :, columns(chunk)],
            outs[matrix].at[:, columns(chunk)],
            out_sem.at[chunk],
        )

    def finish(chunk):
        arrived(chunk, 0).wait_recv()
        term = got[0, chunk].astype(jnp.float32)

        @pl.when(inner)
        def _():
            arrived(chunk, 1).wait_recv()
            total = term + got[1, chunk].astype(jnp.float32)
            result[chunk // per, :, columns(chunk)] = total

        @pl.when(jnp.logical_not(inner))
        def _():
            total = term + result[chunk // per, :, columns(chunk)]
            result[chunk // per, :, columns(chunk)] = total

        for matrix in range(3):

            @pl.when(chunk // per == matrix)
            def _():
                store(chunk, matrix).start()

    for which in range(3):
        loads[which].wait()
        for chunk in range(per):
            swap(which * per + chunk).start()
    for load in loads[3:]:
        load.wait()
    shared.start()

    @pl.loop(0, bands)
    def _(band):
        start = pl.multiple_of(band * REACH, REACH)
        for part in range(pairs):
            low = slice(part * block, (part + 1) * block)
            turned[low, pl.ds(start, REACH)] = pair_sent[band, part].T
            turned[low, pl.ds(length + start, REACH)] = theirs[pl.ds(start, REACH), low].T

    hold = 2
    lag = 3 * chunks // 4

    @pl.loop(0, chunks + lag)
    def _(step):
        @pl.when(step < chunks)
        def _():
            halve(step)

        @pl.when((step >= hold) & (step < chunks + hold))
        def _():
            onward(step - hold)

        @pl.when(step >= lag)
        def _():
            finish(step - lag)

        unit = (step - 1) // 2

        @pl.when((lax.rem(step, 2) == 1) & (unit < grad_in.units))
        def _():
            grad_in.work(unit)

    for unit in range(min((chunks + lag) // 2, grad_in.units), grad_in.units):
        grad_in.work(unit)
    shared.finish()
    grad_in.finish(grad_in.bands - 1)
    @pl.loop(0, chunks)
    def _(chunk):
        swap(chunk).wait_send()
        x_copy(chunk).wait_send()
        deep_copy(chunk).wait_send()
        store(chunk, 0).wait()

        @pl.when(inner)
        def _():
            rim_copy(chunk).wait_send()

    grad_in.drain()


def final_grads(whole, theirs, grads, lines, weights, entries):
    count = lax.axis_size("sp")
    parts = lax.axis_size("tp")
    pairs = parts // 2
    length, features = whole.shape
    width = weights[0].shape[1]
    depth = features // count
    block = features // parts
    bands = length // REACH
    vmem = pl.BlockSpec(memory_space=pltpu.VMEM)
    anywhere = pl.BlockSpec(memory_space=pl.ANY)
    out = jax.ShapeDtypeStruct((depth, width), jnp.float32)
    dma = pltpu.SemaphoreType.DMA
    low = jnp.bfloat16
    pair = paired(count, parts)
    tile = min(width, LANES)
    chunks = 3 * width // tile
    scratch = [
        pltpu.VMEM((features // 2, 2 * length) if pair else (length, features), low),
        pltpu.VMEM((3, length, width), low),
        pltpu.VMEM((3, features, width), low),
        pltpu.VMEM((count - 1,) + lines.shape, jnp.float32),
        pltpu.VMEM((bands, pairs, REACH, block), low),
        pltpu.VMEM((bands, pairs, REACH, block), low),
        pltpu.VMEM((bands, pairs - 1, REACH, block), low),
        pltpu.VMEM((bands, pairs - 1, REACH, block), low),
        pltpu.VMEM((bands, REACH, block), jnp.float32),
        dma((7,)),
        dma((count - 1,)),
        dma((count - 1,)),
        dma((bands, pairs)),
        dma((bands, pairs)),
        dma((bands, pairs - 1)),
        dma((bands, pairs - 1)),
    ]
    if pair:
        scratch += [
            pltpu.VMEM((length, features // 2), low),
            pltpu.VMEM((3, length, width), low),
            pltpu.VMEM((chunks, 2, depth, tile), low),
            pltpu.VMEM((chunks, 2, depth, tile), low),
            pltpu.VMEM((2, chunks, depth, tile), low),
            pltpu.VMEM((2, chunks, depth, tile), low),
            pltpu.VMEM((3, depth, width), jnp.float32),
            dma((1 + bands * pairs,)),
            dma((chunks,)),
            dma((chunks,)),
            dma((chunks,)),
            dma((chunks,)),
            dma((2, chunks)),
            dma((2, chunks)),
            dma((chunks,)),
        ]
    else:
        scratch += [
            pltpu.VMEM((2, 3, depth // 2, width), low),
            pltpu.VMEM((2, 3, count - 1, depth // 2, width), low),
            dma((2, 3, count - 1)),
            dma((2, 3, count - 1)),
        ]
    place = anywhere if pair else vmem
    return pl.pallas_call(
        functools.partial(pair_kernel if pair else ring_kernel, count, parts),
        in_specs=[anywhere] * (7 + pair) + [vmem],
        out_specs=[vmem] + [place] * 3 + [vmem],
        out_shape=[
            jax.ShapeDtypeStruct((length, block), low),
            out,
            out,
            out,
            jax.ShapeDtypeStruct((lines.shape[0], entries), jnp.float32),
        ],
        scratch_shapes=scratch,
        compiler_params=pltpu.CompilerParams(
            collective_id=0, has_side_effects=True, vmem_limit_bytes=63 * 1024 * 1024
        ),
        cost_estimate=pl.CostEstimate(
            flops=12 * length * features * width,
            bytes_accessed=400_000_000,
            transcendentals=0,
        ),
    )(whole, *grads, *weights, *theirs, lines)


def gather_kernel(
    parts,
    tokens_ref,
    wq_ref,
    wk_ref,
    wv_ref,
    g_ref,
    bias_ref,
    whole_ref,
    theirs_ref,
    dq_ref,
    dk_ref,
    dv_ref,
    line_ref,
    held,
    weights,
    total,
    halo,
    halo_got,
    back,
    after,
    q_all,
    k_all,
    v_all,
    bias_all,
    bias_sum,
    dk_all,
    dv_all,
    side_send,
    side_recv,
    far_send,
    far_recv,
    relay_send,
    relay_recv,
    halo_send,
    halo_recv,
    back_send,
    back_recv,
    load_sem,
    store_sem,
    *ship_refs,
):
    me = lax.axis_index("tp")
    seat = lax.axis_index("sp")
    seats = lax.axis_size("sp")
    partner = me + 1 - 2 * lax.rem(me, 2)
    chunks = held.shape[0]
    block = tokens_ref.shape[1]
    grain = held.shape[2]
    length = tokens_ref.shape[0]
    heads, entries = bias_ref.shape
    pairs = parts // 2
    matrices = (wq_ref, wk_ref, wv_ref)

    def source(device, away):
        return lax.rem(device + parts - 2 * away, parts)

    order = [me, partner]
    for away in range(1, pairs):
        order += [source(me, away), source(partner, away)]

    def load(slot, matrix):
        start = pl.multiple_of(order[slot] * block, block)
        return pltpu.make_async_copy(
            matrices[matrix].at[pl.ds(start, block)],
            weights.at[slot, matrix],
            load_sem.at[slot, matrix],
        )

    for slot in range(parts):
        for matrix in range(3):
            load(slot, matrix).start()

    barrier = pltpu.get_barrier_semaphore()
    for ahead in range(1, parts):
        pl.semaphore_signal(
            barrier,
            inc=1,
            device_id={"tp": lax.rem(me + ahead, parts)},
            device_id_type=pl.DeviceIdType.MESH,
        )
    onward = lax.rem(seat + 1, seats)
    for other in (onward, lax.rem(seat + seats - 1, seats)):
        pl.semaphore_signal(
            barrier, inc=1, device_id={"sp": other}, device_id_type=pl.DeviceIdType.MESH
        )
    ship = len(ship_refs) > 0
    if ship:
        level, lane, inner, near, made, mate = pair_places(seat)
        pl.semaphore_signal(
            barrier, inc=1, device_id={"sp": mate}, device_id_type=pl.DeviceIdType.MESH
        )
    pl.semaphore_wait(barrier, parts + 1 + ship)

    def rows(chunk):
        return pl.ds(chunk * grain, grain)

    def far(chunk, away):
        return remote(
            tokens_ref.at[rows(chunk)],
            held.at[chunk, me],
            far_send.at[chunk, away - 1],
            far_recv.at[chunk, away - 1],
            {"tp": lax.rem(me + 2 * away, parts)},
        )

    def side(chunk):
        return remote(
            tokens_ref.at[rows(chunk)],
            held.at[chunk, me],
            side_send.at[chunk],
            side_recv.at[chunk],
            {"tp": partner},
        )

    def relay(chunk, away):
        place = held.at[chunk, source(me, away)]
        return remote(
            place,
            place,
            relay_send.at[chunk, away - 1],
            relay_recv.at[chunk, away - 1],
            {"tp": partner},
        )

    def neighbour():
        return remote(halo, halo_got, halo_send, halo_recv, {"sp": onward})

    def behind():
        device = {"sp": lax.rem(seat + seats - 1, seats)}
        return remote(back, after, back_send, back_recv, device)

    scratch = (bias_all, bias_sum, dk_all, dv_all)
    factor = (q_all.shape[1] // heads) ** (-0.5)
    work = Attention(factor, heads, q_all, k_all, v_all, g_ref, dq_ref, scratch)

    def store(chunk, slot):
        start = pl.multiple_of(order[slot] * block, block)
        src = tokens_ref.at[rows(chunk)] if slot == 0 else held.at[chunk, order[slot]]
        return pltpu.make_async_copy(
            src, whole_ref.at[rows(chunk), pl.ds(start, block)], store_sem.at[chunk, slot]
        )

    def add(chunk, slot, value):
        for matrix in range(3):
            term = jnp.dot(value, weights[slot, matrix], preferred_element_type=jnp.float32)
            if slot == 0:
                total[matrix, chunk] = term
            else:
                total[matrix, chunk] += term

    if ship:
        ship_got, ship_send, ship_recv, pass_send, pass_recv, keep_sem = ship_refs
        core = lax.rem(me, 2)
        shipped = jnp.where(inner, near, 1 - near)
        ready = me // 2 == shipped

        def ship_copy(chunk, src):
            return remote(
                src,
                ship_got.at[chunk, core],
                ship_send.at[chunk],
                ship_recv.at[chunk],
                {"sp": mate},
            )

        def pass_on(chunk):
            place = ship_got.at[chunk, core]
            return remote(
                place, place, pass_send.at[chunk], pass_recv.at[chunk], {"tp": partner}
            )

        def keep(chunk, which):
            start = pl.multiple_of(which * block, block)
            return pltpu.make_async_copy(
                ship_got.at[chunk, which],
                theirs_ref.at[rows(chunk), pl.ds(start, block)],
                keep_sem.at[chunk, which],
            )

    tail = REACH // grain
    sequence = list(range(chunks - tail, chunks)) + list(range(chunks - tail))
    for chunk in sequence:
        for away in range(1, pairs):
            far(chunk, away).start()
        side(chunk).start()
    for slot in range(2):
        for matrix in range(3):
            load(slot, matrix).wait()
        for chunk in sequence:
            if slot == 1:
                side(chunk).wait_recv()
            store(chunk, slot).start()
            value = tokens_ref[rows(chunk)] if slot == 0 else held[chunk, partner]
            add(chunk, slot, value)
    for slot in range(2, parts):
        for matrix in range(3):
            load(slot, matrix).wait()
    work.begin(exact(bias_ref[...], table_map(entries), 0))
    done = []
    waiting = list(range(0, length, ROWS))

    def attend_ready(early):
        known = {row for chunk in done for row in range(chunk * grain, (chunk + 1) * grain, ROWS)}
        for start in list(waiting):
            needs = range(max(0, start - REACH), start + ROWS, ROWS)
            if start < REACH and early:
                continue
            if set(needs) <= known:
                if start == 0:
                    take_halo()
                work.attend(start)
                waiting.remove(start)
                if start == REACH - ROWS:
                    send_behind()

    def take_halo():
        @pl.when(seat > 0)
        def _():
            neighbour().wait_recv()

        @pl.when(seat == 0)
        def _():
            halo_got[...] = jnp.zeros_like(halo_got)

        k_all[:REACH] = halo_got[0]
        v_all[:REACH] = halo_got[1]

    def send_behind():
        @pl.when(seat > 0)
        def _():
            work.behind(back)
            behind().start()

    for chunk in sequence:
        for away in range(1, pairs):
            far(chunk, away).wait_recv()
            relay(chunk, away).start()
            if ship:

                @pl.when(ready)
                def _():
                    ship_copy(chunk, tokens_ref.at[rows(chunk)]).start()

                @pl.when(jnp.logical_not(ready))
                def _():
                    ship_copy(chunk, held.at[chunk, source(me, 1)]).start()

            store(chunk, 2 * away).start()
            add(chunk, 2 * away, held[chunk, source(me, away)])
        for away in range(1, pairs):
            relay(chunk, away).wait_recv()
            store(chunk, 2 * away + 1).start()
            add(chunk, 2 * away + 1, held[chunk, source(partner, away)])
        low = chunk * grain
        q_all[low : low + grain] = total[0, chunk].astype(jnp.bfloat16)
        k_all[REACH + low : REACH + low + grain] = total[1, chunk].astype(jnp.bfloat16)
        v_all[REACH + low : REACH + low + grain] = total[2, chunk].astype(jnp.bfloat16)
        done.append(chunk)
        if chunk == chunks - 1:
            halo[0] = k_all[length:]
            halo[1] = v_all[length:]

            @pl.when(seat < seats - 1)
            def _():
                neighbour().start()

        attend_ready(len(done) < chunks - 1)
    attend_ready(False)
    work.end(dk_ref, dv_ref, line_ref)

    @pl.when(seat < seats - 1)
    def _():
        behind().wait_recv()

    @pl.when(seat == seats - 1)
    def _():
        after[...] = jnp.zeros_like(after)

    work.join(dk_ref, dv_ref, after)

    @pl.when(seat > 0)
    def _():
        behind().wait_send()

    @pl.when(seat < seats - 1)
    def _():
        neighbour().wait_send()

    if ship:
        for chunk in sequence:
            ship_copy(chunk, tokens_ref.at[rows(chunk)]).wait_recv()
            pass_on(chunk).start()
            keep(chunk, core).start()
        for chunk in sequence:
            pass_on(chunk).wait_recv()
            keep(chunk, 1 - core).start()
        for chunk in sequence:
            ship_copy(chunk, tokens_ref.at[rows(chunk)]).wait_send()
            pass_on(chunk).wait_send()
            keep(chunk, core).wait()
            keep(chunk, 1 - core).wait()
    for chunk in sequence:
        side(chunk).wait_send()
        for away in range(1, pairs):
            far(chunk, away).wait_send()
            relay(chunk, away).wait_send()
        for slot in range(parts):
            store(chunk, slot).wait()


def attention_grads(tokens, query_weight, key_weight, value_weight, position_bias, out_grad):
    parts = lax.axis_size("tp")
    length, block = tokens.shape
    width = query_weight.shape[1]
    heads = position_bias.shape[0]
    chunks = length // GRAIN
    pairs = parts // 2
    vmem = pl.BlockSpec(memory_space=pltpu.VMEM)
    anywhere = pl.BlockSpec(memory_space=pl.ANY)
    low = jnp.bfloat16

    def shape(kind, *sizes):
        return jax.ShapeDtypeStruct(sizes, kind)

    dma = pltpu.SemaphoreType.DMA
    ship = paired(lax.axis_size("sp"), parts)
    extra = []
    if ship:
        extra = [
            pltpu.VMEM((chunks, 2, GRAIN, block), jnp.bfloat16),
            dma((chunks,)),
            dma((chunks,)),
            dma((chunks,)),
            dma((chunks,)),
            dma((chunks, 2)),
        ]
    return pl.pallas_call(
        functools.partial(gather_kernel, parts),
        in_specs=[vmem, anywhere, anywhere, anywhere, vmem, vmem],
        out_specs=[anywhere] * 2 + [vmem] * 4,
        out_shape=[
            shape(low, length, block * parts),
            shape(low, *((length, 2 * block) if ship else (8, LANES))),
            shape(low, length, width),
            shape(low, length, width),
            shape(low, length, width),
            shape(jnp.float32, heads, TABLE),
        ],
        scratch_shapes=[
            pltpu.VMEM((chunks, parts, GRAIN, block), low),
            pltpu.VMEM((parts, 3, block, width), jnp.bfloat16),
            pltpu.VMEM((3, chunks, GRAIN, width), jnp.float32),
            pltpu.VMEM((2, REACH, width), low),
            pltpu.VMEM((2, REACH, width), low),
            pltpu.VMEM((2, REACH, width), low),
            pltpu.VMEM((2, REACH, width), low),
            pltpu.VMEM((length, width), low),
            pltpu.VMEM((length + REACH, width), low),
            pltpu.VMEM((length + REACH, width), low),
            pltpu.VMEM((heads, ROWS, WINDOW), jnp.float32),
            pltpu.VMEM((heads, ROWS, WINDOW), jnp.float32),
            pltpu.VMEM((length + REACH, width), jnp.float32),
            pltpu.VMEM((length + REACH, width), jnp.float32),
            dma((chunks,)),
            dma((chunks,)),
            dma((chunks, pairs - 1)),
            dma((chunks, pairs - 1)),
            dma((chunks, pairs - 1)),
            dma((chunks, pairs - 1)),
            dma(()),
            dma(()),
            dma(()),
            dma(()),
            dma((parts, 3)),
            dma((chunks, parts)),
        ]
        + extra,
        compiler_params=pltpu.CompilerParams(
            collective_id=1, has_side_effects=True, vmem_limit_bytes=56 * 1024 * 1024
        ),
        cost_estimate=pl.CostEstimate(
            flops=6 * length * block * parts * width, bytes_accessed=150_000_000, transcendentals=0
        ),
    )(tokens, query_weight, key_weight, value_weight, out_grad, position_bias)


def shards(tokens, query_weight, key_weight, value_weight, position_bias, out_grad):
    outs = attention_grads(
        tokens, query_weight, key_weight, value_weight, position_bias, out_grad
    )
    whole, theirs, query_grad, key_grad, value_grad, lines = outs
    *large, bias_grad = final_grads(
        whole,
        (theirs,) if paired(lax.axis_size("sp"), lax.axis_size("tp")) else (),
        (query_grad, key_grad, value_grad),
        lines,
        (query_weight, key_weight, value_weight),
        position_bias.shape[1],
    )
    return (*hand_on(large), bias_grad)


def hand_kernel(*refs):
    half = len(refs) // 2
    for source, target in zip(refs[:half], refs[half:]):
        target[...] = source[...]


def hand_on(arrays, steps=4):
    specs = [
        pl.BlockSpec((array.shape[0] // steps, array.shape[1]), lambda i: (i, 0))
        for array in arrays
    ]
    size = sum(2 * array.size * array.dtype.itemsize for array in arrays)
    return pl.pallas_call(
        hand_kernel,
        grid=(steps,),
        in_specs=specs,
        out_specs=specs,
        out_shape=[jax.ShapeDtypeStruct(array.shape, array.dtype) for array in arrays],
        cost_estimate=pl.CostEstimate(flops=0, bytes_accessed=size, transcendentals=0),
    )(*arrays)


def solution(mesh):
    in_specs = (
        P("sp", "tp"),
        P(None, "tp"),
        P(None, "tp"),
        P(None, "tp"),
        P("tp", None),
        P("sp", "tp"),
    )
    out_specs = (P("sp", "tp"), P("sp", "tp"), P("sp", "tp"), P("sp", "tp"), P("tp", None))
    return jax.shard_map(shards, mesh=mesh, in_specs=in_specs, out_specs=out_specs, check_vma=False)
```

```python
import functools

import jax
import jax.numpy as jnp
from jax import lax
from jax.experimental import pallas as pl
from jax.experimental.pallas import tpu as pltpu
from jax.sharding import PartitionSpec as P

SEGMENT = 64
PREVIOUS = 4
CLIP = 256
ROWS = 2 * SEGMENT
REACH = PREVIOUS * SEGMENT
WINDOW = ROWS + REACH
TABLE = 512
LANES = 128
GRAIN = 128
HIDDEN = -1e30


def contract_rows(left, right):
    return lax.dot_general(
        left, right, (((0,), (0,)), ((), ())), preferred_element_type=jnp.float32
    )


def contract_cols(left, right):
    return lax.dot_general(
        left, right, (((1,), (1,)), ((), ())), preferred_element_type=jnp.float32
    )


def diagonal_sums(tile):
    half = tile.shape[0] // 2
    while half >= 8:
        tile = tile[:half] + pltpu.roll(tile[half:], TABLE - half, 1)
        half //= 2
    row = lax.broadcasted_iota(jnp.int32, tile.shape, 0)
    for step in (4, 2, 1):
        tile = jnp.where((row & step) != 0, pltpu.roll(tile, TABLE - step, 1), tile)
    return jnp.sum(tile, axis=0, keepdims=True)


def table_map(entries):
    entry = lax.broadcasted_iota(jnp.int32, (entries, TABLE), 0)
    column = lax.broadcasted_iota(jnp.int32, (entries, TABLE), 1)
    near = column + entry == entries - 1
    far = (column >= WINDOW) & (entry == entries - 1)
    return jnp.where(near | far, 1.0, 0.0).astype(jnp.float32)


def exact(left, right, axis):
    return lax.dot_general(
        left,
        right,
        (((1,), (axis,)), ((), ())),
        precision=lax.Precision.HIGHEST,
        preferred_element_type=jnp.float32,
    )


class Attention:
    def __init__(self, factor, heads, q_all, k_all, v_all, g_ref, dq_ref, scratch):
        self.factor, self.heads = factor, heads
        self.q_all, self.k_all, self.v_all = q_all, k_all, v_all
        self.g_ref, self.dq_ref = g_ref, dq_ref
        self.bias_all, self.bias_sum, self.dk_all, self.dv_all = scratch
        self.head = q_all.shape[1] // heads

    def begin(self, table_rows):
        self.dk_all[...] = jnp.zeros_like(self.dk_all)
        self.dv_all[...] = jnp.zeros_like(self.dv_all)
        self.bias_sum[...] = jnp.zeros_like(self.bias_sum)
        row = lax.broadcasted_iota(jnp.int32, (ROWS, WINDOW), 0) // SEGMENT
        column = lax.broadcasted_iota(jnp.int32, (ROWS, WINDOW), 1)
        behind = column // SEGMENT - row
        seen = (behind >= 0) & (behind <= PREVIOUS)
        for head in range(self.heads):
            table = jnp.broadcast_to(table_rows[head : head + 1], (ROWS, TABLE))
            bias = pltpu.roll(table, 0, 1, stride=1, stride_axis=0)[:, :WINDOW]
            self.bias_all[head] = jnp.where(seen, bias, HIDDEN)

    def attend(self, start):
        @pl.loop(0, self.heads, unroll=2)
        def _(head):
            columns = pl.ds(pl.multiple_of(head * self.head, self.head), self.head)
            rows = slice(start, start + ROWS)
            window = slice(start, start + WINDOW)
            q = self.q_all[rows, columns]
            g = self.g_ref[rows, columns]
            k = self.k_all[window, columns]
            v = self.v_all[window, columns]
            mask = self.bias_all[head]
            if start < REACH:
                first = jnp.where(lax.axis_index("sp") == 0, REACH - start, 0)
                column = lax.broadcasted_iota(jnp.int32, (ROWS, WINDOW), 1)
                mask = jnp.where(column < first, HIDDEN, mask)
            scores = contract_cols(q, k) * self.factor + mask
            top = jnp.max(scores, axis=1, keepdims=True)
            raised = jnp.exp(scores - top)
            weights = raised * (1.0 / jnp.sum(raised, axis=1, keepdims=True))
            prob_grad = contract_cols(g, v)
            delta = jnp.sum(weights * prob_grad, axis=1, keepdims=True)
            score_grad = weights * (prob_grad - delta)
            self.bias_sum[head] += score_grad
            low = score_grad.astype(jnp.bfloat16)
            dq = jnp.dot(low, k, preferred_element_type=jnp.float32) * self.factor
            self.dq_ref[rows, columns] = dq.astype(jnp.bfloat16)
            self.dk_all[window, columns] += contract_rows(low, q)
            self.dv_all[window, columns] += contract_rows(weights.astype(jnp.bfloat16), g)

    def behind(self, back):
        back[0] = (self.dk_all[:REACH] * self.factor).astype(jnp.bfloat16)
        back[1] = self.dv_all[:REACH].astype(jnp.bfloat16)

    def end(self, dk_ref, dv_ref, line_ref):
        length = self.q_all.shape[0]
        body = length - REACH
        dk_all, dv_all, factor = self.dk_all, self.dv_all, self.factor
        dk_ref[:body] = (dk_all[REACH:length] * factor).astype(jnp.bfloat16)
        dv_ref[:body] = dv_all[REACH:length].astype(jnp.bfloat16)
        for head in range(self.heads):
            blank = jnp.zeros((ROWS, TABLE - WINDOW), jnp.float32)
            padded = jnp.concatenate([self.bias_sum[head], blank], axis=1)
            line_ref[head : head + 1] = diagonal_sums(padded)

    def join(self, dk_ref, dv_ref, after):
        length = self.q_all.shape[0]
        dk = self.dk_all[length:] * self.factor + after[0].astype(jnp.float32)
        dk_ref[length - REACH :] = dk.astype(jnp.bfloat16)
        dv = self.dv_all[length:] + after[1].astype(jnp.float32)
        dv_ref[length - REACH :] = dv.astype(jnp.bfloat16)


def ring_columns(count):
    columns = 1
    while (2 * columns) ** 2 <= count:
        columns *= 2
    return columns


def ring_place(index, count):
    columns = ring_columns(count)
    rows = count // columns
    row, column = index // columns, index % columns
    above = rows - 1 - row
    across = jnp.where(above % 2 == 0, column - 1, columns - 1 - column)
    return jnp.where(column == 0, row, rows + above * (columns - 1) + across)


def ring_index(place, count):
    columns = ring_columns(count)
    rows = count // columns
    later = jnp.maximum(place - rows, 0)
    above, across = later // (columns - 1), later % (columns - 1)
    column = jnp.where(above % 2 == 0, 1 + across, columns - 1 - across)
    return jnp.where(place < rows, place * columns, (rows - 1 - above) * columns + column)


def remote(src, dst, send, recv, device):
    return pltpu.make_async_remote_copy(
        src_ref=src,
        dst_ref=dst,
        send_sem=send,
        recv_sem=recv,
        device_id=device,
        device_id_type=pl.DeviceIdType.MESH,
    )


def meet(count, parts):
    me = lax.axis_index("sp")
    seat = lax.axis_index("tp")
    barrier = pltpu.get_barrier_semaphore()
    for ahead in range(1, count):
        peer = lax.rem(me + ahead, count)
        pl.semaphore_signal(
            barrier, inc=1, device_id={"sp": peer}, device_id_type=pl.DeviceIdType.MESH
        )
    for ahead in range(1, parts):
        peer = lax.rem(seat + ahead, parts)
        pl.semaphore_signal(
            barrier, inc=1, device_id={"tp": peer}, device_id_type=pl.DeviceIdType.MESH
        )
    pl.semaphore_wait(barrier, count + parts - 2)


def final_loads(hbm, grads, weights, load_sem):
    dq_hbm, dk_hbm, dv_hbm, wq_hbm, wk_hbm, wv_hbm = hbm
    return [
        pltpu.make_async_copy(dq_hbm, grads.at[0], load_sem.at[0]),
        pltpu.make_async_copy(dk_hbm, grads.at[1], load_sem.at[1]),
        pltpu.make_async_copy(dv_hbm, grads.at[2], load_sem.at[2]),
        pltpu.make_async_copy(wq_hbm, weights.at[0], load_sem.at[3]),
        pltpu.make_async_copy(wk_hbm, weights.at[1], load_sem.at[4]),
        pltpu.make_async_copy(wv_hbm, weights.at[2], load_sem.at[5]),
    ]


class Lines:
    def __init__(self, count, line_ref, out_ref, lines, send, recv):
        self.me = lax.axis_index("sp")
        self.count = count
        self.line_ref, self.out_ref, self.lines = line_ref, out_ref, lines
        self.sems = (send, recv)

    def copy(self, ahead):
        return remote(
            self.line_ref,
            self.lines.at[ahead - 1],
            self.sems[0].at[ahead - 1],
            self.sems[1].at[ahead - 1],
            {"sp": lax.rem(self.me + ahead, self.count)},
        )

    def start(self):
        for ahead in range(1, self.count):
            self.copy(ahead).start()

    def finish(self):
        total = self.line_ref[...]
        for ahead in range(1, self.count):
            self.copy(ahead).wait()
            total = total + self.lines[ahead - 1]
        self.out_ref[...] = exact(total, table_map(self.out_ref.shape[1]), 1)


class InputGrad:
    def __init__(self, parts, grads, weights, input_ref, buffers, sems):
        self.seat = lax.axis_index("tp")
        self.core = lax.rem(self.seat, 2)
        self.row = self.seat // 2
        self.parts, self.pairs = parts, parts // 2
        self.grads, self.weights, self.input_ref = grads, weights, input_ref
        self.pair_sent, self.pair_got, self.cross_sent, self.cross_got, self.kept = buffers
        self.sems = sems
        self.block = input_ref.shape[1]
        self.bands = input_ref.shape[0] // REACH
        self.units = 2 * self.bands

    def rows(self, band):
        return pl.ds(pl.multiple_of(band * REACH, REACH), REACH)

    def part(self, band, target):
        block = pl.ds(pl.multiple_of(target * self.block, self.block), self.block)
        rows = self.rows(band)
        term = contract_cols(self.grads[0, rows], self.weights[0, block])
        term += contract_cols(self.grads[1, rows], self.weights[1, block])
        return term + contract_cols(self.grads[2, rows], self.weights[2, block])

    def pair_copy(self, band, away):
        return remote(
            self.pair_sent.at[band, away],
            self.pair_got.at[band, away],
            self.sems[0].at[band, away],
            self.sems[1].at[band, away],
            {"tp": self.seat + 1 - 2 * self.core},
        )

    def cross_copy(self, band, away):
        return remote(
            self.cross_sent.at[band, away - 1],
            self.cross_got.at[band, away - 1],
            self.sems[2].at[band, away - 1],
            self.sems[3].at[band, away - 1],
            {"tp": lax.rem(self.seat + 2 * away, self.parts)},
        )

    def to_partner(self, band):
        for away in range(self.pairs):
            target = 2 * lax.rem(self.row + away, self.pairs) + 1 - self.core
            self.pair_sent[band, away] = self.part(band, target).astype(jnp.bfloat16)
            self.pair_copy(band, away).start()

    def across(self, band):
        for away in range(1, self.pairs):
            term = self.part(band, lax.rem(self.seat + 2 * away, self.parts))
            self.pair_copy(band, away).wait_recv()
            term = term + self.pair_got[band, away].astype(jnp.float32)
            self.cross_sent[band, away - 1] = term.astype(jnp.bfloat16)
            self.cross_copy(band, away).start()
        term = self.part(band, self.seat)
        self.pair_copy(band, 0).wait_recv()
        self.kept[band] = term + self.pair_got[band, 0].astype(jnp.float32)

    def finish(self, band):
        term = self.kept[band]
        for away in range(1, self.pairs):
            self.cross_copy(band, away).wait_recv()
            term = term + self.cross_got[band, away - 1].astype(jnp.float32)
        self.input_ref[self.rows(band)] = term.astype(jnp.bfloat16)

    def work(self, unit):
        band = unit // 2

        @pl.when(lax.rem(unit, 2) == 0)
        def _():
            self.to_partner(band)

        @pl.when(lax.rem(unit, 2) == 1)
        def _():
            self.across(band)

        @pl.when((lax.rem(unit, 2) == 1) & (unit > 2))
        def _():
            self.finish(band - 1)

    def drain(self):
        @pl.loop(0, self.bands)
        def _(band):
            for away in range(self.pairs):
                self.pair_copy(band, away).wait_send()
            for away in range(1, self.pairs):
                self.cross_copy(band, away).wait_send()


def ring_kernel(
    count,
    parts,
    whole_hbm,
    dq_hbm,
    dk_hbm,
    dv_hbm,
    wq_hbm,
    wk_hbm,
    wv_hbm,
    line_ref,
    input_ref,
    oq_ref,
    ok_ref,
    ov_ref,
    line_out_ref,
    whole,
    grads,
    weights,
    lines,
    pair_sent,
    pair_got,
    cross_sent,
    cross_got,
    kept,
    load_sem,
    line_send,
    line_recv,
    pair_send,
    pair_recv,
    cross_send,
    cross_recv,
    sent,
    got,
    send_sem,
    recv_sem,
):
    me = lax.axis_index("sp")
    place = ring_place(me, count)
    hbm = (dq_hbm, dk_hbm, dv_hbm, wq_hbm, wk_hbm, wv_hbm)
    loads = final_loads(hbm, grads, weights, load_sem)
    loads.append(pltpu.make_async_copy(whole_hbm, whole, load_sem.at[6]))
    for load in loads:
        load.start()
    meet(count, parts)
    shared = Lines(count, line_ref, line_out_ref, lines, line_send, line_recv)
    buffers = (pair_sent, pair_got, cross_sent, cross_got, kept)
    sems = (pair_send, pair_recv, cross_send, cross_recv)
    grad_in = InputGrad(parts, grads, weights, input_ref, buffers, sems)

    outs = (oq_ref, ok_ref, ov_ref)
    half = got.shape[3]
    onward = (
        ring_index(lax.rem(place + 1, count), count),
        ring_index(lax.rem(place + count - 1, count), count),
    )

    def own(target, side, chain):
        start = pl.multiple_of((2 * ring_index(target, count) + side) * half, half)
        return contract_rows(whole[:, pl.ds(start, half)], grads[chain])

    def target_of(step, side):
        if side == 0:
            return lax.rem(place - 1 - step + 2 * count, count)
        return lax.rem(place + 1 + step, count)

    def copy_of(src, step, side, chain):
        return remote(
            src,
            got.at[side, chain, step],
            send_sem.at[side, chain, step],
            recv_sem.at[side, chain, step],
            {"sp": onward[side]},
        )

    for load in loads:
        load.wait()
    for chain in range(3):
        for side in range(2):
            sent[side, chain] = own(target_of(0, side), side, chain).astype(jnp.bfloat16)
            copy_of(sent.at[side, chain], 0, side, chain).start()
    shared.start()

    chains = [(chain, side) for chain in range(3) for side in range(2)]

    @pl.loop(1, count - 1)
    def _(step):
        for chain, side in chains:
            part_of = own(target_of(step, side), side, chain)
            place_of = got.at[side, chain, step - 1]
            copy_of(sent.at[side, chain], step - 1, side, chain).wait_recv()
            total = part_of + place_of[...].astype(jnp.float32)
            place_of[...] = total.astype(jnp.bfloat16)
            copy_of(place_of, step, side, chain).start()
            if (chain, side) == (1, 1):

                @pl.when(step <= grad_in.units)
                def _():
                    grad_in.work(step - 1)

    for unit in range(min(count - 2, grad_in.units), grad_in.units):
        grad_in.work(unit)
    shared.finish()
    for chain, side in chains:
        if (chain, side) == (2, 0):
            grad_in.finish(grad_in.bands - 1)
        part_of = own(place, side, chain)
        copy_of(sent.at[side, chain], count - 2, side, chain).wait_recv()
        total = part_of + got[side, chain, count - 2].astype(jnp.float32)
        outs[chain][side * half : (side + 1) * half] = total

    @pl.loop(0, count - 1)
    def _(step):
        for chain, side in chains:
            copy_of(sent.at[side, chain], step, side, chain).wait_send()

    grad_in.drain()


def paired(count, parts):
    return count == 8 and ring_columns(count) == 2 and parts == 4


def pair_places(me):
    level, side = me // 2, lax.rem(me, 2)
    inner = (level == 1) | (level == 2)
    near = level // 2
    made = jnp.where(inner, 1 - near, near)
    partner = 2 * (level + 1 - 2 * lax.rem(level, 2)) + side
    return level, side, inner, near, made, partner


def pair_kernel(
    count,
    parts,
    whole_hbm,
    dq_hbm,
    dk_hbm,
    dv_hbm,
    wq_hbm,
    wk_hbm,
    wv_hbm,
    theirs_hbm,
    line_ref,
    input_ref,
    oq_ref,
    ok_ref,
    ov_ref,
    line_out_ref,
    turned,
    grads,
    weights,
    lines,
    pair_sent,
    pair_got,
    cross_sent,
    cross_got,
    kept,
    load_sem,
    line_send,
    line_recv,
    pair_send,
    pair_recv,
    cross_send,
    cross_recv,
    theirs,
    their_grads,
    x_sent,
    x_got,
    sent,
    got,
    result,
    theirs_sem,
    swap_send,
    swap_recv,
    x_send,
    x_recv,
    send_sem,
    recv_sem,
    out_sem,
):
    me = lax.axis_index("sp")
    level, side, inner, near, made, partner = pair_places(me)
    hbm = (dq_hbm, dk_hbm, dv_hbm, wq_hbm, wk_hbm, wv_hbm)
    loads = final_loads(hbm, grads, weights, load_sem)
    bands, pairs, _, block = pair_sent.shape
    length = grads.shape[1]

    def rows(band):
        return pl.ds(band * REACH, REACH)

    def piece(band, part):
        start = pl.multiple_of((made * pairs + part) * block, block)
        return pltpu.make_async_copy(
            whole_hbm.at[rows(band), pl.ds(start, block)],
            pair_sent.at[band, part],
            theirs_sem.at[1 + band * pairs + part],
        )

    own_loads = [piece(band, part) for band in range(bands) for part in range(pairs)]
    loads[3:3] = own_loads + [pltpu.make_async_copy(theirs_hbm, theirs, theirs_sem.at[0])]
    for load in loads:
        load.start()
    meet(count, parts)
    shared = Lines(count, line_ref, line_out_ref, lines, line_send, line_recv)
    buffers = (pair_sent, pair_got, cross_sent, cross_got, kept)
    sems = (pair_send, pair_recv, cross_send, cross_recv)
    grad_in = InputGrad(parts, grads, weights, input_ref, buffers, sems)

    chunks, depth, tile = x_sent.shape[0], x_sent.shape[2], x_sent.shape[3]
    per = chunks // 3
    outs = (oq_ref, ok_ref, ov_ref)
    deep = 2 * (1 + made)
    rim = 6 * made
    slot = jnp.where(inner, 0, 1)

    def columns(chunk):
        return pl.ds(pl.multiple_of(lax.rem(chunk, per) * tile, tile), tile)

    def swap(chunk):
        return remote(
            grads.at[chunk // per, :, columns(chunk)],
            their_grads.at[chunk // per, :, columns(chunk)],
            swap_send.at[chunk],
            swap_recv.at[chunk],
            {"sp": partner},
        )

    def x_copy(chunk):
        return remote(
            x_sent.at[chunk],
            x_got.at[chunk],
            x_send.at[chunk],
            x_recv.at[chunk],
            {"sp": 2 * level + 1 - side},
        )

    def deep_copy(chunk):
        return remote(
            sent.at[0, chunk],
            got.at[slot, chunk],
            send_sem.at[0, chunk],
            recv_sem.at[slot, chunk],
            {"sp": deep + side},
        )

    def rim_copy(chunk):
        return remote(
            sent.at[1, chunk],
            got.at[0, chunk],
            send_sem.at[1, chunk],
            recv_sem.at[0, chunk],
            {"sp": rim + side},
        )

    def arrived(chunk, which):
        return remote(
            sent.at[0, chunk],
            got.at[which, chunk],
            send_sem.at[0, chunk],
            recv_sem.at[which, chunk],
            {"sp": deep + side},
        )

    def sums(target, chunk):
        start = pl.multiple_of((target - made * (count // 2)) * depth, depth)
        features = pl.ds(start, depth)
        mine = grads[chunk // per, :, columns(chunk)]
        other = their_grads[chunk // per, :, columns(chunk)]
        term = jnp.dot(turned[features, :length], mine, preferred_element_type=jnp.float32)
        return term + jnp.dot(
            turned[features, length:], other, preferred_element_type=jnp.float32
        )

    def halve(chunk):
        swap(chunk).wait_recv()
        x_sent[chunk, 0] = sums(deep + 1 - side, chunk).astype(jnp.bfloat16)
        x_sent[chunk, 1] = sums(rim + 1 - side, chunk).astype(jnp.bfloat16)
        x_copy(chunk).start()

    def onward(chunk):
        term = sums(deep + side, chunk)
        x_copy(chunk).wait_recv()
        term = term + x_got[chunk, 0].astype(jnp.float32)
        sent[0, chunk] = term.astype(jnp.bfloat16)
        deep_copy(chunk).start()
        term = sums(rim + side, chunk) + x_got[chunk, 1].astype(jnp.float32)

        @pl.when(inner)
        def _():
            sent[1, chunk] = term.astype(jnp.bfloat16)

        @pl.when(jnp.logical_not(inner))
        def _():
            result[chunk // per, :, columns(chunk)] = term

    def store(chunk, matrix):
        return pltpu.make_async_copy(
            result.at[matrix, :, columns(chunk)],
            outs[matrix].at[:, columns(chunk)],
            out_sem.at[chunk],
        )

    def finish(chunk):
        arrived(chunk, 0).wait_recv()
        term = got[0, chunk].astype(jnp.float32)

        @pl.when(inner)
        def _():
            arrived(chunk, 1).wait_recv()
            total = term + got[1, chunk].astype(jnp.float32)
            result[chunk // per, :, columns(chunk)] = total

        @pl.when(jnp.logical_not(inner))
        def _():
            total = term + result[chunk // per, :, columns(chunk)]
            result[chunk // per, :, columns(chunk)] = total

        for matrix in range(3):

            @pl.when(chunk // per == matrix)
            def _():
                store(chunk, matrix).start()

    for which in range(3):
        loads[which].wait()
        for chunk in range(per):
            swap(which * per + chunk).start()
    shared.start()
    for load in loads[3:-3]:
        load.wait()

    @pl.loop(0, bands)
    def _(band):
        start = pl.multiple_of(band * REACH, REACH)
        for part in range(pairs):
            low = slice(part * block, (part + 1) * block)
            turned[low, pl.ds(start, REACH)] = pair_sent[band, part].T
            turned[low, pl.ds(length + start, REACH)] = theirs[pl.ds(start, REACH), low].T

    hold = 2
    rest = hold + 3
    lag = 3 * chunks // 4

    @pl.loop(0, chunks + lag)
    def _(step):
        @pl.when(step < chunks)
        def _():
            halve(step)

        @pl.when((step >= hold) & (step < chunks + hold))
        def _():
            onward(step - hold)

        @pl.when(inner & (step >= rest) & (step < chunks + hold))
        def _():
            rim_copy(step - rest).start()

        @pl.when(inner & (step == chunks + hold))
        def _():
            for chunk in range(chunks + hold - rest, chunks):
                rim_copy(chunk).start()

        @pl.when(step >= lag)
        def _():
            finish(step - lag)

        unit = (step - 1) // 2

        @pl.when(step == 1)
        def _():
            for load in loads[-3:]:
                load.wait()

        @pl.when((lax.rem(step, 2) == 1) & (unit < grad_in.units))
        def _():
            grad_in.work(unit)

    for unit in range(min((chunks + lag) // 2, grad_in.units), grad_in.units):
        grad_in.work(unit)
    shared.finish()
    grad_in.finish(grad_in.bands - 1)

    @pl.loop(0, chunks)
    def _(chunk):
        swap(chunk).wait_send()
        x_copy(chunk).wait_send()
        deep_copy(chunk).wait_send()
        store(chunk, 0).wait()

        @pl.when(inner)
        def _():
            rim_copy(chunk).wait_send()

    grad_in.drain()


def final_grads(whole, theirs, grads, lines, weights, entries):
    count = lax.axis_size("sp")
    parts = lax.axis_size("tp")
    pairs = parts // 2
    length, features = whole.shape
    width = weights[0].shape[1]
    depth = features // count
    block = features // parts
    bands = length // REACH
    vmem = pl.BlockSpec(memory_space=pltpu.VMEM)
    anywhere = pl.BlockSpec(memory_space=pl.ANY)
    out = jax.ShapeDtypeStruct((depth, width), jnp.float32)
    dma = pltpu.SemaphoreType.DMA
    low = jnp.bfloat16
    pair = paired(count, parts)
    tile = min(width, LANES)
    chunks = 3 * width // tile
    scratch = [
        pltpu.VMEM((features // 2, 2 * length) if pair else (length, features), low),
        pltpu.VMEM((3, length, width), low),
        pltpu.VMEM((3, features, width), low),
        pltpu.VMEM((count - 1,) + lines.shape, jnp.float32),
        pltpu.VMEM((bands, pairs, REACH, block), low),
        pltpu.VMEM((bands, pairs, REACH, block), low),
        pltpu.VMEM((bands, pairs - 1, REACH, block), low),
        pltpu.VMEM((bands, pairs - 1, REACH, block), low),
        pltpu.VMEM((bands, REACH, block), jnp.float32),
        dma((7,)),
        dma((count - 1,)),
        dma((count - 1,)),
        dma((bands, pairs)),
        dma((bands, pairs)),
        dma((bands, pairs - 1)),
        dma((bands, pairs - 1)),
    ]
    if pair:
        scratch += [
            pltpu.VMEM((length, features // 2), low),
            pltpu.VMEM((3, length, width), low),
            pltpu.VMEM((chunks, 2, depth, tile), low),
            pltpu.VMEM((chunks, 2, depth, tile), low),
            pltpu.VMEM((2, chunks, depth, tile), low),
            pltpu.VMEM((2, chunks, depth, tile), low),
            pltpu.VMEM((3, depth, width), jnp.float32),
            dma((1 + bands * pairs,)),
            dma((chunks,)),
            dma((chunks,)),
            dma((chunks,)),
            dma((chunks,)),
            dma((2, chunks)),
            dma((2, chunks)),
            dma((chunks,)),
        ]
    else:
        scratch += [
            pltpu.VMEM((2, 3, depth // 2, width), low),
            pltpu.VMEM((2, 3, count - 1, depth // 2, width), low),
            dma((2, 3, count - 1)),
            dma((2, 3, count - 1)),
        ]
    place = anywhere if pair else vmem
    return pl.pallas_call(
        functools.partial(pair_kernel if pair else ring_kernel, count, parts),
        in_specs=[anywhere] * (7 + pair) + [vmem],
        out_specs=[vmem] + [place] * 3 + [vmem],
        out_shape=[
            jax.ShapeDtypeStruct((length, block), low),
            out,
            out,
            out,
            jax.ShapeDtypeStruct((lines.shape[0], entries), jnp.float32),
        ],
        scratch_shapes=scratch,
        compiler_params=pltpu.CompilerParams(
            collective_id=0, has_side_effects=True, vmem_limit_bytes=63 * 1024 * 1024
        ),
        cost_estimate=pl.CostEstimate(
            flops=12 * length * features * width,
            bytes_accessed=400_000_000,
            transcendentals=0,
        ),
    )(whole, *grads, *weights, *theirs, lines)


def gather_kernel(
    parts,
    tokens_ref,
    wq_ref,
    wk_ref,
    wv_ref,
    g_ref,
    bias_ref,
    whole_ref,
    theirs_ref,
    dq_ref,
    dk_ref,
    dv_ref,
    line_ref,
    held,
    weights,
    total,
    halo,
    halo_got,
    back,
    after,
    q_all,
    k_all,
    v_all,
    bias_all,
    bias_sum,
    dk_all,
    dv_all,
    side_send,
    side_recv,
    far_send,
    far_recv,
    relay_send,
    relay_recv,
    halo_send,
    halo_recv,
    back_send,
    back_recv,
    load_sem,
    store_sem,
    *ship_refs,
):
    me = lax.axis_index("tp")
    seat = lax.axis_index("sp")
    seats = lax.axis_size("sp")
    partner = me + 1 - 2 * lax.rem(me, 2)
    chunks = held.shape[0]
    block = tokens_ref.shape[1]
    grain = held.shape[2]
    length = tokens_ref.shape[0]
    heads, entries = bias_ref.shape
    pairs = parts // 2
    matrices = (wq_ref, wk_ref, wv_ref)

    def source(device, away):
        return lax.rem(device + parts - 2 * away, parts)

    order = [me, partner]
    for away in range(1, pairs):
        order += [source(me, away), source(partner, away)]

    def load(slot, matrix):
        start = pl.multiple_of(order[slot] * block, block)
        return pltpu.make_async_copy(
            matrices[matrix].at[pl.ds(start, block)],
            weights.at[slot, matrix],
            load_sem.at[slot, matrix],
        )

    for slot in range(parts):
        for matrix in range(3):
            load(slot, matrix).start()

    barrier = pltpu.get_barrier_semaphore()
    for ahead in range(1, parts):
        pl.semaphore_signal(
            barrier,
            inc=1,
            device_id={"tp": lax.rem(me + ahead, parts)},
            device_id_type=pl.DeviceIdType.MESH,
        )
    onward = lax.rem(seat + 1, seats)
    for other in (onward, lax.rem(seat + seats - 1, seats)):
        pl.semaphore_signal(
            barrier, inc=1, device_id={"sp": other}, device_id_type=pl.DeviceIdType.MESH
        )
    ship = len(ship_refs) > 0
    if ship:
        level, lane, inner, near, made, mate = pair_places(seat)
        pl.semaphore_signal(
            barrier, inc=1, device_id={"sp": mate}, device_id_type=pl.DeviceIdType.MESH
        )
    pl.semaphore_wait(barrier, parts + 1 + ship)

    def rows(chunk):
        return pl.ds(chunk * grain, grain)

    def far(chunk, away):
        return remote(
            tokens_ref.at[rows(chunk)],
            held.at[chunk, me],
            far_send.at[chunk, away - 1],
            far_recv.at[chunk, away - 1],
            {"tp": lax.rem(me + 2 * away, parts)},
        )

    def side(chunk):
        return remote(
            tokens_ref.at[rows(chunk)],
            held.at[chunk, me],
            side_send.at[chunk],
            side_recv.at[chunk],
            {"tp": partner},
        )

    def relay(chunk, away):
        place = held.at[chunk, source(me, away)]
        return remote(
            place,
            place,
            relay_send.at[chunk, away - 1],
            relay_recv.at[chunk, away - 1],
            {"tp": partner},
        )

    def neighbour():
        return remote(halo, halo_got, halo_send, halo_recv, {"sp": onward})

    def behind():
        device = {"sp": lax.rem(seat + seats - 1, seats)}
        return remote(back, after, back_send, back_recv, device)

    scratch = (bias_all, bias_sum, dk_all, dv_all)
    factor = (q_all.shape[1] // heads) ** (-0.5)
    work = Attention(factor, heads, q_all, k_all, v_all, g_ref, dq_ref, scratch)

    def store(chunk, slot):
        start = pl.multiple_of(order[slot] * block, block)
        src = tokens_ref.at[rows(chunk)] if slot == 0 else held.at[chunk, order[slot]]
        return pltpu.make_async_copy(
            src, whole_ref.at[rows(chunk), pl.ds(start, block)], store_sem.at[chunk, slot]
        )

    def add(chunk, slot, value):
        for matrix in range(3):
            term = jnp.dot(value, weights[slot, matrix], preferred_element_type=jnp.float32)
            if slot == 0:
                total[matrix, chunk] = term
            else:
                total[matrix, chunk] += term

    if ship:
        ship_got, ship_send, ship_recv, pass_send, pass_recv, keep_sem = ship_refs
        core = lax.rem(me, 2)
        shipped = jnp.where(inner, near, 1 - near)
        ready = me // 2 == shipped

        def ship_copy(chunk, src):
            return remote(
                src,
                ship_got.at[chunk, core],
                ship_send.at[chunk],
                ship_recv.at[chunk],
                {"sp": mate},
            )

        def pass_on(chunk):
            place = ship_got.at[chunk, core]
            return remote(
                place, place, pass_send.at[chunk], pass_recv.at[chunk], {"tp": partner}
            )

        def keep(chunk, which):
            start = pl.multiple_of(which * block, block)
            return pltpu.make_async_copy(
                ship_got.at[chunk, which],
                theirs_ref.at[rows(chunk), pl.ds(start, block)],
                keep_sem.at[chunk, which],
            )

    tail = REACH // grain
    sequence = list(range(chunks - tail, chunks)) + list(range(chunks - tail))
    for chunk in sequence:
        for away in range(1, pairs):
            far(chunk, away).start()
        side(chunk).start()
    for slot in range(2):
        for matrix in range(3):
            load(slot, matrix).wait()
        for chunk in sequence:
            if slot == 1:
                side(chunk).wait_recv()
            store(chunk, slot).start()
            value = tokens_ref[rows(chunk)] if slot == 0 else held[chunk, partner]
            add(chunk, slot, value)
    for slot in range(2, parts):
        for matrix in range(3):
            load(slot, matrix).wait()
    work.begin(exact(bias_ref[...], table_map(entries), 0))
    done = []
    waiting = list(range(0, length, ROWS))

    def attend_ready(early):
        known = {row for chunk in done for row in range(chunk * grain, (chunk + 1) * grain, ROWS)}
        for start in list(waiting):
            needs = range(max(0, start - REACH), start + ROWS, ROWS)
            if start < REACH and early:
                continue
            if set(needs) <= known:
                if start == 0:
                    take_halo()
                work.attend(start)
                waiting.remove(start)
                if start == REACH - ROWS:
                    send_behind()

    def take_halo():
        @pl.when(seat > 0)
        def _():
            neighbour().wait_recv()

        @pl.when(seat == 0)
        def _():
            halo_got[...] = jnp.zeros_like(halo_got)

        k_all[:REACH] = halo_got[0]
        v_all[:REACH] = halo_got[1]

    def send_behind():
        @pl.when(seat > 0)
        def _():
            work.behind(back)
            behind().start()

    for chunk in sequence:
        for away in range(1, pairs):
            far(chunk, away).wait_recv()
            relay(chunk, away).start()
            if ship:

                @pl.when(ready)
                def _():
                    ship_copy(chunk, tokens_ref.at[rows(chunk)]).start()

                @pl.when(jnp.logical_not(ready))
                def _():
                    ship_copy(chunk, held.at[chunk, source(me, 1)]).start()

            store(chunk, 2 * away).start()
            add(chunk, 2 * away, held[chunk, source(me, away)])
        for away in range(1, pairs):
            relay(chunk, away).wait_recv()
            store(chunk, 2 * away + 1).start()
            add(chunk, 2 * away + 1, held[chunk, source(partner, away)])
        low = chunk * grain
        q_all[low : low + grain] = total[0, chunk].astype(jnp.bfloat16)
        k_all[REACH + low : REACH + low + grain] = total[1, chunk].astype(jnp.bfloat16)
        v_all[REACH + low : REACH + low + grain] = total[2, chunk].astype(jnp.bfloat16)
        done.append(chunk)
        if chunk == chunks - 1:
            halo[0] = k_all[length:]
            halo[1] = v_all[length:]

            @pl.when(seat < seats - 1)
            def _():
                neighbour().start()

        attend_ready(len(done) < chunks - 1)
    attend_ready(False)
    work.end(dk_ref, dv_ref, line_ref)

    @pl.when(seat < seats - 1)
    def _():
        behind().wait_recv()

    @pl.when(seat == seats - 1)
    def _():
        after[...] = jnp.zeros_like(after)

    work.join(dk_ref, dv_ref, after)

    @pl.when(seat > 0)
    def _():
        behind().wait_send()

    @pl.when(seat < seats - 1)
    def _():
        neighbour().wait_send()

    if ship:
        for chunk in sequence:
            ship_copy(chunk, tokens_ref.at[rows(chunk)]).wait_recv()
            pass_on(chunk).start()
            keep(chunk, core).start()
        for chunk in sequence:
            pass_on(chunk).wait_recv()
            keep(chunk, 1 - core).start()
        for chunk in sequence:
            ship_copy(chunk, tokens_ref.at[rows(chunk)]).wait_send()
            pass_on(chunk).wait_send()
            keep(chunk, core).wait()
            keep(chunk, 1 - core).wait()
    for chunk in sequence:
        side(chunk).wait_send()
        for away in range(1, pairs):
            far(chunk, away).wait_send()
            relay(chunk, away).wait_send()
        for slot in range(parts):
            store(chunk, slot).wait()


def attention_grads(tokens, query_weight, key_weight, value_weight, position_bias, out_grad):
    parts = lax.axis_size("tp")
    length, block = tokens.shape
    width = query_weight.shape[1]
    heads = position_bias.shape[0]
    chunks = length // GRAIN
    pairs = parts // 2
    vmem = pl.BlockSpec(memory_space=pltpu.VMEM)
    anywhere = pl.BlockSpec(memory_space=pl.ANY)
    low = jnp.bfloat16

    def shape(kind, *sizes):
        return jax.ShapeDtypeStruct(sizes, kind)

    dma = pltpu.SemaphoreType.DMA
    ship = paired(lax.axis_size("sp"), parts)
    extra = []
    if ship:
        extra = [
            pltpu.VMEM((chunks, 2, GRAIN, block), jnp.bfloat16),
            dma((chunks,)),
            dma((chunks,)),
            dma((chunks,)),
            dma((chunks,)),
            dma((chunks, 2)),
        ]
    return pl.pallas_call(
        functools.partial(gather_kernel, parts),
        in_specs=[vmem, anywhere, anywhere, anywhere, vmem, vmem],
        out_specs=[anywhere] * 2 + [vmem] * 4,
        out_shape=[
            shape(low, length, block * parts),
            shape(low, *((length, 2 * block) if ship else (8, LANES))),
            shape(low, length, width),
            shape(low, length, width),
            shape(low, length, width),
            shape(jnp.float32, heads, TABLE),
        ],
        scratch_shapes=[
            pltpu.VMEM((chunks, parts, GRAIN, block), low),
            pltpu.VMEM((parts, 3, block, width), jnp.bfloat16),
            pltpu.VMEM((3, chunks, GRAIN, width), jnp.float32),
            pltpu.VMEM((2, REACH, width), low),
            pltpu.VMEM((2, REACH, width), low),
            pltpu.VMEM((2, REACH, width), low),
            pltpu.VMEM((2, REACH, width), low),
            pltpu.VMEM((length, width), low),
            pltpu.VMEM((length + REACH, width), low),
            pltpu.VMEM((length + REACH, width), low),
            pltpu.VMEM((heads, ROWS, WINDOW), jnp.float32),
            pltpu.VMEM((heads, ROWS, WINDOW), jnp.float32),
            pltpu.VMEM((length + REACH, width), jnp.float32),
            pltpu.VMEM((length + REACH, width), jnp.float32),
            dma((chunks,)),
            dma((chunks,)),
            dma((chunks, pairs - 1)),
            dma((chunks, pairs - 1)),
            dma((chunks, pairs - 1)),
            dma((chunks, pairs - 1)),
            dma(()),
            dma(()),
            dma(()),
            dma(()),
            dma((parts, 3)),
            dma((chunks, parts)),
        ]
        + extra,
        compiler_params=pltpu.CompilerParams(
            collective_id=1, has_side_effects=True, vmem_limit_bytes=56 * 1024 * 1024
        ),
        cost_estimate=pl.CostEstimate(
            flops=6 * length * block * parts * width, bytes_accessed=150_000_000, transcendentals=0
        ),
    )(tokens, query_weight, key_weight, value_weight, out_grad, position_bias)


def shards(tokens, query_weight, key_weight, value_weight, position_bias, out_grad):
    outs = attention_grads(
        tokens, query_weight, key_weight, value_weight, position_bias, out_grad
    )
    whole, theirs, query_grad, key_grad, value_grad, lines = outs
    *large, bias_grad = final_grads(
        whole,
        (theirs,) if paired(lax.axis_size("sp"), lax.axis_size("tp")) else (),
        (query_grad, key_grad, value_grad),
        lines,
        (query_weight, key_weight, value_weight),
        position_bias.shape[1],
    )
    return (*hand_on(large), bias_grad)


def hand_kernel(*refs):
    half = len(refs) // 2
    for source, target in zip(refs[:half], refs[half:]):
        target[...] = source[...]


def hand_on(arrays, steps=2):
    specs = [
        pl.BlockSpec((array.shape[0], array.shape[1] // steps), lambda i: (0, i))
        for array in arrays
    ]
    size = sum(2 * array.size * array.dtype.itemsize for array in arrays)
    return pl.pallas_call(
        hand_kernel,
        grid=(steps,),
        in_specs=specs,
        out_specs=specs,
        out_shape=[jax.ShapeDtypeStruct(array.shape, array.dtype) for array in arrays],
        cost_estimate=pl.CostEstimate(flops=0, bytes_accessed=size, transcendentals=0),
    )(*arrays)


def solution(mesh):
    in_specs = (
        P("sp", "tp"),
        P(None, "tp"),
        P(None, "tp"),
        P(None, "tp"),
        P("tp", None),
        P("sp", "tp"),
    )
    out_specs = (P("sp", "tp"), P("sp", "tp"), P("sp", "tp"), P("sp", "tp"), P("tp", None))
    return jax.shard_map(shards, mesh=mesh, in_specs=in_specs, out_specs=out_specs, check_vma=False)
```

```python
import functools

import jax
import jax.numpy as jnp
from jax import lax
from jax.experimental import pallas as pl
from jax.experimental.pallas import tpu as pltpu
from jax.sharding import PartitionSpec as P

SEGMENT = 64
PREVIOUS = 4
CLIP = 256
ROWS = 2 * SEGMENT
REACH = PREVIOUS * SEGMENT
WINDOW = ROWS + REACH
TABLE = 512
LANES = 128
GRAIN = 128
HIDDEN = -1e30


def contract_rows(left, right):
    return lax.dot_general(
        left, right, (((0,), (0,)), ((), ())), preferred_element_type=jnp.float32
    )


def contract_cols(left, right):
    return lax.dot_general(
        left, right, (((1,), (1,)), ((), ())), preferred_element_type=jnp.float32
    )


def diagonal_sums(tile):
    half = tile.shape[0] // 2
    while half >= 8:
        tile = tile[:half] + pltpu.roll(tile[half:], TABLE - half, 1)
        half //= 2
    row = lax.broadcasted_iota(jnp.int32, tile.shape, 0)
    for step in (4, 2, 1):
        tile = jnp.where((row & step) != 0, pltpu.roll(tile, TABLE - step, 1), tile)
    return jnp.sum(tile, axis=0, keepdims=True)


def table_map(entries):
    entry = lax.broadcasted_iota(jnp.int32, (entries, TABLE), 0)
    column = lax.broadcasted_iota(jnp.int32, (entries, TABLE), 1)
    near = column + entry == entries - 1
    far = (column >= WINDOW) & (entry == entries - 1)
    return jnp.where(near | far, 1.0, 0.0).astype(jnp.float32)


def exact(left, right, axis):
    return lax.dot_general(
        left,
        right,
        (((1,), (axis,)), ((), ())),
        precision=lax.Precision.HIGHEST,
        preferred_element_type=jnp.float32,
    )


class Attention:
    def __init__(self, factor, heads, q_all, k_all, v_all, g_ref, dq_ref, scratch):
        self.factor, self.heads = factor, heads
        self.q_all, self.k_all, self.v_all = q_all, k_all, v_all
        self.g_ref, self.dq_ref = g_ref, dq_ref
        self.bias_all, self.bias_sum, self.dk_all, self.dv_all = scratch
        self.head = q_all.shape[1] // heads

    def begin(self, table_rows):
        self.dk_all[...] = jnp.zeros_like(self.dk_all)
        self.dv_all[...] = jnp.zeros_like(self.dv_all)
        self.bias_sum[...] = jnp.zeros_like(self.bias_sum)
        row = lax.broadcasted_iota(jnp.int32, (ROWS, WINDOW), 0) // SEGMENT
        column = lax.broadcasted_iota(jnp.int32, (ROWS, WINDOW), 1)
        behind = column // SEGMENT - row
        seen = (behind >= 0) & (behind <= PREVIOUS)
        for head in range(self.heads):
            table = jnp.broadcast_to(table_rows[head : head + 1], (ROWS, TABLE))
            bias = pltpu.roll(table, 0, 1, stride=1, stride_axis=0)[:, :WINDOW]
            self.bias_all[head] = jnp.where(seen, bias, HIDDEN)

    def attend(self, start):
        @pl.loop(0, self.heads, unroll=2)
        def _(head):
            columns = pl.ds(pl.multiple_of(head * self.head, self.head), self.head)
            rows = slice(start, start + ROWS)
            window = slice(start, start + WINDOW)
            q = self.q_all[rows, columns]
            g = self.g_ref[rows, columns]
            k = self.k_all[window, columns]
            v = self.v_all[window, columns]
            mask = self.bias_all[head]
            if start < REACH:
                first = jnp.where(lax.axis_index("sp") == 0, REACH - start, 0)
                column = lax.broadcasted_iota(jnp.int32, (ROWS, WINDOW), 1)
                mask = jnp.where(column < first, HIDDEN, mask)
            scores = contract_cols(q, k) * self.factor + mask
            top = jnp.max(scores, axis=1, keepdims=True)
            raised = jnp.exp(scores - top)
            weights = raised * (1.0 / jnp.sum(raised, axis=1, keepdims=True))
            prob_grad = contract_cols(g, v)
            delta = jnp.sum(weights * prob_grad, axis=1, keepdims=True)
            score_grad = weights * (prob_grad - delta)
            self.bias_sum[head] += score_grad
            low = score_grad.astype(jnp.bfloat16)
            dq = jnp.dot(low, k, preferred_element_type=jnp.float32) * self.factor
            self.dq_ref[rows, columns] = dq.astype(jnp.bfloat16)
            self.dk_all[window, columns] += contract_rows(low, q)
            self.dv_all[window, columns] += contract_rows(weights.astype(jnp.bfloat16), g)

    def behind(self, back):
        back[0] = (self.dk_all[:REACH] * self.factor).astype(jnp.bfloat16)
        back[1] = self.dv_all[:REACH].astype(jnp.bfloat16)

    def end(self, dk_ref, dv_ref, line_ref):
        length = self.q_all.shape[0]
        body = length - REACH
        dk_all, dv_all, factor = self.dk_all, self.dv_all, self.factor
        dk_ref[:body] = (dk_all[REACH:length] * factor).astype(jnp.bfloat16)
        dv_ref[:body] = dv_all[REACH:length].astype(jnp.bfloat16)
        for head in range(self.heads):
            blank = jnp.zeros((ROWS, TABLE - WINDOW), jnp.float32)
            padded = jnp.concatenate([self.bias_sum[head], blank], axis=1)
            line_ref[head : head + 1] = diagonal_sums(padded)

    def join(self, dk_ref, dv_ref, after):
        length = self.q_all.shape[0]
        dk = self.dk_all[length:] * self.factor + after[0].astype(jnp.float32)
        dk_ref[length - REACH :] = dk.astype(jnp.bfloat16)
        dv = self.dv_all[length:] + after[1].astype(jnp.float32)
        dv_ref[length - REACH :] = dv.astype(jnp.bfloat16)


def ring_columns(count):
    columns = 1
    while (2 * columns) ** 2 <= count:
        columns *= 2
    return columns


def ring_place(index, count):
    columns = ring_columns(count)
    rows = count // columns
    row, column = index // columns, index % columns
    above = rows - 1 - row
    across = jnp.where(above % 2 == 0, column - 1, columns - 1 - column)
    return jnp.where(column == 0, row, rows + above * (columns - 1) + across)


def ring_index(place, count):
    columns = ring_columns(count)
    rows = count // columns
    later = jnp.maximum(place - rows, 0)
    above, across = later // (columns - 1), later % (columns - 1)
    column = jnp.where(above % 2 == 0, 1 + across, columns - 1 - across)
    return jnp.where(place < rows, place * columns, (rows - 1 - above) * columns + column)


def remote(src, dst, send, recv, device):
    return pltpu.make_async_remote_copy(
        src_ref=src,
        dst_ref=dst,
        send_sem=send,
        recv_sem=recv,
        device_id=device,
        device_id_type=pl.DeviceIdType.MESH,
    )


def meet(count, parts):
    me = lax.axis_index("sp")
    seat = lax.axis_index("tp")
    barrier = pltpu.get_barrier_semaphore()
    for ahead in range(1, count):
        peer = lax.rem(me + ahead, count)
        pl.semaphore_signal(
            barrier, inc=1, device_id={"sp": peer}, device_id_type=pl.DeviceIdType.MESH
        )
    for ahead in range(1, parts):
        peer = lax.rem(seat + ahead, parts)
        pl.semaphore_signal(
            barrier, inc=1, device_id={"tp": peer}, device_id_type=pl.DeviceIdType.MESH
        )
    pl.semaphore_wait(barrier, count + parts - 2)


def final_loads(hbm, grads, weights, load_sem):
    dq_hbm, dk_hbm, dv_hbm, wq_hbm, wk_hbm, wv_hbm = hbm
    return [
        pltpu.make_async_copy(dq_hbm, grads.at[0], load_sem.at[0]),
        pltpu.make_async_copy(dk_hbm, grads.at[1], load_sem.at[1]),
        pltpu.make_async_copy(dv_hbm, grads.at[2], load_sem.at[2]),
        pltpu.make_async_copy(wq_hbm, weights.at[0], load_sem.at[3]),
        pltpu.make_async_copy(wk_hbm, weights.at[1], load_sem.at[4]),
        pltpu.make_async_copy(wv_hbm, weights.at[2], load_sem.at[5]),
    ]


class Lines:
    def __init__(self, count, line_ref, out_ref, lines, send, recv):
        self.me = lax.axis_index("sp")
        self.count = count
        self.line_ref, self.out_ref, self.lines = line_ref, out_ref, lines
        self.sems = (send, recv)

    def copy(self, ahead):
        return remote(
            self.line_ref,
            self.lines.at[ahead - 1],
            self.sems[0].at[ahead - 1],
            self.sems[1].at[ahead - 1],
            {"sp": lax.rem(self.me + ahead, self.count)},
        )

    def start(self):
        for ahead in range(1, self.count):
            self.copy(ahead).start()

    def finish(self):
        total = self.line_ref[...]
        for ahead in range(1, self.count):
            self.copy(ahead).wait()
            total = total + self.lines[ahead - 1]
        self.out_ref[...] = exact(total, table_map(self.out_ref.shape[1]), 1)


class InputGrad:
    def __init__(self, parts, grads, weights, input_ref, buffers, sems):
        self.seat = lax.axis_index("tp")
        self.core = lax.rem(self.seat, 2)
        self.row = self.seat // 2
        self.parts, self.pairs = parts, parts // 2
        self.grads, self.weights, self.input_ref = grads, weights, input_ref
        self.pair_sent, self.pair_got, self.cross_sent, self.cross_got, self.kept = buffers
        self.sems = sems
        self.block = input_ref.shape[1]
        self.bands = input_ref.shape[0] // REACH
        self.units = 2 * self.bands

    def rows(self, band):
        return pl.ds(pl.multiple_of(band * REACH, REACH), REACH)

    def part(self, band, target):
        block = pl.ds(pl.multiple_of(target * self.block, self.block), self.block)
        rows = self.rows(band)
        term = contract_cols(self.grads[0, rows], self.weights[0, block])
        term += contract_cols(self.grads[1, rows], self.weights[1, block])
        return term + contract_cols(self.grads[2, rows], self.weights[2, block])

    def pair_copy(self, band, away):
        return remote(
            self.pair_sent.at[band, away],
            self.pair_got.at[band, away],
            self.sems[0].at[band, away],
            self.sems[1].at[band, away],
            {"tp": self.seat + 1 - 2 * self.core},
        )

    def cross_copy(self, band, away):
        return remote(
            self.cross_sent.at[band, away - 1],
            self.cross_got.at[band, away - 1],
            self.sems[2].at[band, away - 1],
            self.sems[3].at[band, away - 1],
            {"tp": lax.rem(self.seat + 2 * away, self.parts)},
        )

    def to_partner(self, band):
        for away in range(self.pairs):
            target = 2 * lax.rem(self.row + away, self.pairs) + 1 - self.core
            self.pair_sent[band, away] = self.part(band, target).astype(jnp.bfloat16)
            self.pair_copy(band, away).start()

    def across(self, band):
        for away in range(1, self.pairs):
            term = self.part(band, lax.rem(self.seat + 2 * away, self.parts))
            self.pair_copy(band, away).wait_recv()
            term = term + self.pair_got[band, away].astype(jnp.float32)
            self.cross_sent[band, away - 1] = term.astype(jnp.bfloat16)
            self.cross_copy(band, away).start()
        term = self.part(band, self.seat)
        self.pair_copy(band, 0).wait_recv()
        self.kept[band] = term + self.pair_got[band, 0].astype(jnp.float32)

    def finish(self, band):
        term = self.kept[band]
        for away in range(1, self.pairs):
            self.cross_copy(band, away).wait_recv()
            term = term + self.cross_got[band, away - 1].astype(jnp.float32)
        self.input_ref[self.rows(band)] = term.astype(jnp.bfloat16)

    def work(self, unit):
        band = unit // 2

        @pl.when(lax.rem(unit, 2) == 0)
        def _():
            self.to_partner(band)

        @pl.when(lax.rem(unit, 2) == 1)
        def _():
            self.across(band)

        @pl.when((lax.rem(unit, 2) == 1) & (unit > 2))
        def _():
            self.finish(band - 1)

    def drain(self):
        @pl.loop(0, self.bands)
        def _(band):
            for away in range(self.pairs):
                self.pair_copy(band, away).wait_send()
            for away in range(1, self.pairs):
                self.cross_copy(band, away).wait_send()


def ring_kernel(
    count,
    parts,
    whole_hbm,
    dq_hbm,
    dk_hbm,
    dv_hbm,
    wq_hbm,
    wk_hbm,
    wv_hbm,
    line_ref,
    input_ref,
    oq_ref,
    ok_ref,
    ov_ref,
    line_out_ref,
    whole,
    grads,
    weights,
    lines,
    pair_sent,
    pair_got,
    cross_sent,
    cross_got,
    kept,
    load_sem,
    line_send,
    line_recv,
    pair_send,
    pair_recv,
    cross_send,
    cross_recv,
    sent,
    got,
    send_sem,
    recv_sem,
):
    me = lax.axis_index("sp")
    place = ring_place(me, count)
    hbm = (dq_hbm, dk_hbm, dv_hbm, wq_hbm, wk_hbm, wv_hbm)
    loads = final_loads(hbm, grads, weights, load_sem)
    loads.append(pltpu.make_async_copy(whole_hbm, whole, load_sem.at[6]))
    for load in loads:
        load.start()
    meet(count, parts)
    shared = Lines(count, line_ref, line_out_ref, lines, line_send, line_recv)
    buffers = (pair_sent, pair_got, cross_sent, cross_got, kept)
    sems = (pair_send, pair_recv, cross_send, cross_recv)
    grad_in = InputGrad(parts, grads, weights, input_ref, buffers, sems)

    outs = (oq_ref, ok_ref, ov_ref)
    half = got.shape[3]
    onward = (
        ring_index(lax.rem(place + 1, count), count),
        ring_index(lax.rem(place + count - 1, count), count),
    )

    def own(target, side, chain):
        start = pl.multiple_of((2 * ring_index(target, count) + side) * half, half)
        return contract_rows(whole[:, pl.ds(start, half)], grads[chain])

    def target_of(step, side):
        if side == 0:
            return lax.rem(place - 1 - step + 2 * count, count)
        return lax.rem(place + 1 + step, count)

    def copy_of(src, step, side, chain):
        return remote(
            src,
            got.at[side, chain, step],
            send_sem.at[side, chain, step],
            recv_sem.at[side, chain, step],
            {"sp": onward[side]},
        )

    for load in loads:
        load.wait()
    for chain in range(3):
        for side in range(2):
            sent[side, chain] = own(target_of(0, side), side, chain).astype(jnp.bfloat16)
            copy_of(sent.at[side, chain], 0, side, chain).start()
    shared.start()

    chains = [(chain, side) for chain in range(3) for side in range(2)]

    @pl.loop(1, count - 1)
    def _(step):
        for chain, side in chains:
            part_of = own(target_of(step, side), side, chain)
            place_of = got.at[side, chain, step - 1]
            copy_of(sent.at[side, chain], step - 1, side, chain).wait_recv()
            total = part_of + place_of[...].astype(jnp.float32)
            place_of[...] = total.astype(jnp.bfloat16)
            copy_of(place_of, step, side, chain).start()
            if (chain, side) == (1, 1):

                @pl.when(step <= grad_in.units)
                def _():
                    grad_in.work(step - 1)

    for unit in range(min(count - 2, grad_in.units), grad_in.units):
        grad_in.work(unit)
    shared.finish()
    for chain, side in chains:
        if (chain, side) == (2, 0):
            grad_in.finish(grad_in.bands - 1)
        part_of = own(place, side, chain)
        copy_of(sent.at[side, chain], count - 2, side, chain).wait_recv()
        total = part_of + got[side, chain, count - 2].astype(jnp.float32)
        outs[chain][side * half : (side + 1) * half] = total

    @pl.loop(0, count - 1)
    def _(step):
        for chain, side in chains:
            copy_of(sent.at[side, chain], step, side, chain).wait_send()

    grad_in.drain()


def paired(count, parts):
    return count == 8 and ring_columns(count) == 2 and parts == 4


def pair_places(me):
    level, side = me // 2, lax.rem(me, 2)
    inner = (level == 1) | (level == 2)
    near = level // 2
    made = jnp.where(inner, 1 - near, near)
    partner = 2 * (level + 1 - 2 * lax.rem(level, 2)) + side
    return level, side, inner, near, made, partner


def pair_kernel(
    count,
    parts,
    whole_hbm,
    dq_hbm,
    dk_hbm,
    dv_hbm,
    wq_hbm,
    wk_hbm,
    wv_hbm,
    theirs_hbm,
    line_ref,
    input_ref,
    oq_ref,
    ok_ref,
    ov_ref,
    line_out_ref,
    turned,
    grads,
    weights,
    lines,
    pair_sent,
    pair_got,
    cross_sent,
    cross_got,
    kept,
    load_sem,
    line_send,
    line_recv,
    pair_send,
    pair_recv,
    cross_send,
    cross_recv,
    theirs,
    their_grads,
    x_sent,
    x_got,
    sent,
    got,
    result,
    theirs_sem,
    swap_send,
    swap_recv,
    x_send,
    x_recv,
    send_sem,
    recv_sem,
    out_sem,
):
    me = lax.axis_index("sp")
    level, side, inner, near, made, partner = pair_places(me)
    hbm = (dq_hbm, dk_hbm, dv_hbm, wq_hbm, wk_hbm, wv_hbm)
    loads = final_loads(hbm, grads, weights, load_sem)
    bands, pairs, _, block = pair_sent.shape
    length = grads.shape[1]

    def rows(band):
        return pl.ds(band * REACH, REACH)

    def piece(band, part):
        start = pl.multiple_of((made * pairs + part) * block, block)
        return pltpu.make_async_copy(
            whole_hbm.at[rows(band), pl.ds(start, block)],
            pair_sent.at[band, part],
            theirs_sem.at[1 + band * pairs + part],
        )

    own_loads = [piece(band, part) for band in range(bands) for part in range(pairs)]
    loads[3:3] = own_loads + [pltpu.make_async_copy(theirs_hbm, theirs, theirs_sem.at[0])]
    for load in loads:
        load.start()
    meet(count, parts)
    shared = Lines(count, line_ref, line_out_ref, lines, line_send, line_recv)
    buffers = (pair_sent, pair_got, cross_sent, cross_got, kept)
    sems = (pair_send, pair_recv, cross_send, cross_recv)
    grad_in = InputGrad(parts, grads, weights, input_ref, buffers, sems)

    chunks, depth, tile = x_sent.shape[0], x_sent.shape[2], x_sent.shape[3]
    per = chunks // 3
    outs = (oq_ref, ok_ref, ov_ref)
    deep = 2 * (1 + made)
    rim = 6 * made
    slot = jnp.where(inner, 0, 1)

    def columns(chunk):
        return pl.ds(pl.multiple_of(lax.rem(chunk, per) * tile, tile), tile)

    def swap(chunk):
        return remote(
            grads.at[chunk // per, :, columns(chunk)],
            their_grads.at[chunk // per, :, columns(chunk)],
            swap_send.at[chunk],
            swap_recv.at[chunk],
            {"sp": partner},
        )

    def x_copy(chunk):
        return remote(
            x_sent.at[chunk],
            x_got.at[chunk],
            x_send.at[chunk],
            x_recv.at[chunk],
            {"sp": 2 * level + 1 - side},
        )

    def deep_copy(chunk):
        return remote(
            sent.at[0, chunk],
            got.at[slot, chunk],
            send_sem.at[0, chunk],
            recv_sem.at[slot, chunk],
            {"sp": deep + side},
        )

    def rim_copy(chunk):
        return remote(
            sent.at[1, chunk],
            got.at[0, chunk],
            send_sem.at[1, chunk],
            recv_sem.at[0, chunk],
            {"sp": rim + side},
        )

    def arrived(chunk, which):
        return remote(
            sent.at[0, chunk],
            got.at[which, chunk],
            send_sem.at[0, chunk],
            recv_sem.at[which, chunk],
            {"sp": deep + side},
        )

    def sums(target, chunk):
        start = pl.multiple_of((target - made * (count // 2)) * depth, depth)
        features = pl.ds(start, depth)
        mine = grads[chunk // per, :, columns(chunk)]
        other = their_grads[chunk // per, :, columns(chunk)]
        term = jnp.dot(turned[features, :length], mine, preferred_element_type=jnp.float32)
        return term + jnp.dot(
            turned[features, length:], other, preferred_element_type=jnp.float32
        )

    def halve(chunk):
        swap(chunk).wait_recv()
        x_sent[chunk, 0] = sums(deep + 1 - side, chunk).astype(jnp.bfloat16)
        x_sent[chunk, 1] = sums(rim + 1 - side, chunk).astype(jnp.bfloat16)
        x_copy(chunk).start()

    def onward(chunk):
        term = sums(deep + side, chunk)
        x_copy(chunk).wait_recv()
        term = term + x_got[chunk, 0].astype(jnp.float32)
        sent[0, chunk] = term.astype(jnp.bfloat16)
        deep_copy(chunk).start()
        term = sums(rim + side, chunk) + x_got[chunk, 1].astype(jnp.float32)

        @pl.when(inner)
        def _():
            sent[1, chunk] = term.astype(jnp.bfloat16)

        @pl.when(jnp.logical_not(inner))
        def _():
            result[chunk // per, :, columns(chunk)] = term

    def store(chunk, matrix):
        return pltpu.make_async_copy(
            result.at[matrix, :, columns(chunk)],
            outs[matrix].at[:, columns(chunk)],
            out_sem.at[chunk],
        )

    def finish(chunk):
        arrived(chunk, 0).wait_recv()
        term = got[0, chunk].astype(jnp.float32)

        @pl.when(inner)
        def _():
            arrived(chunk, 1).wait_recv()
            total = term + got[1, chunk].astype(jnp.float32)
            result[chunk // per, :, columns(chunk)] = total

        @pl.when(jnp.logical_not(inner))
        def _():
            total = term + result[chunk // per, :, columns(chunk)]
            result[chunk // per, :, columns(chunk)] = total

        for matrix in range(3):

            @pl.when(chunk // per == matrix)
            def _():
                store(chunk, matrix).start()

    for which in range(3):
        loads[which].wait()
        for chunk in range(per):
            swap(which * per + chunk).start()
    shared.start()
    for load in loads[3:-3]:
        load.wait()

    @pl.loop(0, bands)
    def _(band):
        start = pl.multiple_of(band * REACH, REACH)
        for part in range(pairs):
            low = slice(part * block, (part + 1) * block)
            turned[low, pl.ds(start, REACH)] = pair_sent[band, part].T
            turned[low, pl.ds(length + start, REACH)] = theirs[pl.ds(start, REACH), low].T

    hold = 2
    rest = hold + 2
    lag = 3 * chunks // 4

    @pl.loop(0, chunks + lag)
    def _(step):
        @pl.when(step < chunks)
        def _():
            halve(step)

        @pl.when((step >= hold) & (step < chunks + hold))
        def _():
            onward(step - hold)

        @pl.when(inner & (step >= rest) & (step < chunks + hold))
        def _():
            rim_copy(step - rest).start()

        @pl.when(inner & (step == chunks + hold))
        def _():
            for chunk in range(chunks + hold - rest, chunks):
                rim_copy(chunk).start()

        @pl.when(step >= lag)
        def _():
            finish(step - lag)

        unit = (step - 1) // 2

        @pl.when(step == 1)
        def _():
            for load in loads[-3:]:
                load.wait()

        @pl.when((lax.rem(step, 2) == 1) & (unit < grad_in.units))
        def _():
            grad_in.work(unit)

    for unit in range(min((chunks + lag) // 2, grad_in.units), grad_in.units):
        grad_in.work(unit)
    shared.finish()
    grad_in.finish(grad_in.bands - 1)

    @pl.loop(0, chunks)
    def _(chunk):
        swap(chunk).wait_send()
        x_copy(chunk).wait_send()
        deep_copy(chunk).wait_send()
        store(chunk, 0).wait()

        @pl.when(inner)
        def _():
            rim_copy(chunk).wait_send()

    grad_in.drain()


def final_grads(whole, theirs, grads, lines, weights, entries):
    count = lax.axis_size("sp")
    parts = lax.axis_size("tp")
    pairs = parts // 2
    length, features = whole.shape
    width = weights[0].shape[1]
    depth = features // count
    block = features // parts
    bands = length // REACH
    vmem = pl.BlockSpec(memory_space=pltpu.VMEM)
    anywhere = pl.BlockSpec(memory_space=pl.ANY)
    out = jax.ShapeDtypeStruct((depth, width), jnp.float32)
    dma = pltpu.SemaphoreType.DMA
    low = jnp.bfloat16
    pair = paired(count, parts)
    tile = min(width, LANES)
    chunks = 3 * width // tile
    scratch = [
        pltpu.VMEM((features // 2, 2 * length) if pair else (length, features), low),
        pltpu.VMEM((3, length, width), low),
        pltpu.VMEM((3, features, width), low),
        pltpu.VMEM((count - 1,) + lines.shape, jnp.float32),
        pltpu.VMEM((bands, pairs, REACH, block), low),
        pltpu.VMEM((bands, pairs, REACH, block), low),
        pltpu.VMEM((bands, pairs - 1, REACH, block), low),
        pltpu.VMEM((bands, pairs - 1, REACH, block), low),
        pltpu.VMEM((bands, REACH, block), jnp.float32),
        dma((7,)),
        dma((count - 1,)),
        dma((count - 1,)),
        dma((bands, pairs)),
        dma((bands, pairs)),
        dma((bands, pairs - 1)),
        dma((bands, pairs - 1)),
    ]
    if pair:
        scratch += [
            pltpu.VMEM((length, features // 2), low),
            pltpu.VMEM((3, length, width), low),
            pltpu.VMEM((chunks, 2, depth, tile), low),
            pltpu.VMEM((chunks, 2, depth, tile), low),
            pltpu.VMEM((2, chunks, depth, tile), low),
            pltpu.VMEM((2, chunks, depth, tile), low),
            pltpu.VMEM((3, depth, width), jnp.float32),
            dma((1 + bands * pairs,)),
            dma((chunks,)),
            dma((chunks,)),
            dma((chunks,)),
            dma((chunks,)),
            dma((2, chunks)),
            dma((2, chunks)),
            dma((chunks,)),
        ]
    else:
        scratch += [
            pltpu.VMEM((2, 3, depth // 2, width), low),
            pltpu.VMEM((2, 3, count - 1, depth // 2, width), low),
            dma((2, 3, count - 1)),
            dma((2, 3, count - 1)),
        ]
    place = anywhere if pair else vmem
    return pl.pallas_call(
        functools.partial(pair_kernel if pair else ring_kernel, count, parts),
        in_specs=[anywhere] * (7 + pair) + [vmem],
        out_specs=[vmem] + [place] * 3 + [vmem],
        out_shape=[
            jax.ShapeDtypeStruct((length, block), low),
            out,
            out,
            out,
            jax.ShapeDtypeStruct((lines.shape[0], entries), jnp.float32),
        ],
        scratch_shapes=scratch,
        compiler_params=pltpu.CompilerParams(
            collective_id=0, has_side_effects=True, vmem_limit_bytes=63 * 1024 * 1024
        ),
        cost_estimate=pl.CostEstimate(
            flops=12 * length * features * width,
            bytes_accessed=400_000_000,
            transcendentals=0,
        ),
    )(whole, *grads, *weights, *theirs, lines)


def gather_kernel(
    parts,
    tokens_ref,
    wq_ref,
    wk_ref,
    wv_ref,
    g_ref,
    bias_ref,
    whole_ref,
    theirs_ref,
    dq_ref,
    dk_ref,
    dv_ref,
    line_ref,
    held,
    weights,
    total,
    halo,
    halo_got,
    back,
    after,
    q_all,
    k_all,
    v_all,
    bias_all,
    bias_sum,
    dk_all,
    dv_all,
    side_send,
    side_recv,
    far_send,
    far_recv,
    relay_send,
    relay_recv,
    halo_send,
    halo_recv,
    back_send,
    back_recv,
    load_sem,
    store_sem,
    *ship_refs,
):
    me = lax.axis_index("tp")
    seat = lax.axis_index("sp")
    seats = lax.axis_size("sp")
    partner = me + 1 - 2 * lax.rem(me, 2)
    chunks = held.shape[0]
    block = tokens_ref.shape[1]
    grain = held.shape[2]
    length = tokens_ref.shape[0]
    heads, entries = bias_ref.shape
    pairs = parts // 2
    matrices = (wq_ref, wk_ref, wv_ref)

    def source(device, away):
        return lax.rem(device + parts - 2 * away, parts)

    order = [me, partner]
    for away in range(1, pairs):
        order += [source(me, away), source(partner, away)]

    def load(slot, matrix):
        start = pl.multiple_of(order[slot] * block, block)
        return pltpu.make_async_copy(
            matrices[matrix].at[pl.ds(start, block)],
            weights.at[slot, matrix],
            load_sem.at[slot, matrix],
        )

    for slot in range(parts):
        for matrix in range(3):
            load(slot, matrix).start()

    barrier = pltpu.get_barrier_semaphore()
    for ahead in range(1, parts):
        pl.semaphore_signal(
            barrier,
            inc=1,
            device_id={"tp": lax.rem(me + ahead, parts)},
            device_id_type=pl.DeviceIdType.MESH,
        )
    onward = lax.rem(seat + 1, seats)
    for other in (onward, lax.rem(seat + seats - 1, seats)):
        pl.semaphore_signal(
            barrier, inc=1, device_id={"sp": other}, device_id_type=pl.DeviceIdType.MESH
        )
    ship = len(ship_refs) > 0
    if ship:
        level, lane, inner, near, made, mate = pair_places(seat)
        pl.semaphore_signal(
            barrier, inc=1, device_id={"sp": mate}, device_id_type=pl.DeviceIdType.MESH
        )
    pl.semaphore_wait(barrier, parts + 1 + ship)

    def rows(chunk):
        return pl.ds(chunk * grain, grain)

    def far(chunk, away):
        return remote(
            tokens_ref.at[rows(chunk)],
            held.at[chunk, me],
            far_send.at[chunk, away - 1],
            far_recv.at[chunk, away - 1],
            {"tp": lax.rem(me + 2 * away, parts)},
        )

    def side(chunk):
        return remote(
            tokens_ref.at[rows(chunk)],
            held.at[chunk, me],
            side_send.at[chunk],
            side_recv.at[chunk],
            {"tp": partner},
        )

    def relay(chunk, away):
        place = held.at[chunk, source(me, away)]
        return remote(
            place,
            place,
            relay_send.at[chunk, away - 1],
            relay_recv.at[chunk, away - 1],
            {"tp": partner},
        )

    def neighbour():
        return remote(halo, halo_got, halo_send, halo_recv, {"sp": onward})

    def behind():
        device = {"sp": lax.rem(seat + seats - 1, seats)}
        return remote(back, after, back_send, back_recv, device)

    scratch = (bias_all, bias_sum, dk_all, dv_all)
    factor = (q_all.shape[1] // heads) ** (-0.5)
    work = Attention(factor, heads, q_all, k_all, v_all, g_ref, dq_ref, scratch)

    def store(chunk, slot):
        start = pl.multiple_of(order[slot] * block, block)
        src = tokens_ref.at[rows(chunk)] if slot == 0 else held.at[chunk, order[slot]]
        return pltpu.make_async_copy(
            src, whole_ref.at[rows(chunk), pl.ds(start, block)], store_sem.at[chunk, slot]
        )

    def add(chunk, slot, value):
        for matrix in range(3):
            term = jnp.dot(value, weights[slot, matrix], preferred_element_type=jnp.float32)
            if slot == 0:
                total[matrix, chunk] = term
            else:
                total[matrix, chunk] += term

    if ship:
        ship_got, ship_send, ship_recv, pass_send, pass_recv, keep_sem = ship_refs
        core = lax.rem(me, 2)
        shipped = jnp.where(inner, near, 1 - near)
        ready = me // 2 == shipped

        def ship_copy(chunk, src):
            return remote(
                src,
                ship_got.at[chunk, core],
                ship_send.at[chunk],
                ship_recv.at[chunk],
                {"sp": mate},
            )

        def pass_on(chunk):
            place = ship_got.at[chunk, core]
            return remote(
                place, place, pass_send.at[chunk], pass_recv.at[chunk], {"tp": partner}
            )

        def keep(chunk, which):
            start = pl.multiple_of(which * block, block)
            return pltpu.make_async_copy(
                ship_got.at[chunk, which],
                theirs_ref.at[rows(chunk), pl.ds(start, block)],
                keep_sem.at[chunk, which],
            )

    tail = REACH // grain
    sequence = list(range(chunks - tail, chunks)) + list(range(chunks - tail))
    for chunk in sequence:
        for away in range(1, pairs):
            far(chunk, away).start()
        side(chunk).start()
    for slot in range(2):
        for matrix in range(3):
            load(slot, matrix).wait()
        for chunk in sequence:
            if slot == 1:
                side(chunk).wait_recv()
            store(chunk, slot).start()
            value = tokens_ref[rows(chunk)] if slot == 0 else held[chunk, partner]
            add(chunk, slot, value)
    for slot in range(2, parts):
        for matrix in range(3):
            load(slot, matrix).wait()
    work.begin(exact(bias_ref[...], table_map(entries), 0))
    done = []
    waiting = list(range(0, length, ROWS))

    def attend_ready(early):
        known = {row for chunk in done for row in range(chunk * grain, (chunk + 1) * grain, ROWS)}
        for start in list(waiting):
            needs = range(max(0, start - REACH), start + ROWS, ROWS)
            if start < REACH and early:
                continue
            if set(needs) <= known:
                if start == 0:
                    take_halo()
                work.attend(start)
                waiting.remove(start)
                if start == REACH - ROWS:
                    send_behind()

    def take_halo():
        @pl.when(seat > 0)
        def _():
            neighbour().wait_recv()

        @pl.when(seat == 0)
        def _():
            halo_got[...] = jnp.zeros_like(halo_got)

        k_all[:REACH] = halo_got[0]
        v_all[:REACH] = halo_got[1]

    def send_behind():
        @pl.when(seat > 0)
        def _():
            work.behind(back)
            behind().start()

    for chunk in sequence:
        for away in range(1, pairs):
            far(chunk, away).wait_recv()
            relay(chunk, away).start()
            if ship:

                @pl.when(ready)
                def _():
                    ship_copy(chunk, tokens_ref.at[rows(chunk)]).start()

                @pl.when(jnp.logical_not(ready))
                def _():
                    ship_copy(chunk, held.at[chunk, source(me, 1)]).start()

            store(chunk, 2 * away).start()
            add(chunk, 2 * away, held[chunk, source(me, away)])
        for away in range(1, pairs):
            relay(chunk, away).wait_recv()
            store(chunk, 2 * away + 1).start()
            add(chunk, 2 * away + 1, held[chunk, source(partner, away)])
        low = chunk * grain
        q_all[low : low + grain] = total[0, chunk].astype(jnp.bfloat16)
        k_all[REACH + low : REACH + low + grain] = total[1, chunk].astype(jnp.bfloat16)
        v_all[REACH + low : REACH + low + grain] = total[2, chunk].astype(jnp.bfloat16)
        done.append(chunk)
        if chunk == chunks - 1:
            halo[0] = k_all[length:]
            halo[1] = v_all[length:]

            @pl.when(seat < seats - 1)
            def _():
                neighbour().start()

        attend_ready(len(done) < chunks - 1)
    attend_ready(False)
    work.end(dk_ref, dv_ref, line_ref)

    @pl.when(seat < seats - 1)
    def _():
        behind().wait_recv()

    @pl.when(seat == seats - 1)
    def _():
        after[...] = jnp.zeros_like(after)

    work.join(dk_ref, dv_ref, after)

    @pl.when(seat > 0)
    def _():
        behind().wait_send()

    @pl.when(seat < seats - 1)
    def _():
        neighbour().wait_send()

    if ship:
        for chunk in sequence:
            ship_copy(chunk, tokens_ref.at[rows(chunk)]).wait_recv()
            pass_on(chunk).start()
            keep(chunk, core).start()
        for chunk in sequence:
            pass_on(chunk).wait_recv()
            keep(chunk, 1 - core).start()
        for chunk in sequence:
            ship_copy(chunk, tokens_ref.at[rows(chunk)]).wait_send()
            pass_on(chunk).wait_send()
            keep(chunk, core).wait()
            keep(chunk, 1 - core).wait()
    for chunk in sequence:
        side(chunk).wait_send()
        for away in range(1, pairs):
            far(chunk, away).wait_send()
            relay(chunk, away).wait_send()
        for slot in range(parts):
            store(chunk, slot).wait()


def attention_grads(tokens, query_weight, key_weight, value_weight, position_bias, out_grad):
    parts = lax.axis_size("tp")
    length, block = tokens.shape
    width = query_weight.shape[1]
    heads = position_bias.shape[0]
    chunks = length // GRAIN
    pairs = parts // 2
    vmem = pl.BlockSpec(memory_space=pltpu.VMEM)
    anywhere = pl.BlockSpec(memory_space=pl.ANY)
    low = jnp.bfloat16

    def shape(kind, *sizes):
        return jax.ShapeDtypeStruct(sizes, kind)

    dma = pltpu.SemaphoreType.DMA
    ship = paired(lax.axis_size("sp"), parts)
    extra = []
    if ship:
        extra = [
            pltpu.VMEM((chunks, 2, GRAIN, block), jnp.bfloat16),
            dma((chunks,)),
            dma((chunks,)),
            dma((chunks,)),
            dma((chunks,)),
            dma((chunks, 2)),
        ]
    return pl.pallas_call(
        functools.partial(gather_kernel, parts),
        in_specs=[vmem, anywhere, anywhere, anywhere, vmem, vmem],
        out_specs=[anywhere] * 2 + [vmem] * 4,
        out_shape=[
            shape(low, length, block * parts),
            shape(low, *((length, 2 * block) if ship else (8, LANES))),
            shape(low, length, width),
            shape(low, length, width),
            shape(low, length, width),
            shape(jnp.float32, heads, TABLE),
        ],
        scratch_shapes=[
            pltpu.VMEM((chunks, parts, GRAIN, block), low),
            pltpu.VMEM((parts, 3, block, width), jnp.bfloat16),
            pltpu.VMEM((3, chunks, GRAIN, width), jnp.float32),
            pltpu.VMEM((2, REACH, width), low),
            pltpu.VMEM((2, REACH, width), low),
            pltpu.VMEM((2, REACH, width), low),
            pltpu.VMEM((2, REACH, width), low),
            pltpu.VMEM((length, width), low),
            pltpu.VMEM((length + REACH, width), low),
            pltpu.VMEM((length + REACH, width), low),
            pltpu.VMEM((heads, ROWS, WINDOW), jnp.float32),
            pltpu.VMEM((heads, ROWS, WINDOW), jnp.float32),
            pltpu.VMEM((length + REACH, width), jnp.float32),
            pltpu.VMEM((length + REACH, width), jnp.float32),
            dma((chunks,)),
            dma((chunks,)),
            dma((chunks, pairs - 1)),
            dma((chunks, pairs - 1)),
            dma((chunks, pairs - 1)),
            dma((chunks, pairs - 1)),
            dma(()),
            dma(()),
            dma(()),
            dma(()),
            dma((parts, 3)),
            dma((chunks, parts)),
        ]
        + extra,
        compiler_params=pltpu.CompilerParams(
            collective_id=1, has_side_effects=True, vmem_limit_bytes=56 * 1024 * 1024
        ),
        cost_estimate=pl.CostEstimate(
            flops=6 * length * block * parts * width, bytes_accessed=150_000_000, transcendentals=0
        ),
    )(tokens, query_weight, key_weight, value_weight, out_grad, position_bias)


def shards(tokens, query_weight, key_weight, value_weight, position_bias, out_grad):
    outs = attention_grads(
        tokens, query_weight, key_weight, value_weight, position_bias, out_grad
    )
    whole, theirs, query_grad, key_grad, value_grad, lines = outs
    *large, bias_grad = final_grads(
        whole,
        (theirs,) if paired(lax.axis_size("sp"), lax.axis_size("tp")) else (),
        (query_grad, key_grad, value_grad),
        lines,
        (query_weight, key_weight, value_weight),
        position_bias.shape[1],
    )
    return (*hand_on(large), bias_grad)


def hand_kernel(*refs):
    half = len(refs) // 2
    for source, target in zip(refs[:half], refs[half:]):
        target[...] = source[...]


def hand_on(arrays, steps=2):
    specs = [
        pl.BlockSpec((array.shape[0], array.shape[1] // steps), lambda i: (0, i))
        for array in arrays
    ]
    size = sum(2 * array.size * array.dtype.itemsize for array in arrays)
    return pl.pallas_call(
        hand_kernel,
        grid=(steps,),
        in_specs=specs,
        out_specs=specs,
        out_shape=[jax.ShapeDtypeStruct(array.shape, array.dtype) for array in arrays],
        cost_estimate=pl.CostEstimate(flops=0, bytes_accessed=size, transcendentals=0),
    )(*arrays)


def solution(mesh):
    in_specs = (
        P("sp", "tp"),
        P(None, "tp"),
        P(None, "tp"),
        P(None, "tp"),
        P("tp", None),
        P("sp", "tp"),
    )
    out_specs = (P("sp", "tp"), P("sp", "tp"), P("sp", "tp"), P("sp", "tp"), P("tp", None))
    return jax.shard_map(shards, mesh=mesh, in_specs=in_specs, out_specs=out_specs, check_vma=False)
```

```python
import functools

import jax
import jax.numpy as jnp
from jax import lax
from jax.experimental import pallas as pl
from jax.experimental.pallas import tpu as pltpu
from jax.sharding import PartitionSpec as P

SEGMENT = 64
PREVIOUS = 4
CLIP = 256
ROWS = 2 * SEGMENT
REACH = PREVIOUS * SEGMENT
WINDOW = ROWS + REACH
TABLE = 512
LANES = 128
GRAIN = 128
HIDDEN = -1e30


def contract_rows(left, right):
    return lax.dot_general(
        left, right, (((0,), (0,)), ((), ())), preferred_element_type=jnp.float32
    )


def contract_cols(left, right):
    return lax.dot_general(
        left, right, (((1,), (1,)), ((), ())), preferred_element_type=jnp.float32
    )


def diagonal_sums(tile):
    half = tile.shape[0] // 2
    while half >= 8:
        tile = tile[:half] + pltpu.roll(tile[half:], TABLE - half, 1)
        half //= 2
    row = lax.broadcasted_iota(jnp.int32, tile.shape, 0)
    for step in (4, 2, 1):
        tile = jnp.where((row & step) != 0, pltpu.roll(tile, TABLE - step, 1), tile)
    return jnp.sum(tile, axis=0, keepdims=True)


def table_map(entries):
    entry = lax.broadcasted_iota(jnp.int32, (entries, TABLE), 0)
    column = lax.broadcasted_iota(jnp.int32, (entries, TABLE), 1)
    near = column + entry == entries - 1
    far = (column >= WINDOW) & (entry == entries - 1)
    return jnp.where(near | far, 1.0, 0.0).astype(jnp.float32)


def exact(left, right, axis):
    return lax.dot_general(
        left,
        right,
        (((1,), (axis,)), ((), ())),
        precision=lax.Precision.HIGHEST,
        preferred_element_type=jnp.float32,
    )


class Attention:
    def __init__(self, factor, heads, q_all, k_all, v_all, g_ref, dq_ref, scratch):
        self.factor, self.heads = factor, heads
        self.q_all, self.k_all, self.v_all = q_all, k_all, v_all
        self.g_ref, self.dq_ref = g_ref, dq_ref
        self.bias_all, self.bias_sum, self.dk_all, self.dv_all = scratch
        self.head = q_all.shape[1] // heads

    def begin(self, table_rows):
        self.dk_all[...] = jnp.zeros_like(self.dk_all)
        self.dv_all[...] = jnp.zeros_like(self.dv_all)
        self.bias_sum[...] = jnp.zeros_like(self.bias_sum)
        row = lax.broadcasted_iota(jnp.int32, (ROWS, WINDOW), 0) // SEGMENT
        column = lax.broadcasted_iota(jnp.int32, (ROWS, WINDOW), 1)
        behind = column // SEGMENT - row
        seen = (behind >= 0) & (behind <= PREVIOUS)
        for head in range(self.heads):
            table = jnp.broadcast_to(table_rows[head : head + 1], (ROWS, TABLE))
            bias = pltpu.roll(table, 0, 1, stride=1, stride_axis=0)[:, :WINDOW]
            self.bias_all[head] = jnp.where(seen, bias, HIDDEN)

    def attend(self, start):
        @pl.loop(0, self.heads, unroll=2)
        def _(head):
            columns = pl.ds(pl.multiple_of(head * self.head, self.head), self.head)
            rows = slice(start, start + ROWS)
            window = slice(start, start + WINDOW)
            q = self.q_all[rows, columns]
            g = self.g_ref[rows, columns]
            k = self.k_all[window, columns]
            v = self.v_all[window, columns]
            mask = self.bias_all[head]
            if start < REACH:
                first = jnp.where(lax.axis_index("sp") == 0, REACH - start, 0)
                column = lax.broadcasted_iota(jnp.int32, (ROWS, WINDOW), 1)
                mask = jnp.where(column < first, HIDDEN, mask)
            scores = contract_cols(q, k) * self.factor + mask
            top = jnp.max(scores, axis=1, keepdims=True)
            raised = jnp.exp(scores - top)
            weights = raised * (1.0 / jnp.sum(raised, axis=1, keepdims=True))
            prob_grad = contract_cols(g, v)
            delta = jnp.sum(weights * prob_grad, axis=1, keepdims=True)
            score_grad = weights * (prob_grad - delta)
            self.bias_sum[head] += score_grad
            low = score_grad.astype(jnp.bfloat16)
            dq = jnp.dot(low, k, preferred_element_type=jnp.float32) * self.factor
            self.dq_ref[rows, columns] = dq.astype(jnp.bfloat16)
            self.dk_all[window, columns] += contract_rows(low, q)
            self.dv_all[window, columns] += contract_rows(weights.astype(jnp.bfloat16), g)

    def behind(self, back):
        back[0] = (self.dk_all[:REACH] * self.factor).astype(jnp.bfloat16)
        back[1] = self.dv_all[:REACH].astype(jnp.bfloat16)

    def end(self, dk_ref, dv_ref, line_ref):
        length = self.q_all.shape[0]
        body = length - REACH
        dk_all, dv_all, factor = self.dk_all, self.dv_all, self.factor
        dk_ref[:body] = (dk_all[REACH:length] * factor).astype(jnp.bfloat16)
        dv_ref[:body] = dv_all[REACH:length].astype(jnp.bfloat16)
        for head in range(self.heads):
            blank = jnp.zeros((ROWS, TABLE - WINDOW), jnp.float32)
            padded = jnp.concatenate([self.bias_sum[head], blank], axis=1)
            line_ref[head : head + 1] = diagonal_sums(padded)

    def join(self, dk_ref, dv_ref, after):
        length = self.q_all.shape[0]
        dk = self.dk_all[length:] * self.factor + after[0].astype(jnp.float32)
        dk_ref[length - REACH :] = dk.astype(jnp.bfloat16)
        dv = self.dv_all[length:] + after[1].astype(jnp.float32)
        dv_ref[length - REACH :] = dv.astype(jnp.bfloat16)


def ring_columns(count):
    columns = 1
    while (2 * columns) ** 2 <= count:
        columns *= 2
    return columns


def ring_place(index, count):
    columns = ring_columns(count)
    rows = count // columns
    row, column = index // columns, index % columns
    above = rows - 1 - row
    across = jnp.where(above % 2 == 0, column - 1, columns - 1 - column)
    return jnp.where(column == 0, row, rows + above * (columns - 1) + across)


def ring_index(place, count):
    columns = ring_columns(count)
    rows = count // columns
    later = jnp.maximum(place - rows, 0)
    above, across = later // (columns - 1), later % (columns - 1)
    column = jnp.where(above % 2 == 0, 1 + across, columns - 1 - across)
    return jnp.where(place < rows, place * columns, (rows - 1 - above) * columns + column)


def remote(src, dst, send, recv, device):
    return pltpu.make_async_remote_copy(
        src_ref=src,
        dst_ref=dst,
        send_sem=send,
        recv_sem=recv,
        device_id=device,
        device_id_type=pl.DeviceIdType.MESH,
    )


def meet(count, parts):
    me = lax.axis_index("sp")
    seat = lax.axis_index("tp")
    barrier = pltpu.get_barrier_semaphore()
    for ahead in range(1, count):
        peer = lax.rem(me + ahead, count)
        pl.semaphore_signal(
            barrier, inc=1, device_id={"sp": peer}, device_id_type=pl.DeviceIdType.MESH
        )
    for ahead in range(1, parts):
        peer = lax.rem(seat + ahead, parts)
        pl.semaphore_signal(
            barrier, inc=1, device_id={"tp": peer}, device_id_type=pl.DeviceIdType.MESH
        )
    pl.semaphore_wait(barrier, count + parts - 2)


def final_loads(hbm, grads, weights, load_sem):
    dq_hbm, dk_hbm, dv_hbm, wq_hbm, wk_hbm, wv_hbm = hbm
    return [
        pltpu.make_async_copy(dq_hbm, grads.at[0], load_sem.at[0]),
        pltpu.make_async_copy(dk_hbm, grads.at[1], load_sem.at[1]),
        pltpu.make_async_copy(dv_hbm, grads.at[2], load_sem.at[2]),
        pltpu.make_async_copy(wq_hbm, weights.at[0], load_sem.at[3]),
        pltpu.make_async_copy(wk_hbm, weights.at[1], load_sem.at[4]),
        pltpu.make_async_copy(wv_hbm, weights.at[2], load_sem.at[5]),
    ]


class Lines:
    def __init__(self, count, line_ref, out_ref, lines, send, recv):
        self.me = lax.axis_index("sp")
        self.count = count
        self.line_ref, self.out_ref, self.lines = line_ref, out_ref, lines
        self.sems = (send, recv)

    def copy(self, ahead):
        return remote(
            self.line_ref,
            self.lines.at[ahead - 1],
            self.sems[0].at[ahead - 1],
            self.sems[1].at[ahead - 1],
            {"sp": lax.rem(self.me + ahead, self.count)},
        )

    def start(self):
        for ahead in range(1, self.count):
            self.copy(ahead).start()

    def finish(self):
        total = self.line_ref[...]
        for ahead in range(1, self.count):
            self.copy(ahead).wait()
            total = total + self.lines[ahead - 1]
        self.out_ref[...] = exact(total, table_map(self.out_ref.shape[1]), 1)


class InputGrad:
    def __init__(self, parts, grads, weights, input_ref, buffers, sems):
        self.seat = lax.axis_index("tp")
        self.core = lax.rem(self.seat, 2)
        self.row = self.seat // 2
        self.parts, self.pairs = parts, parts // 2
        self.grads, self.weights, self.input_ref = grads, weights, input_ref
        self.pair_sent, self.pair_got, self.cross_sent, self.cross_got, self.kept = buffers
        self.sems = sems
        self.block = input_ref.shape[1]
        self.bands = input_ref.shape[0] // REACH
        self.units = 2 * self.bands

    def rows(self, band):
        return pl.ds(pl.multiple_of(band * REACH, REACH), REACH)

    def part(self, band, target):
        block = pl.ds(pl.multiple_of(target * self.block, self.block), self.block)
        rows = self.rows(band)
        term = contract_cols(self.grads[0, rows], self.weights[0, block])
        term += contract_cols(self.grads[1, rows], self.weights[1, block])
        return term + contract_cols(self.grads[2, rows], self.weights[2, block])

    def pair_copy(self, band, away):
        return remote(
            self.pair_sent.at[band, away],
            self.pair_got.at[band, away],
            self.sems[0].at[band, away],
            self.sems[1].at[band, away],
            {"tp": self.seat + 1 - 2 * self.core},
        )

    def cross_copy(self, band, away):
        return remote(
            self.cross_sent.at[band, away - 1],
            self.cross_got.at[band, away - 1],
            self.sems[2].at[band, away - 1],
            self.sems[3].at[band, away - 1],
            {"tp": lax.rem(self.seat + 2 * away, self.parts)},
        )

    def to_partner(self, band):
        for away in range(self.pairs):
            target = 2 * lax.rem(self.row + away, self.pairs) + 1 - self.core
            self.pair_sent[band, away] = self.part(band, target).astype(jnp.bfloat16)
            self.pair_copy(band, away).start()

    def across(self, band):
        for away in range(1, self.pairs):
            term = self.part(band, lax.rem(self.seat + 2 * away, self.parts))
            self.pair_copy(band, away).wait_recv()
            term = term + self.pair_got[band, away].astype(jnp.float32)
            self.cross_sent[band, away - 1] = term.astype(jnp.bfloat16)
            self.cross_copy(band, away).start()
        term = self.part(band, self.seat)
        self.pair_copy(band, 0).wait_recv()
        self.kept[band] = term + self.pair_got[band, 0].astype(jnp.float32)

    def finish(self, band):
        term = self.kept[band]
        for away in range(1, self.pairs):
            self.cross_copy(band, away).wait_recv()
            term = term + self.cross_got[band, away - 1].astype(jnp.float32)
        self.input_ref[self.rows(band)] = term.astype(jnp.bfloat16)

    def work(self, unit):
        band = unit // 2

        @pl.when(lax.rem(unit, 2) == 0)
        def _():
            self.to_partner(band)

        @pl.when(lax.rem(unit, 2) == 1)
        def _():
            self.across(band)

        @pl.when((lax.rem(unit, 2) == 1) & (unit > 2))
        def _():
            self.finish(band - 1)

    def drain(self):
        @pl.loop(0, self.bands)
        def _(band):
            for away in range(self.pairs):
                self.pair_copy(band, away).wait_send()
            for away in range(1, self.pairs):
                self.cross_copy(band, away).wait_send()


def ring_kernel(
    count,
    parts,
    whole_hbm,
    dq_hbm,
    dk_hbm,
    dv_hbm,
    wq_hbm,
    wk_hbm,
    wv_hbm,
    line_ref,
    input_ref,
    oq_ref,
    ok_ref,
    ov_ref,
    line_out_ref,
    whole,
    grads,
    weights,
    lines,
    pair_sent,
    pair_got,
    cross_sent,
    cross_got,
    kept,
    load_sem,
    line_send,
    line_recv,
    pair_send,
    pair_recv,
    cross_send,
    cross_recv,
    sent,
    got,
    send_sem,
    recv_sem,
):
    me = lax.axis_index("sp")
    place = ring_place(me, count)
    hbm = (dq_hbm, dk_hbm, dv_hbm, wq_hbm, wk_hbm, wv_hbm)
    loads = final_loads(hbm, grads, weights, load_sem)
    loads.append(pltpu.make_async_copy(whole_hbm, whole, load_sem.at[6]))
    for load in loads:
        load.start()
    meet(count, parts)
    shared = Lines(count, line_ref, line_out_ref, lines, line_send, line_recv)
    buffers = (pair_sent, pair_got, cross_sent, cross_got, kept)
    sems = (pair_send, pair_recv, cross_send, cross_recv)
    grad_in = InputGrad(parts, grads, weights, input_ref, buffers, sems)

    outs = (oq_ref, ok_ref, ov_ref)
    half = got.shape[3]
    onward = (
        ring_index(lax.rem(place + 1, count), count),
        ring_index(lax.rem(place + count - 1, count), count),
    )

    def own(target, side, chain):
        start = pl.multiple_of((2 * ring_index(target, count) + side) * half, half)
        return contract_rows(whole[:, pl.ds(start, half)], grads[chain])

    def target_of(step, side):
        if side == 0:
            return lax.rem(place - 1 - step + 2 * count, count)
        return lax.rem(place + 1 + step, count)

    def copy_of(src, step, side, chain):
        return remote(
            src,
            got.at[side, chain, step],
            send_sem.at[side, chain, step],
            recv_sem.at[side, chain, step],
            {"sp": onward[side]},
        )

    for load in loads:
        load.wait()
    for chain in range(3):
        for side in range(2):
            sent[side, chain] = own(target_of(0, side), side, chain).astype(jnp.bfloat16)
            copy_of(sent.at[side, chain], 0, side, chain).start()
    shared.start()

    chains = [(chain, side) for chain in range(3) for side in range(2)]

    @pl.loop(1, count - 1)
    def _(step):
        for chain, side in chains:
            part_of = own(target_of(step, side), side, chain)
            place_of = got.at[side, chain, step - 1]
            copy_of(sent.at[side, chain], step - 1, side, chain).wait_recv()
            total = part_of + place_of[...].astype(jnp.float32)
            place_of[...] = total.astype(jnp.bfloat16)
            copy_of(place_of, step, side, chain).start()
            if (chain, side) == (1, 1):

                @pl.when(step <= grad_in.units)
                def _():
                    grad_in.work(step - 1)

    for unit in range(min(count - 2, grad_in.units), grad_in.units):
        grad_in.work(unit)
    shared.finish()
    for chain, side in chains:
        if (chain, side) == (2, 0):
            grad_in.finish(grad_in.bands - 1)
        part_of = own(place, side, chain)
        copy_of(sent.at[side, chain], count - 2, side, chain).wait_recv()
        total = part_of + got[side, chain, count - 2].astype(jnp.float32)
        outs[chain][side * half : (side + 1) * half] = total

    @pl.loop(0, count - 1)
    def _(step):
        for chain, side in chains:
            copy_of(sent.at[side, chain], step, side, chain).wait_send()

    grad_in.drain()


def paired(count, parts):
    return count == 8 and ring_columns(count) == 2 and parts == 4


def pair_places(me):
    level, side = me // 2, lax.rem(me, 2)
    inner = (level == 1) | (level == 2)
    near = level // 2
    made = jnp.where(inner, 1 - near, near)
    partner = 2 * (level + 1 - 2 * lax.rem(level, 2)) + side
    return level, side, inner, near, made, partner


def pair_kernel(
    count,
    parts,
    whole_hbm,
    dq_hbm,
    dk_hbm,
    dv_hbm,
    wq_hbm,
    wk_hbm,
    wv_hbm,
    theirs_hbm,
    line_ref,
    input_ref,
    oq_ref,
    ok_ref,
    ov_ref,
    line_out_ref,
    turned,
    grads,
    weights,
    lines,
    pair_sent,
    pair_got,
    cross_sent,
    cross_got,
    kept,
    load_sem,
    line_send,
    line_recv,
    pair_send,
    pair_recv,
    cross_send,
    cross_recv,
    theirs,
    their_grads,
    x_sent,
    x_got,
    sent,
    got,
    result,
    theirs_sem,
    swap_send,
    swap_recv,
    x_send,
    x_recv,
    send_sem,
    recv_sem,
    out_sem,
):
    me = lax.axis_index("sp")
    level, side, inner, near, made, partner = pair_places(me)
    hbm = (dq_hbm, dk_hbm, dv_hbm, wq_hbm, wk_hbm, wv_hbm)
    loads = final_loads(hbm, grads, weights, load_sem)
    bands, pairs, _, block = pair_sent.shape
    length = grads.shape[1]

    def rows(band):
        return pl.ds(band * REACH, REACH)

    def piece(band, part):
        start = pl.multiple_of((made * pairs + part) * block, block)
        return pltpu.make_async_copy(
            whole_hbm.at[rows(band), pl.ds(start, block)],
            pair_sent.at[band, part],
            theirs_sem.at[1 + band * pairs + part],
        )

    own_loads = [piece(band, part) for band in range(bands) for part in range(pairs)]
    loads[3:3] = own_loads + [pltpu.make_async_copy(theirs_hbm, theirs, theirs_sem.at[0])]
    for load in loads:
        load.start()
    meet(count, parts)
    shared = Lines(count, line_ref, line_out_ref, lines, line_send, line_recv)
    buffers = (pair_sent, pair_got, cross_sent, cross_got, kept)
    sems = (pair_send, pair_recv, cross_send, cross_recv)
    grad_in = InputGrad(parts, grads, weights, input_ref, buffers, sems)

    chunks, depth, tile = x_sent.shape[0], x_sent.shape[2], x_sent.shape[3]
    per = chunks // 3
    outs = (oq_ref, ok_ref, ov_ref)
    deep = 2 * (1 + made)
    rim = 6 * made
    slot = jnp.where(inner, 0, 1)

    def columns(chunk):
        return pl.ds(pl.multiple_of(lax.rem(chunk, per) * tile, tile), tile)

    def swap(chunk):
        return remote(
            grads.at[chunk // per, :, columns(chunk)],
            their_grads.at[chunk // per, :, columns(chunk)],
            swap_send.at[chunk],
            swap_recv.at[chunk],
            {"sp": partner},
        )

    def x_copy(chunk, which):
        return remote(
            x_sent.at[chunk, which],
            x_got.at[chunk, which],
            x_send.at[chunk, which],
            x_recv.at[chunk, which],
            {"sp": 2 * level + 1 - side},
        )

    def deep_copy(chunk):
        return remote(
            sent.at[0, chunk],
            got.at[slot, chunk],
            send_sem.at[0, chunk],
            recv_sem.at[slot, chunk],
            {"sp": deep + side},
        )

    def rim_copy(chunk):
        return remote(
            sent.at[1, chunk],
            got.at[0, chunk],
            send_sem.at[1, chunk],
            recv_sem.at[0, chunk],
            {"sp": rim + side},
        )

    def arrived(chunk, which):
        return remote(
            sent.at[0, chunk],
            got.at[which, chunk],
            send_sem.at[0, chunk],
            recv_sem.at[which, chunk],
            {"sp": deep + side},
        )

    def sums(target, chunk):
        start = pl.multiple_of((target - made * (count // 2)) * depth, depth)
        features = pl.ds(start, depth)
        mine = grads[chunk // per, :, columns(chunk)]
        other = their_grads[chunk // per, :, columns(chunk)]
        term = jnp.dot(turned[features, :length], mine, preferred_element_type=jnp.float32)
        return term + jnp.dot(
            turned[features, length:], other, preferred_element_type=jnp.float32
        )

    def halve(chunk):
        swap(chunk).wait_recv()
        x_sent[chunk, 0] = sums(deep + 1 - side, chunk).astype(jnp.bfloat16)
        x_copy(chunk, 0).start()
        x_sent[chunk, 1] = sums(rim + 1 - side, chunk).astype(jnp.bfloat16)
        x_copy(chunk, 1).start()

    def onward(chunk):
        term = sums(deep + side, chunk)
        x_copy(chunk, 0).wait_recv()
        term = term + x_got[chunk, 0].astype(jnp.float32)
        sent[0, chunk] = term.astype(jnp.bfloat16)
        deep_copy(chunk).start()
        term = sums(rim + side, chunk)
        x_copy(chunk, 1).wait_recv()
        term = term + x_got[chunk, 1].astype(jnp.float32)

        @pl.when(inner)
        def _():
            sent[1, chunk] = term.astype(jnp.bfloat16)

        @pl.when(jnp.logical_not(inner))
        def _():
            result[chunk // per, :, columns(chunk)] = term

    def store(chunk, matrix):
        return pltpu.make_async_copy(
            result.at[matrix, :, columns(chunk)],
            outs[matrix].at[:, columns(chunk)],
            out_sem.at[chunk],
        )

    def finish(chunk):
        arrived(chunk, 0).wait_recv()
        term = got[0, chunk].astype(jnp.float32)

        @pl.when(inner)
        def _():
            arrived(chunk, 1).wait_recv()
            total = term + got[1, chunk].astype(jnp.float32)
            result[chunk // per, :, columns(chunk)] = total

        @pl.when(jnp.logical_not(inner))
        def _():
            total = term + result[chunk // per, :, columns(chunk)]
            result[chunk // per, :, columns(chunk)] = total

        for matrix in range(3):

            @pl.when(chunk // per == matrix)
            def _():
                store(chunk, matrix).start()

    for which in range(3):
        loads[which].wait()
        for chunk in range(per):
            swap(which * per + chunk).start()
    shared.start()
    for load in loads[3:-3]:
        load.wait()

    @pl.loop(0, bands)
    def _(band):
        start = pl.multiple_of(band * REACH, REACH)
        for part in range(pairs):
            low = slice(part * block, (part + 1) * block)
            turned[low, pl.ds(start, REACH)] = pair_sent[band, part].T
            turned[low, pl.ds(length + start, REACH)] = theirs[pl.ds(start, REACH), low].T

    hold = 2
    rest = hold + 2
    lag = 3 * chunks // 4

    @pl.loop(0, chunks + lag)
    def _(step):
        @pl.when(step < chunks)
        def _():
            halve(step)

        @pl.when((step >= hold) & (step < chunks + hold))
        def _():
            onward(step - hold)

        @pl.when(inner & (step >= rest) & (step < chunks + hold))
        def _():
            rim_copy(step - rest).start()

        @pl.when(inner & (step == chunks + hold))
        def _():
            for chunk in range(chunks + hold - rest, chunks):
                rim_copy(chunk).start()

        @pl.when(step >= lag)
        def _():
            finish(step - lag)

        unit = (step - 1) // 2

        @pl.when(step == 1)
        def _():
            for load in loads[-3:]:
                load.wait()

        @pl.when((lax.rem(step, 2) == 1) & (unit < grad_in.units))
        def _():
            grad_in.work(unit)

    for unit in range(min((chunks + lag) // 2, grad_in.units), grad_in.units):
        grad_in.work(unit)
    shared.finish()
    grad_in.finish(grad_in.bands - 1)

    @pl.loop(0, chunks)
    def _(chunk):
        swap(chunk).wait_send()
        x_copy(chunk, 0).wait_send()
        x_copy(chunk, 1).wait_send()
        deep_copy(chunk).wait_send()
        store(chunk, 0).wait()

        @pl.when(inner)
        def _():
            rim_copy(chunk).wait_send()

    grad_in.drain()


def final_grads(whole, theirs, grads, lines, weights, entries):
    count = lax.axis_size("sp")
    parts = lax.axis_size("tp")
    pairs = parts // 2
    length, features = whole.shape
    width = weights[0].shape[1]
    depth = features // count
    block = features // parts
    bands = length // REACH
    vmem = pl.BlockSpec(memory_space=pltpu.VMEM)
    anywhere = pl.BlockSpec(memory_space=pl.ANY)
    out = jax.ShapeDtypeStruct((depth, width), jnp.float32)
    dma = pltpu.SemaphoreType.DMA
    low = jnp.bfloat16
    pair = paired(count, parts)
    tile = min(width, LANES)
    chunks = 3 * width // tile
    scratch = [
        pltpu.VMEM((features // 2, 2 * length) if pair else (length, features), low),
        pltpu.VMEM((3, length, width), low),
        pltpu.VMEM((3, features, width), low),
        pltpu.VMEM((count - 1,) + lines.shape, jnp.float32),
        pltpu.VMEM((bands, pairs, REACH, block), low),
        pltpu.VMEM((bands, pairs, REACH, block), low),
        pltpu.VMEM((bands, pairs - 1, REACH, block), low),
        pltpu.VMEM((bands, pairs - 1, REACH, block), low),
        pltpu.VMEM((bands, REACH, block), jnp.float32),
        dma((7,)),
        dma((count - 1,)),
        dma((count - 1,)),
        dma((bands, pairs)),
        dma((bands, pairs)),
        dma((bands, pairs - 1)),
        dma((bands, pairs - 1)),
    ]
    if pair:
        scratch += [
            pltpu.VMEM((length, features // 2), low),
            pltpu.VMEM((3, length, width), low),
            pltpu.VMEM((chunks, 2, depth, tile), low),
            pltpu.VMEM((chunks, 2, depth, tile), low),
            pltpu.VMEM((2, chunks, depth, tile), low),
            pltpu.VMEM((2, chunks, depth, tile), low),
            pltpu.VMEM((3, depth, width), jnp.float32),
            dma((1 + bands * pairs,)),
            dma((chunks,)),
            dma((chunks,)),
            dma((chunks, 2)),
            dma((chunks, 2)),
            dma((2, chunks)),
            dma((2, chunks)),
            dma((chunks,)),
        ]
    else:
        scratch += [
            pltpu.VMEM((2, 3, depth // 2, width), low),
            pltpu.VMEM((2, 3, count - 1, depth // 2, width), low),
            dma((2, 3, count - 1)),
            dma((2, 3, count - 1)),
        ]
    place = anywhere if pair else vmem
    return pl.pallas_call(
        functools.partial(pair_kernel if pair else ring_kernel, count, parts),
        in_specs=[anywhere] * (7 + pair) + [vmem],
        out_specs=[vmem] + [place] * 3 + [vmem],
        out_shape=[
            jax.ShapeDtypeStruct((length, block), low),
            out,
            out,
            out,
            jax.ShapeDtypeStruct((lines.shape[0], entries), jnp.float32),
        ],
        scratch_shapes=scratch,
        compiler_params=pltpu.CompilerParams(
            collective_id=0, has_side_effects=True, vmem_limit_bytes=63 * 1024 * 1024
        ),
        cost_estimate=pl.CostEstimate(
            flops=12 * length * features * width,
            bytes_accessed=400_000_000,
            transcendentals=0,
        ),
    )(whole, *grads, *weights, *theirs, lines)


def gather_kernel(
    parts,
    tokens_ref,
    wq_ref,
    wk_ref,
    wv_ref,
    g_ref,
    bias_ref,
    whole_ref,
    theirs_ref,
    dq_ref,
    dk_ref,
    dv_ref,
    line_ref,
    held,
    weights,
    total,
    halo,
    halo_got,
    back,
    after,
    q_all,
    k_all,
    v_all,
    bias_all,
    bias_sum,
    dk_all,
    dv_all,
    side_send,
    side_recv,
    far_send,
    far_recv,
    relay_send,
    relay_recv,
    halo_send,
    halo_recv,
    back_send,
    back_recv,
    load_sem,
    store_sem,
    *ship_refs,
):
    me = lax.axis_index("tp")
    seat = lax.axis_index("sp")
    seats = lax.axis_size("sp")
    partner = me + 1 - 2 * lax.rem(me, 2)
    chunks = held.shape[0]
    block = tokens_ref.shape[1]
    grain = held.shape[2]
    length = tokens_ref.shape[0]
    heads, entries = bias_ref.shape
    pairs = parts // 2
    matrices = (wq_ref, wk_ref, wv_ref)

    def source(device, away):
        return lax.rem(device + parts - 2 * away, parts)

    order = [me, partner]
    for away in range(1, pairs):
        order += [source(me, away), source(partner, away)]

    def load(slot, matrix):
        start = pl.multiple_of(order[slot] * block, block)
        return pltpu.make_async_copy(
            matrices[matrix].at[pl.ds(start, block)],
            weights.at[slot, matrix],
            load_sem.at[slot, matrix],
        )

    for slot in range(parts):
        for matrix in range(3):
            load(slot, matrix).start()

    barrier = pltpu.get_barrier_semaphore()
    for ahead in range(1, parts):
        pl.semaphore_signal(
            barrier,
            inc=1,
            device_id={"tp": lax.rem(me + ahead, parts)},
            device_id_type=pl.DeviceIdType.MESH,
        )
    onward = lax.rem(seat + 1, seats)
    for other in (onward, lax.rem(seat + seats - 1, seats)):
        pl.semaphore_signal(
            barrier, inc=1, device_id={"sp": other}, device_id_type=pl.DeviceIdType.MESH
        )
    ship = len(ship_refs) > 0
    if ship:
        level, lane, inner, near, made, mate = pair_places(seat)
        pl.semaphore_signal(
            barrier, inc=1, device_id={"sp": mate}, device_id_type=pl.DeviceIdType.MESH
        )
    pl.semaphore_wait(barrier, parts + 1 + ship)

    def rows(chunk):
        return pl.ds(chunk * grain, grain)

    def far(chunk, away):
        return remote(
            tokens_ref.at[rows(chunk)],
            held.at[chunk, me],
            far_send.at[chunk, away - 1],
            far_recv.at[chunk, away - 1],
            {"tp": lax.rem(me + 2 * away, parts)},
        )

    def side(chunk):
        return remote(
            tokens_ref.at[rows(chunk)],
            held.at[chunk, me],
            side_send.at[chunk],
            side_recv.at[chunk],
            {"tp": partner},
        )

    def relay(chunk, away):
        place = held.at[chunk, source(me, away)]
        return remote(
            place,
            place,
            relay_send.at[chunk, away - 1],
            relay_recv.at[chunk, away - 1],
            {"tp": partner},
        )

    def neighbour():
        return remote(halo, halo_got, halo_send, halo_recv, {"sp": onward})

    def behind():
        device = {"sp": lax.rem(seat + seats - 1, seats)}
        return remote(back, after, back_send, back_recv, device)

    scratch = (bias_all, bias_sum, dk_all, dv_all)
    factor = (q_all.shape[1] // heads) ** (-0.5)
    work = Attention(factor, heads, q_all, k_all, v_all, g_ref, dq_ref, scratch)

    def store(chunk, slot):
        start = pl.multiple_of(order[slot] * block, block)
        src = tokens_ref.at[rows(chunk)] if slot == 0 else held.at[chunk, order[slot]]
        return pltpu.make_async_copy(
            src, whole_ref.at[rows(chunk), pl.ds(start, block)], store_sem.at[chunk, slot]
        )

    def add(chunk, slot, value):
        for matrix in range(3):
            term = jnp.dot(value, weights[slot, matrix], preferred_element_type=jnp.float32)
            if slot == 0:
                total[matrix, chunk] = term
            else:
                total[matrix, chunk] += term

    if ship:
        ship_got, ship_send, ship_recv, pass_send, pass_recv, keep_sem = ship_refs
        core = lax.rem(me, 2)
        shipped = jnp.where(inner, near, 1 - near)
        ready = me // 2 == shipped

        def ship_copy(chunk, src):
            return remote(
                src,
                ship_got.at[chunk, core],
                ship_send.at[chunk],
                ship_recv.at[chunk],
                {"sp": mate},
            )

        def pass_on(chunk):
            place = ship_got.at[chunk, core]
            return remote(
                place, place, pass_send.at[chunk], pass_recv.at[chunk], {"tp": partner}
            )

        def keep(chunk, which):
            start = pl.multiple_of(which * block, block)
            return pltpu.make_async_copy(
                ship_got.at[chunk, which],
                theirs_ref.at[rows(chunk), pl.ds(start, block)],
                keep_sem.at[chunk, which],
            )

    tail = REACH // grain
    sequence = list(range(chunks - tail, chunks)) + list(range(chunks - tail))
    for chunk in sequence:
        for away in range(1, pairs):
            far(chunk, away).start()
        side(chunk).start()
    for slot in range(2):
        for matrix in range(3):
            load(slot, matrix).wait()
        for chunk in sequence:
            if slot == 1:
                side(chunk).wait_recv()
            store(chunk, slot).start()
            value = tokens_ref[rows(chunk)] if slot == 0 else held[chunk, partner]
            add(chunk, slot, value)
    for slot in range(2, parts):
        for matrix in range(3):
            load(slot, matrix).wait()
    work.begin(exact(bias_ref[...], table_map(entries), 0))
    done = []
    waiting = list(range(0, length, ROWS))

    def attend_ready(early):
        known = {row for chunk in done for row in range(chunk * grain, (chunk + 1) * grain, ROWS)}
        for start in list(waiting):
            needs = range(max(0, start - REACH), start + ROWS, ROWS)
            if start < REACH and early:
                continue
            if set(needs) <= known:
                if start == 0:
                    take_halo()
                work.attend(start)
                waiting.remove(start)
                if start == REACH - ROWS:
                    send_behind()

    def take_halo():
        @pl.when(seat > 0)
        def _():
            neighbour().wait_recv()

        @pl.when(seat == 0)
        def _():
            halo_got[...] = jnp.zeros_like(halo_got)

        k_all[:REACH] = halo_got[0]
        v_all[:REACH] = halo_got[1]

    def send_behind():
        @pl.when(seat > 0)
        def _():
            work.behind(back)
            behind().start()

    for chunk in sequence:
        for away in range(1, pairs):
            far(chunk, away).wait_recv()
            relay(chunk, away).start()
            if ship:

                @pl.when(ready)
                def _():
                    ship_copy(chunk, tokens_ref.at[rows(chunk)]).start()

                @pl.when(jnp.logical_not(ready))
                def _():
                    ship_copy(chunk, held.at[chunk, source(me, 1)]).start()

            store(chunk, 2 * away).start()
            add(chunk, 2 * away, held[chunk, source(me, away)])
        for away in range(1, pairs):
            relay(chunk, away).wait_recv()
            store(chunk, 2 * away + 1).start()
            add(chunk, 2 * away + 1, held[chunk, source(partner, away)])
        low = chunk * grain
        q_all[low : low + grain] = total[0, chunk].astype(jnp.bfloat16)
        k_all[REACH + low : REACH + low + grain] = total[1, chunk].astype(jnp.bfloat16)
        v_all[REACH + low : REACH + low + grain] = total[2, chunk].astype(jnp.bfloat16)
        done.append(chunk)
        if chunk == chunks - 1:
            halo[0] = k_all[length:]
            halo[1] = v_all[length:]

            @pl.when(seat < seats - 1)
            def _():
                neighbour().start()

        attend_ready(len(done) < chunks - 1)
    attend_ready(False)
    work.end(dk_ref, dv_ref, line_ref)

    @pl.when(seat < seats - 1)
    def _():
        behind().wait_recv()

    @pl.when(seat == seats - 1)
    def _():
        after[...] = jnp.zeros_like(after)

    work.join(dk_ref, dv_ref, after)

    @pl.when(seat > 0)
    def _():
        behind().wait_send()

    @pl.when(seat < seats - 1)
    def _():
        neighbour().wait_send()

    if ship:
        for chunk in sequence:
            ship_copy(chunk, tokens_ref.at[rows(chunk)]).wait_recv()
            pass_on(chunk).start()
            keep(chunk, core).start()
        for chunk in sequence:
            pass_on(chunk).wait_recv()
            keep(chunk, 1 - core).start()
        for chunk in sequence:
            ship_copy(chunk, tokens_ref.at[rows(chunk)]).wait_send()
            pass_on(chunk).wait_send()
            keep(chunk, core).wait()
            keep(chunk, 1 - core).wait()
    for chunk in sequence:
        side(chunk).wait_send()
        for away in range(1, pairs):
            far(chunk, away).wait_send()
            relay(chunk, away).wait_send()
        for slot in range(parts):
            store(chunk, slot).wait()


def attention_grads(tokens, query_weight, key_weight, value_weight, position_bias, out_grad):
    parts = lax.axis_size("tp")
    length, block = tokens.shape
    width = query_weight.shape[1]
    heads = position_bias.shape[0]
    chunks = length // GRAIN
    pairs = parts // 2
    vmem = pl.BlockSpec(memory_space=pltpu.VMEM)
    anywhere = pl.BlockSpec(memory_space=pl.ANY)
    low = jnp.bfloat16

    def shape(kind, *sizes):
        return jax.ShapeDtypeStruct(sizes, kind)

    dma = pltpu.SemaphoreType.DMA
    ship = paired(lax.axis_size("sp"), parts)
    extra = []
    if ship:
        extra = [
            pltpu.VMEM((chunks, 2, GRAIN, block), jnp.bfloat16),
            dma((chunks,)),
            dma((chunks,)),
            dma((chunks,)),
            dma((chunks,)),
            dma((chunks, 2)),
        ]
    return pl.pallas_call(
        functools.partial(gather_kernel, parts),
        in_specs=[vmem, anywhere, anywhere, anywhere, vmem, vmem],
        out_specs=[anywhere] * 2 + [vmem] * 4,
        out_shape=[
            shape(low, length, block * parts),
            shape(low, *((length, 2 * block) if ship else (8, LANES))),
            shape(low, length, width),
            shape(low, length, width),
            shape(low, length, width),
            shape(jnp.float32, heads, TABLE),
        ],
        scratch_shapes=[
            pltpu.VMEM((chunks, parts, GRAIN, block), low),
            pltpu.VMEM((parts, 3, block, width), jnp.bfloat16),
            pltpu.VMEM((3, chunks, GRAIN, width), jnp.float32),
            pltpu.VMEM((2, REACH, width), low),
            pltpu.VMEM((2, REACH, width), low),
            pltpu.VMEM((2, REACH, width), low),
            pltpu.VMEM((2, REACH, width), low),
            pltpu.VMEM((length, width), low),
            pltpu.VMEM((length + REACH, width), low),
            pltpu.VMEM((length + REACH, width), low),
            pltpu.VMEM((heads, ROWS, WINDOW), jnp.float32),
            pltpu.VMEM((heads, ROWS, WINDOW), jnp.float32),
            pltpu.VMEM((length + REACH, width), jnp.float32),
            pltpu.VMEM((length + REACH, width), jnp.float32),
            dma((chunks,)),
            dma((chunks,)),
            dma((chunks, pairs - 1)),
            dma((chunks, pairs - 1)),
            dma((chunks, pairs - 1)),
            dma((chunks, pairs - 1)),
            dma(()),
            dma(()),
            dma(()),
            dma(()),
            dma((parts, 3)),
            dma((chunks, parts)),
        ]
        + extra,
        compiler_params=pltpu.CompilerParams(
            collective_id=1, has_side_effects=True, vmem_limit_bytes=56 * 1024 * 1024
        ),
        cost_estimate=pl.CostEstimate(
            flops=6 * length * block * parts * width, bytes_accessed=150_000_000, transcendentals=0
        ),
    )(tokens, query_weight, key_weight, value_weight, out_grad, position_bias)


def shards(tokens, query_weight, key_weight, value_weight, position_bias, out_grad):
    outs = attention_grads(
        tokens, query_weight, key_weight, value_weight, position_bias, out_grad
    )
    whole, theirs, query_grad, key_grad, value_grad, lines = outs
    *large, bias_grad = final_grads(
        whole,
        (theirs,) if paired(lax.axis_size("sp"), lax.axis_size("tp")) else (),
        (query_grad, key_grad, value_grad),
        lines,
        (query_weight, key_weight, value_weight),
        position_bias.shape[1],
    )
    return (*hand_on(large), bias_grad)


def hand_kernel(*refs):
    half = len(refs) // 2
    for source, target in zip(refs[:half], refs[half:]):
        target[...] = source[...]


def hand_on(arrays, steps=2):
    specs = [
        pl.BlockSpec((array.shape[0], array.shape[1] // steps), lambda i: (0, i))
        for array in arrays
    ]
    size = sum(2 * array.size * array.dtype.itemsize for array in arrays)
    return pl.pallas_call(
        hand_kernel,
        grid=(steps,),
        in_specs=specs,
        out_specs=specs,
        out_shape=[jax.ShapeDtypeStruct(array.shape, array.dtype) for array in arrays],
        cost_estimate=pl.CostEstimate(flops=0, bytes_accessed=size, transcendentals=0),
    )(*arrays)


def solution(mesh):
    in_specs = (
        P("sp", "tp"),
        P(None, "tp"),
        P(None, "tp"),
        P(None, "tp"),
        P("tp", None),
        P("sp", "tp"),
    )
    out_specs = (P("sp", "tp"), P("sp", "tp"), P("sp", "tp"), P("sp", "tp"), P("tp", None))
    return jax.shard_map(shards, mesh=mesh, in_specs=in_specs, out_specs=out_specs, check_vma=False)
```
